32 devices in a mesh: rep: 2 (over x), fs: 8 (over z, y), tp: 2 (over core).
Axes of the slice: x: 2, y: 2, z: 4, core: 2. Of those that a mesh axis runs over, the one named last changes fastest.
Arguments:
- tokens: bfloat16 [12288, 2048], P(('rep', 'fs', 'tp')), may hold values from -6 to 6
- outer_weight: float32 [2048, 1536], P('fs', 'tp'), may hold values from -0.125 to 0.125
- inner_weight: float32 [2048, 1536], P('fs', 'tp'), may hold values from -0.125 to 0.125
- value_weight: float32 [2048, 1536], P('fs', 'tp'), may hold values from -0.125 to 0.125
- conv_taps: float32 [3, 1536], P(None, 'tp'), may hold values from -3 to 3
- mix_out: float32 [1536, 2048], P('tp', 'fs'), may hold values from -0.15625 to 0.15625
- norm_first: float32 [2048], replicated, may hold values from 0.1 to 1.9
- up_weight: float32 [2048, 4096], P('fs', 'tp'), may hold values from -0.125 to 0.125
- down_weight: float32 [4096, 2048], P('tp', 'fs'), may hold values from -0.09375 to 0.09375
- norm_second: float32 [2048], replicated, may hold values from 0.1 to 1.9
Outputs:
- encoded: bfloat16 [12288, 2048], P(('rep', 'fs', 'tp'))
The draws below stay inside these ranges and needn't reach their ends.
All inputs are finite; a program needn't handle non-finite values.
Results may differ from the reference program's by a relative error of at most 0.015.
Values may be sent and summed in bfloat16 or wider, within the bound.
A program may use at most 128 MiB of HBM per device.

```python
import jax
import jax.numpy as jnp
from jax import lax

D = 2048
WA = 1536
FF = 4096
SEQ = 128
TOK_DEV = 384
TOKENS = 12288


def level_of(own_key, dims, split, least, top_value):
    gain, own = 1.0, jax.random.fold_in(own_key, 6)
    for axis_at, parts in split:
        steps = jnp.exp(jax.random.uniform(jax.random.fold_in(own, axis_at), (parts,), jnp.float32, least / len(split), top_value / len(split)))
        gain = gain * jnp.repeat(steps, dims[axis_at] // parts).reshape([-1 if axis == axis_at else 1 for axis in range(len(dims))])
    return gain


def gaussian(rng, dims, width, reach, split=(), kind=jnp.bfloat16):
    drawn = jax.random.normal(rng, dims, jnp.float32) * width
    if len(split) > 0:
        drawn = level_of(rng, dims, split, -0.22, 0.18) * drawn
    return jnp.clip(drawn, min=-reach, max=reach).astype(kind)


def setup_inputs(seed: int = 0) -> dict:
    arg_keys = jax.random.split(jax.random.key(seed), 11)
    tokens = gaussian(arg_keys[0], (TOKENS, D), 1.0, 6.0, ((0, 32),))
    outer_weight = gaussian(arg_keys[1], (D, WA), D ** -0.5, 0.125, ((0, 8), (1, 2)), jnp.float32)
    inner_weight = gaussian(arg_keys[2], (D, WA), D ** -0.5, 0.125, ((0, 8), (1, 2)), jnp.float32)
    value_weight = gaussian(arg_keys[3], (D, WA), D ** -0.5, 0.125, ((0, 8), (1, 2)), jnp.float32)
    conv_taps = gaussian(arg_keys[4], (3, WA), 0.6, 3.0, ((1, 2),), jnp.float32)
    mix_out = gaussian(arg_keys[5], (WA, D), WA ** -0.5, 0.15625, ((0, 2), (1, 8)), jnp.float32)
    norm_first = jnp.clip(1.0 + 0.18 * jax.random.normal(arg_keys[6], (D,), jnp.float32), 0.1, 1.9)
    up_weight = gaussian(arg_keys[7], (D, FF), D ** -0.5, 0.125, ((0, 8), (1, 2)), jnp.float32)
    down_weight = gaussian(arg_keys[8], (FF, D), FF ** -0.5, 0.09375, ((0, 2), (1, 8)), jnp.float32)
    norm_second = jnp.clip(1.0 + 0.18 * jax.random.normal(arg_keys[9], (D,), jnp.float32), 0.1, 1.9)
    return {"tokens": tokens, "outer_weight": outer_weight, "inner_weight": inner_weight, "value_weight": value_weight, "conv_taps": conv_taps, "mix_out": mix_out, "norm_first": norm_first, "up_weight": up_weight, "down_weight": down_weight, "norm_second": norm_second}


residual_scale = 2.0 ** 0.25
norm_epsilon = 1e-05

def layer_norm(values, scaling):
    center = values - lax.optimization_barrier(jnp.mean(values, axis=-1, keepdims=True))
    spread = lax.optimization_barrier(jnp.mean(center * center, axis=-1, keepdims=True))
    return center * lax.rsqrt(spread + norm_epsilon) * scaling

def reference(tokens, outer_weight, inner_weight, value_weight, conv_taps, mix_out, norm_first, up_weight, down_weight, norm_second):
    outer_bf = outer_weight.astype(jnp.bfloat16)
    inner_bf = inner_weight.astype(jnp.bfloat16)
    value_bf = value_weight.astype(jnp.bfloat16)
    mixout_bf = mix_out.astype(jnp.bfloat16)
    upward_bf = up_weight.astype(jnp.bfloat16)
    downward_bf = down_weight.astype(jnp.bfloat16)
    blocks = tokens.reshape(-1, TOK_DEV * 8, D)

    def one_block(rows):
        outer = jnp.dot(rows, outer_bf, preferred_element_type=jnp.float32)
        inner = jnp.dot(rows, inner_bf, preferred_element_type=jnp.float32)
        value = jnp.dot(rows, value_bf, preferred_element_type=jnp.float32)
        framed = (inner * value).reshape(-1, SEQ, WA)
        padded = jnp.pad(framed, ((0, 0), (1, 1), (0, 0)))
        convolved = padded[:, :-2] * conv_taps[0] + framed * conv_taps[1] + padded[:, 2:] * conv_taps[2]
        mixed = (outer * convolved.reshape(-1, WA)).astype(jnp.bfloat16)
        mixing = jnp.dot(mixed, mixout_bf, preferred_element_type=jnp.float32)
        first = layer_norm(residual_scale * rows.astype(jnp.float32) + mixing, norm_first).astype(jnp.bfloat16)
        raised = jax.nn.relu(jnp.dot(first, upward_bf, preferred_element_type=jnp.float32))
        hidden = (raised * raised).astype(jnp.bfloat16)
        lowered = jnp.dot(hidden, downward_bf, preferred_element_type=jnp.float32)
        return layer_norm(residual_scale * first.astype(jnp.float32) + lowered, norm_second).astype(jnp.bfloat16)
    return lax.map(one_block, blocks).reshape(tokens.shape[0], D)
```

```python
import functools

import jax
import jax.numpy as jnp
from jax import lax
from jax.experimental import pallas as pl
from jax.experimental.pallas import tpu as pltpu
from jax.sharding import PartitionSpec as P

SEQ = 128


residual_scale = 2.0**0.25
norm_epsilon = 1e-05


def layer_norm(values, scaling):
    center = values - jnp.mean(values, axis=-1, keepdims=True)
    spread = jnp.mean(center * center, axis=-1, keepdims=True)
    return center * lax.rsqrt(spread + norm_epsilon) * scaling


def short_conv(product, conv_taps):
    places = jnp.arange(product.shape[0], dtype=jnp.int32) % SEQ
    blank = jnp.zeros((1, product.shape[1]), jnp.float32)
    before = jnp.concatenate([blank, product[:-1]], axis=0)
    after = jnp.concatenate([product[1:], blank], axis=0)
    before = jnp.where((places > 0)[:, None], before, 0.0)
    after = jnp.where((places < SEQ - 1)[:, None], after, 0.0)
    return conv_taps[0] * before + conv_taps[1] * product + conv_taps[2] * after


def local(
    tokens,
    outer_weight,
    inner_weight,
    value_weight,
    conv_taps,
    mix_out,
    norm_first,
    up_weight,
    down_weight,
    norm_second,
):
    grouped = lax.all_gather(tokens, "tp", axis=0, tiled=True)
    outer_bf = outer_weight.astype(jnp.bfloat16)
    inner_bf = inner_weight.astype(jnp.bfloat16)
    value_bf = value_weight.astype(jnp.bfloat16)
    outer_full, inner_full, value_full = (
        lax.all_gather(outer_bf, "fs", axis=0, tiled=True),
        lax.all_gather(inner_bf, "fs", axis=0, tiled=True),
        lax.all_gather(value_bf, "fs", axis=0, tiled=True),
    )
    outer = jnp.dot(grouped, outer_full, preferred_element_type=jnp.float32)
    inner = jnp.dot(grouped, inner_full, preferred_element_type=jnp.float32)
    value = jnp.dot(grouped, value_full, preferred_element_type=jnp.float32)
    mixed = (outer * short_conv(inner * value, conv_taps)).astype(jnp.bfloat16)
    mixout_full = lax.all_gather(mix_out.astype(jnp.bfloat16), "fs", axis=1, tiled=True)
    selected = mixed
    mixing = lax.psum_scatter(
        jnp.dot(selected, mixout_full, preferred_element_type=jnp.float32).astype(jnp.bfloat16),
        "tp",
        scatter_dimension=0,
        tiled=True,
    ).astype(jnp.float32)
    first = layer_norm(residual_scale * tokens.astype(jnp.float32) + mixing, norm_first).astype(
        jnp.bfloat16
    )
    grouped_first = lax.all_gather(first, "tp", axis=0, tiled=True)
    upward_bf = up_weight.astype(jnp.bfloat16)
    upward_full = lax.all_gather(upward_bf, "fs", axis=0, tiled=True)
    raised = jnp.dot(grouped_first, upward_full, preferred_element_type=jnp.float32)
    raised = jax.nn.relu(raised)
    hidden = (raised * raised).astype(jnp.bfloat16)
    down_full = lax.all_gather(down_weight.astype(jnp.bfloat16), "fs", axis=1, tiled=True)
    selected = hidden
    lowered = lax.psum_scatter(
        jnp.dot(selected, down_full, preferred_element_type=jnp.float32).astype(jnp.bfloat16),
        "tp",
        scatter_dimension=0,
        tiled=True,
    ).astype(jnp.float32)
    return layer_norm(residual_scale * first.astype(jnp.float32) + lowered, norm_second).astype(
        jnp.bfloat16
    )


MESH = pl.DeviceIdType.MESH
BF = jnp.bfloat16
F32 = jnp.float32


def dot(a, b):
    return jnp.dot(a, b, preferred_element_type=F32)


def layer_kernel(
    n,
    tokens_hbm,
    outer_hbm,
    inner_hbm,
    value_hbm,
    taps_ref,
    mix_hbm,
    norm1_ref,
    up_hbm,
    down_hbm,
    norm2_ref,
    out_ref,
    wa,
    wb,
    wc,
    wd,
    tok,
    acc,
    mixed,
    own,
    psend,
    precv,
    xsend,
    xrecv,
    fst,
    hid,
    load_sem,
    ring_send,
    ring_recv,
    tp_send,
    tp_recv,
    x_send,
    x_recv,
):
    half = n // 2
    r = lax.axis_index("rep")
    f = lax.axis_index("fs")
    t = lax.axis_index("tp")
    rows = tokens_hbm.shape[0]
    both = 2 * rows
    d = tokens_hbm.shape[1]
    ks = outer_hbm.shape[0]
    wch = wb.shape[1]
    ff = wc.shape[1]
    nc = wb.shape[2]
    OWN, TWIN, MATE, DIAG = 0, rows, 2 * rows, 3 * rows

    odd = f % 2
    pos = (1 - odd) * (f // 2) + odd * (n - 1 - f // 2)

    def at(place):
        p = (place + 2 * n) % n
        hi = p // half
        return (1 - hi) * (2 * p) + hi * (2 * (n - 1 - p) + 1)

    right = {"fs": at(pos + 1)}
    left = {"fs": at(pos - 1)}
    across = {"rep": 1 - r}
    mate = {"tp": 1 - t}

    def owners(h):
        if h == 0:
            return [f]
        if h == half:
            return [at(pos + half)]
        return [at(pos - h), at(pos + h)]

    def numbered(h):
        return [(0 if h == 0 else 2 * h - 1 + k, o) for k, o in enumerate(owners(h))]

    every = [item for h in range(half + 1) for item in numbered(h)]

    mine = pl.multiple_of(r * ff, 128)
    share_at = pl.multiple_of(r * wch, 128)
    first_down = min(ff, both)
    rest_down = ff - first_down
    loads = [
        pltpu.make_async_copy(
            src.at[:, pl.ds(share_at, wch)],
            acc.at[pl.ds(i * ks, ks), pl.ds(0, wch)],
            load_sem.at[i],
        )
        for i, src in enumerate((outer_hbm, inner_hbm, value_hbm))
    ]
    loads += [
        pltpu.make_async_copy(
            mix_hbm.at[pl.ds(share_at, wch)], own.at[0, pl.ds(0, wch)], load_sem.at[3]
        ),
        pltpu.make_async_copy(
            up_hbm.at[:, pl.ds(mine, ff)],
            acc.at[pl.ds(3 * ks, ks), pl.ds(0, ff)],
            load_sem.at[4],
        ),
        pltpu.make_async_copy(
            down_hbm.at[pl.ds(mine, first_down)],
            own.at[1, pl.ds(0, first_down)],
            load_sem.at[5],
        ),
        pltpu.make_async_copy(tokens_hbm, tok.at[pl.ds(0, rows)], load_sem.at[6]),
    ]
    if rest_down:
        loads.append(
            pltpu.make_async_copy(
                down_hbm.at[pl.ds(mine + first_down, rest_down)],
                own.at[2, pl.ds(0, rest_down)],
                load_sem.at[7],
            )
        )
    for load in loads[:3]:
        load.start()

    barrier = pltpu.get_barrier_semaphore()
    for device in (right, left, across, mate):
        pl.semaphore_signal(barrier, inc=1, device_id=device, device_id_type=MESH)
    pl.semaphore_wait(barrier, 4)

    mate_copies = {}
    across_copies = {}

    def mate_copy(key, src, dst):
        if key not in mate_copies:
            i = len(mate_copies)
            mate_copies[key] = pltpu.make_async_remote_copy(
                src_ref=src,
                dst_ref=dst,
                send_sem=tp_send.at[i],
                recv_sem=tp_recv.at[i],
                device_id=mate,
                device_id_type=MESH,
            )
        return mate_copies[key]

    def across_copy(key, src, dst):
        if key not in across_copies:
            i = len(across_copies)
            across_copies[key] = pltpu.make_async_remote_copy(
                src_ref=src,
                dst_ref=dst,
                send_sem=x_send.at[i],
                recv_sem=x_recv.at[i],
                device_id=across,
                device_id_type=MESH,
            )
        return across_copies[key]

    def piece(ti, which, owner):
        if ti == 0:
            u = ks // 2
            return wa.at[pl.ds(pl.multiple_of(owner * ks + which * u, 16), u)]
        if ti == 1:
            return wb.at[owner, pl.ds(which * (wch // 2), wch // 2)]
        if ti == 2:
            u = ks // 2
            return wc.at[pl.ds(pl.multiple_of(owner * ks + which * u, 16), u)]
        return wd.at[owner, pl.ds(which * (ff // 2), ff // 2)]

    per = 4 * half - 2
    index = {}
    for h in range(1, half + 1):
        for kind in ("Rq", "Rp", "Lq", "Lp"):
            if h == half and kind in ("Rp", "Lq"):
                continue
            index[kind, h] = len(index)

    copies = {}

    def message(ti, kind, h):
        key = (ti, kind, h)
        if key not in copies:
            which = int(kind[1] == "p")
            if kind[0] == "R":
                src, device = at(pos - (h - 1)), right
            else:
                src, device = at(pos + (h - 1)), left
            i = ti * per + index[kind, h]
            ref = piece(ti, which, src)
            copies[key] = pltpu.make_async_remote_copy(
                src_ref=ref,
                dst_ref=ref,
                send_sem=ring_send.at[i],
                recv_sem=ring_recv.at[i],
                device_id=device,
                device_id_type=MESH,
            )
        return copies[key]

    def send(ti, kind, h):
        if ti < 4 and (kind, h) in index:
            message(ti, kind, h).start()

    def got(ti, kind, h):
        message(ti, kind, h).wait_recv()

    def event(ti, h, which):
        if which == 0:
            got(ti, "Rq", h)
            send(ti, "Rq", h + 1)
            if h == half:
                send(ti + 1, "Rp", 1)
            got(ti, "Lp", h)
            send(ti, "Lp", h + 1)
            if h == half:
                send(ti + 1, "Lq", 1)
        else:
            got(ti, "Rp", h)
            if h + 1 < half:
                send(ti, "Rp", h + 1)
            else:
                send(ti + 1, "Rq", 1)
            got(ti, "Lq", h)
            if h + 1 < half:
                send(ti, "Lq", h + 1)
            else:
                send(ti + 1, "Lp", 1)

    def events(ti):
        out = []
        for h in range(1, half + 1):
            out.append((ti, h, 0))
            if h < half:
                out.append((ti, h, 1))
        return out

    def block_of(o):
        return pl.ds(pl.multiple_of(o * ks, 128), ks)

    def twin_tokens(k, o):
        return across_copy(
            ("tok", k),
            tokens_hbm.at[:, block_of(o)],
            tok.at[pl.ds(TWIN, rows), block_of(o)],
        )

    def diag_tokens(k, o):
        return mate_copy(
            ("tok", k),
            tok.at[pl.ds(TWIN, rows), block_of(o)],
            tok.at[pl.ds(DIAG, rows), block_of(o)],
        )

    share = mate_copy("share", tokens_hbm, tok.at[pl.ds(MATE, rows)])
    for k, o in every:
        twin_tokens(k, o).start()
    for i in range(3):
        loads[i].wait()
        wa[pl.ds(pl.multiple_of(f * ks, 16), ks), pl.ds(i * wch, wch)] = acc[
            pl.ds(i * ks, ks), pl.ds(0, wch)
        ].astype(BF)
    send(0, "Rq", 1)
    send(0, "Lp", 1)
    send(0, "Rp", 1)
    send(0, "Lq", 1)
    for load in loads[3:]:
        load.start()
    share.start()
    loads[3].wait()
    wb[f] = own[0, pl.ds(0, wch)].astype(BF)
    loads[4].wait()
    wc[pl.ds(pl.multiple_of(f * ks, 16), ks), :] = acc[
        pl.ds(3 * ks, ks), pl.ds(0, ff)
    ].astype(BF)
    loads[5].wait()
    wd[f, pl.ds(0, first_down)] = own[1, pl.ds(0, first_down)].astype(BF)
    if rest_down:
        loads[7].wait()
        wd[f, pl.ds(first_down, rest_down)] = own[2, pl.ds(0, rest_down)].astype(BF)
    loads[6].wait()
    share.wait_recv()

    tn = 256
    seq = SEQ
    pieces = rows // seq
    most = pieces - 1
    EARLY, LATE, ALL = (0, most * seq), (most * seq, seq), (0, rows)

    def relay_tokens(h):
        for k, o in numbered(h):
            twin_tokens(k, o).wait_recv()
            diag_tokens(k, o).start()

    def project(h, base):
        who = owners(h)

        def unit(i, _):
            m = pl.ds(pl.multiple_of(i % 2 * MATE + base, 16), rows)
            c = pl.ds(pl.multiple_of(i // 2 * wch, 128), wch)
            total = None
            for o in who:
                w = wa[pl.ds(pl.multiple_of(o * ks, 16), ks), c]
                term = dot(tok[m, block_of(o)], w)
                total = term if total is None else total + term
            if h == 0:
                acc[m, c] = total
            else:
                acc[m, c] += total
            return 0

        lax.fori_loop(0, 2 * 3, unit, 0)

    def project_near(h):
        project(h, OWN)

    def project_far(h):
        for k, o in numbered(h):
            diag_tokens(k, o).wait_recv()
        project(h, TWIN)

    def mix(base, part):
        start, count = part
        tc = 128
        seqs = count // seq

        def unit(i, _):
            j = i % (2 * seqs)
            m = pl.ds(
                pl.multiple_of(base + j // seqs * MATE + start + j % seqs * seq, seq), seq
            )
            c = pl.multiple_of(i // (2 * seqs) * tc, tc)
            o = acc[m, pl.ds(c, tc)]
            p = (
                acc[m, pl.ds(pl.multiple_of(wch + c, tc), tc)]
                * acc[m, pl.ds(pl.multiple_of(2 * wch + c, tc), tc)]
            )
            place = lax.broadcasted_iota(jnp.int32, p.shape, 0)
            before = jnp.where(place > 0, pltpu.roll(p, 1, 0), 0.0)
            after = jnp.where(place < seq - 1, pltpu.roll(p, seq - 1, 0), 0.0)
            taps = taps_ref[:, pl.ds(pl.multiple_of(share_at + c, tc), tc)]
            conv = taps[0:1] * before + taps[1:2] * p + taps[2:3] * after
            mixed[m, pl.ds(c, tc)] = (o * conv).astype(BF)
            return 0

        lax.fori_loop(0, 2 * seqs * (wch // tc), unit, 0)

    def raise_part(size, start, x_base, acc_base, hs, new, final):
        who = [o for h in hs for o in owners(h)]
        tiles = ff // tn

        def unit(i, _):
            side = i % 2
            c = pl.ds(pl.multiple_of(i // 2 * tn, tn), tn)
            x_row = pl.multiple_of(x_base + side * MATE + start, 16)
            total = None
            for o in who:
                x = fst[pl.ds(x_row, size), block_of(o)]
                term = dot(x, wc[pl.ds(pl.multiple_of(o * ks, 16), ks), c])
                total = term if total is None else total + term
            span = pl.ds(pl.multiple_of(acc_base + side * rows + start, 16), size)
            if not new:
                total = total + acc[span, c]
            if final:
                total = jnp.maximum(total, 0.0)
                hid[pl.ds(x_row, size), c] = (total * total).astype(BF)
            else:
                acc[span, c] = total
            return 0

        lax.fori_loop(0, 2 * tiles, unit, 0)

    def raise_near(h):
        raise_part(rows, 0, OWN, 0, [h], h == 0, h == half)

    def raise_far(part):
        start, count = part
        for p in range(start // seq, (start + count) // seq):
            diag_first(p).wait_recv()
        raise_part(count, start, TWIN, both, range(half + 1), True, True)

    def far_block(kind, k, o, part):
        span = pl.ds(rows + part[0], part[1])
        return mate_copy((kind, k, part), psend.at[o, span], precv.at[o, span])

    def near_block(kind, k, o):
        span = pl.ds(0, rows)
        return mate_copy((kind, k), psend.at[o, span], precv.at[o, span])

    def across_block(kind, k, o, part):
        span = pl.ds(*part)
        return across_copy((kind, k, part), xsend.at[o, span], xrecv.at[o, span])

    used = []

    def far(kind, x_ref, w_ref, h, part):
        start, count = part
        for k, o in numbered(h):
            span = pl.ds(rows + start, count)
            psend[o, span] = dot(x_ref[pl.ds(DIAG + start, count), :], w_ref[o]).astype(BF)
            far_block(kind, k, o, part).start()
            own[o, span] = dot(x_ref[pl.ds(TWIN + start, count), :], w_ref[o])

    def pass_far(kind, h, part):
        start, count = part
        for k, o in numbered(h):
            far_block(kind, k, o, part).wait_recv()
            span = pl.ds(rows + start, count)
            xsend[o, pl.ds(start, count)] = (own[o, span] + precv[o, span].astype(F32)).astype(BF)
            across_block(kind, k, o, part).start()
            used.append((kind, k, o, part))

    def near(kind, x_ref, w_ref, h):
        span = pl.ds(0, rows)
        for k, o in numbered(h):
            psend[o, span] = dot(x_ref[pl.ds(MATE, rows), :], w_ref[o]).astype(BF)
            near_block(kind, k, o).start()
            own[o, span] = dot(x_ref[pl.ds(OWN, rows), :], w_ref[o])

    def mixout_far(h, part):
        far("mix", mixed, wb, h, part)

    def mixout_near(h):
        near("mix", mixed, wb, h)

    def lower_far(h, part):
        far("low", hid, wd, h, part)

    def lower_near(h):
        near("low", hid, wd, h)

    def mix_pass(h, part):
        pass_far("mix", h, part)

    def low_pass(h, part):
        pass_far("low", h, part)

    def norm(base_ref, gain_ref, dest_ref, start, count):
        tm = 32

        def unit(i, _):
            m = pl.multiple_of(start + i * tm, tm)
            parts = []
            for b in range(n):
                part = (
                    residual_scale
                    * base_ref[pl.ds(m, tm), pl.ds(b * nc, nc)].astype(F32)
                    + own[b, pl.ds(m, tm)]
                )
                for term in (precv, xrecv):
                    part = part + term[b, pl.ds(m, tm)].astype(F32)
                parts.append(part)
            total = parts[0]
            for b in range(1, n):
                total = total + parts[b]
            mean = jnp.sum(total, axis=-1, keepdims=True) / d
            parts = [p - mean for p in parts]
            square = parts[0] * parts[0]
            for b in range(1, n):
                square = square + parts[b] * parts[b]
            spread = jnp.sum(square, axis=-1, keepdims=True) / d
            scale = lax.rsqrt(spread + norm_epsilon)
            for b in range(n):
                cols = pl.ds(b * nc, nc)
                dest_ref[pl.ds(m, tm), cols] = (
                    parts[b] * scale * gain_ref[:, cols]
                ).astype(BF)
            return 0

        lax.fori_loop(0, count // tm, unit, 0)

    def near_first(p):
        return mate_copy(
            ("near", p), fst.at[pl.ds(p * seq, seq)], fst.at[pl.ds(MATE + p * seq, seq)]
        )

    def twin_first(p):
        return across_copy(
            ("twin", p), fst.at[pl.ds(p * seq, seq)], fst.at[pl.ds(TWIN + p * seq, seq)]
        )

    def diag_first(p):
        return mate_copy(
            ("diag", p),
            fst.at[pl.ds(TWIN + p * seq, seq)],
            fst.at[pl.ds(DIAG + p * seq, seq)],
        )

    def take_near_sums(kind):
        for k, o in every:
            near_block(kind, k, o).wait_recv()

    def make_first(part):
        for k, o in every:
            across_block("mix", k, o, part).wait_recv()
        start, count = part
        for p in range(start // seq, (start + count) // seq):
            norm(tok, norm1_ref, fst, p * seq, seq)
            twin_first(p).start()
            near_first(p).start()

    def take_near():
        for p in range(pieces):
            near_first(p).wait_recv()

    def relay_first(p):
        twin_first(p).wait_recv()
        diag_first(p).start()

    def free_sends():
        for k, o in every:
            near_block("mix", k, o).wait_send()
            for part in (EARLY, LATE):
                far_block("mix", k, o, part).wait_send()
                across_block("mix", k, o, part).wait_send()

    plan = {}

    def after(ti, h, which, *work):
        plan.setdefault((ti, h, which), []).extend(work)

    def do(function, *values):
        return lambda: function(*values)

    last = half - 1

    after(0, 1, 0, do(relay_tokens, 0), do(project_near, 0), do(project_far, 0))
    for h in range(1, last):
        after(0, h, 1, do(relay_tokens, h))
        after(0, h + 1, 0, do(project_near, h), do(project_far, h))
    after(0, last, 1, do(relay_tokens, last), do(relay_tokens, half))
    after(0, last, 1, do(project_near, last), do(project_far, last))
    after(0, half, 0, do(project_far, half), do(mix, TWIN, EARLY), do(mixout_far, 0, EARLY))
    after(1, 1, 0, do(project_near, half), do(mix_pass, 0, EARLY), do(mix, TWIN, LATE))
    after(1, 1, 1, do(mixout_far, 1, EARLY), do(mix, OWN, ALL))
    after(1, 2, 0, do(mix_pass, 1, EARLY))
    for h in range(2, half):
        after(1, h, 1, do(mixout_far, h, EARLY))
        after(1, h + 1, 0, do(mix_pass, h, EARLY))
    after(1, half, 0, do(mixout_far, half, EARLY), do(mixout_far, 0, LATE))
    after(1, half, 0, do(mix_pass, half, EARLY))
    for h in range(1, half + 1):
        after(1, half, 0, do(mixout_far, h, LATE), do(mix_pass, h - 1, LATE))
    after(1, half, 0, do(mix_pass, half, LATE))
    for h in range(half + 1):
        after(1, half, 0, do(mixout_near, h))
    after(2, 1, 1, do(take_near_sums, "mix"), do(make_first, EARLY))
    after(2, 2, 1, do(make_first, LATE), do(take_near))
    after(2, 2, 1, do(raise_near, 0), do(raise_near, 1))
    after(2, 3, 0, do(raise_near, 2), do(free_sends))
    for h in range(3, half):
        after(2, h, 1, do(raise_near, h))
    after(2, half, 0, do(relay_first, 0), do(raise_near, half))
    for p in range(1, most):
        after(3, 1, 1, do(relay_first, p))
    after(3, 1, 1, do(lower_near, 0), do(raise_far, EARLY), do(lower_far, 0, EARLY))
    after(3, 1, 1, do(lower_far, 1, EARLY), do(low_pass, 0, EARLY))
    after(3, 2, 0, do(low_pass, 1, EARLY), do(lower_near, 1))
    after(3, 2, 0, do(relay_first, most), do(raise_far, LATE))
    after(3, 2, 0, do(lower_far, 0, LATE), do(lower_far, 1, LATE))
    after(3, 2, 0, do(low_pass, 0, LATE), do(low_pass, 1, LATE))
    for h in range(2, half):
        after(3, h, 1, do(lower_far, h, ALL), do(lower_near, h), do(low_pass, h, ALL))
    after(3, half, 0, do(lower_far, half, ALL), do(lower_near, half))
    after(3, half, 0, do(low_pass, half, ALL))

    for ti in range(4):
        for e in events(ti):
            event(*e)
            for work in plan.get(e, ()):
                work()

    take_near_sums("low")
    for kind, k, o, part in used:
        if kind == "low":
            across_block(kind, k, o, part).wait_recv()
    norm(fst, norm2_ref, out_ref, 0, rows)

    for key, copy in mate_copies.items():
        if key[0] != "mix":
            copy.wait_send()
    for key, copy in across_copies.items():
        if key[0] != "mix":
            copy.wait_send()
    for key in copies:
        copies[key].wait_send()


def fits(mesh, args):
    n = mesh.shape["fs"]
    rows, d = args[0].shape
    ks = args[1].shape[0]
    wch = args[1].shape[1] // 2
    nc = args[5].shape[1]
    ff = args[7].shape[1] // 2
    return (
        mesh.shape["rep"] == 2
        and mesh.shape["tp"] == 2
        and n % 2 == 0
        and n >= 8
        and ks % 128 == 0
        and nc == 256
        and wch % 128 == 0
        and ff % 256 == 0
        and wch <= 2 * rows
        and ff <= 4 * rows
        and ff <= 3 * wch
        and ks <= rows
        and rows % SEQ == 0
        and rows >= 2 * SEQ
    )


def fused(mesh, *args):
    (
        tokens,
        outer_weight,
        inner_weight,
        value_weight,
        conv_taps,
        mix_out,
        norm_first,
        up_weight,
        down_weight,
        norm_second,
    ) = args
    n = mesh.shape["fs"]
    rows, d = tokens.shape
    ks = outer_weight.shape[0]
    wch = outer_weight.shape[1] // 2
    ff = up_weight.shape[1] // 2
    nc = mix_out.shape[1]
    both = 2 * rows
    anywhere = pl.BlockSpec(memory_space=pl.ANY)
    vmem = pl.BlockSpec(memory_space=pltpu.VMEM)
    messages = 4 * (2 * n - 2)
    pairs = 1 + n + 6 * n + 2 * (rows // SEQ)
    crosses = n + 4 * n + rows // SEQ
    return pl.pallas_call(
        functools.partial(layer_kernel, n),
        out_shape=jax.ShapeDtypeStruct((rows, d), BF),
        in_specs=[
            anywhere,
            anywhere,
            anywhere,
            anywhere,
            vmem,
            anywhere,
            vmem,
            anywhere,
            anywhere,
            vmem,
        ],
        out_specs=vmem,
        scratch_shapes=[
            pltpu.VMEM((n * ks, 3 * wch), BF),
            pltpu.VMEM((n, wch, nc), BF),
            pltpu.VMEM((n * ks, ff), BF),
            pltpu.VMEM((n, ff, nc), BF),
            pltpu.VMEM((2 * both, d), BF),
            pltpu.VMEM((2 * both, 3 * wch), F32),
            pltpu.VMEM((2 * both, wch), BF),
            pltpu.VMEM((n, both, nc), F32),
            pltpu.VMEM((n, both, nc), BF),
            pltpu.VMEM((n, both, nc), BF),
            pltpu.VMEM((n, rows, nc), BF),
            pltpu.VMEM((n, rows, nc), BF),
            pltpu.VMEM((2 * both, d), BF),
            pltpu.VMEM((2 * both, ff), BF),
            pltpu.SemaphoreType.DMA((8,)),
            pltpu.SemaphoreType.DMA((messages,)),
            pltpu.SemaphoreType.DMA((messages,)),
            pltpu.SemaphoreType.DMA((pairs,)),
            pltpu.SemaphoreType.DMA((pairs,)),
            pltpu.SemaphoreType.DMA((crosses,)),
            pltpu.SemaphoreType.DMA((crosses,)),
        ],
        compiler_params=pltpu.CompilerParams(
            collective_id=0, has_side_effects=True, vmem_limit_bytes=67043328
        ),
        name="layer",
    )(
        tokens,
        outer_weight,
        inner_weight,
        value_weight,
        conv_taps,
        mix_out,
        norm_first.reshape(1, d),
        up_weight,
        down_weight,
        norm_second.reshape(1, d),
    )


def solution(mesh):
    def body(*args):
        return fused(mesh, *args) if fits(mesh, args) else local(*args)

    return jax.shard_map(
        body,
        mesh=mesh,
        in_specs=(
            P(("rep", "fs", "tp"), None),
            P("fs", "tp"),
            P("fs", "tp"),
            P("fs", "tp"),
            P(None, "tp"),
            P("tp", "fs"),
            P(),
            P("fs", "tp"),
            P("tp", "fs"),
            P(),
        ),
        out_specs=P(("rep", "fs", "tp"), None),
        check_vma=False,
    )
```

```python
import functools

import jax
import jax.numpy as jnp
from jax import lax
from jax.experimental import pallas as pl
from jax.experimental.pallas import tpu as pltpu
from jax.sharding import PartitionSpec as P

SEQ = 128


residual_scale = 2.0**0.25
norm_epsilon = 1e-05


def layer_norm(values, scaling):
    center = values - jnp.mean(values, axis=-1, keepdims=True)
    spread = jnp.mean(center * center, axis=-1, keepdims=True)
    return center * lax.rsqrt(spread + norm_epsilon) * scaling


def short_conv(product, conv_taps):
    places = jnp.arange(product.shape[0], dtype=jnp.int32) % SEQ
    blank = jnp.zeros((1, product.shape[1]), jnp.float32)
    before = jnp.concatenate([blank, product[:-1]], axis=0)
    after = jnp.concatenate([product[1:], blank], axis=0)
    before = jnp.where((places > 0)[:, None], before, 0.0)
    after = jnp.where((places < SEQ - 1)[:, None], after, 0.0)
    return conv_taps[0] * before + conv_taps[1] * product + conv_taps[2] * after


def local(
    tokens,
    outer_weight,
    inner_weight,
    value_weight,
    conv_taps,
    mix_out,
    norm_first,
    up_weight,
    down_weight,
    norm_second,
):
    grouped = lax.all_gather(tokens, "tp", axis=0, tiled=True)
    outer_bf = outer_weight.astype(jnp.bfloat16)
    inner_bf = inner_weight.astype(jnp.bfloat16)
    value_bf = value_weight.astype(jnp.bfloat16)
    outer_full, inner_full, value_full = (
        lax.all_gather(outer_bf, "fs", axis=0, tiled=True),
        lax.all_gather(inner_bf, "fs", axis=0, tiled=True),
        lax.all_gather(value_bf, "fs", axis=0, tiled=True),
    )
    outer = jnp.dot(grouped, outer_full, preferred_element_type=jnp.float32)
    inner = jnp.dot(grouped, inner_full, preferred_element_type=jnp.float32)
    value = jnp.dot(grouped, value_full, preferred_element_type=jnp.float32)
    mixed = (outer * short_conv(inner * value, conv_taps)).astype(jnp.bfloat16)
    mixout_full = lax.all_gather(mix_out.astype(jnp.bfloat16), "fs", axis=1, tiled=True)
    selected = mixed
    mixing = lax.psum_scatter(
        jnp.dot(selected, mixout_full, preferred_element_type=jnp.float32).astype(jnp.bfloat16),
        "tp",
        scatter_dimension=0,
        tiled=True,
    ).astype(jnp.float32)
    first = layer_norm(residual_scale * tokens.astype(jnp.float32) + mixing, norm_first).astype(
        jnp.bfloat16
    )
    grouped_first = lax.all_gather(first, "tp", axis=0, tiled=True)
    upward_bf = up_weight.astype(jnp.bfloat16)
    upward_full = lax.all_gather(upward_bf, "fs", axis=0, tiled=True)
    raised = jnp.dot(grouped_first, upward_full, preferred_element_type=jnp.float32)
    raised = jax.nn.relu(raised)
    hidden = (raised * raised).astype(jnp.bfloat16)
    down_full = lax.all_gather(down_weight.astype(jnp.bfloat16), "fs", axis=1, tiled=True)
    selected = hidden
    lowered = lax.psum_scatter(
        jnp.dot(selected, down_full, preferred_element_type=jnp.float32).astype(jnp.bfloat16),
        "tp",
        scatter_dimension=0,
        tiled=True,
    ).astype(jnp.float32)
    return layer_norm(residual_scale * first.astype(jnp.float32) + lowered, norm_second).astype(
        jnp.bfloat16
    )


MESH = pl.DeviceIdType.MESH
BF = jnp.bfloat16
F32 = jnp.float32


def dot(a, b):
    return jnp.dot(a, b, preferred_element_type=F32)


def layer_kernel(
    n,
    tokens_hbm,
    outer_hbm,
    inner_hbm,
    value_hbm,
    taps_ref,
    mix_hbm,
    norm1_ref,
    up_hbm,
    down_hbm,
    norm2_ref,
    out_ref,
    wa,
    wb,
    wc,
    wd,
    tok,
    acc,
    mixed,
    own,
    psend,
    precv,
    xsend,
    xrecv,
    fst,
    hid,
    stage,
    load_sem,
    ring_send,
    ring_recv,
    tp_send,
    tp_recv,
    x_send,
    x_recv,
):
    half = n // 2
    r = lax.axis_index("rep")
    f = lax.axis_index("fs")
    t = lax.axis_index("tp")
    rows = tokens_hbm.shape[0]
    both = 2 * rows
    d = tokens_hbm.shape[1]
    ks = outer_hbm.shape[0]
    wch = wb.shape[1]
    ff = wc.shape[1]
    nc = wb.shape[2]
    OWN, TWIN, MATE, DIAG = 0, rows, 2 * rows, 3 * rows

    odd = f % 2
    pos = (1 - odd) * (f // 2) + odd * (n - 1 - f // 2)

    def at(place):
        p = (place + 2 * n) % n
        hi = p // half
        return (1 - hi) * (2 * p) + hi * (2 * (n - 1 - p) + 1)

    right = {"fs": at(pos + 1)}
    left = {"fs": at(pos - 1)}
    across = {"rep": 1 - r}
    mate = {"tp": 1 - t}

    def owners(h):
        if h == 0:
            return [f]
        if h == half:
            return [at(pos + half)]
        return [at(pos - h), at(pos + h)]

    def numbered(h):
        return [(0 if h == 0 else 2 * h - 1 + k, o) for k, o in enumerate(owners(h))]

    every = [item for h in range(half + 1) for item in numbered(h)]

    mine = pl.multiple_of(r * ff, 128)
    share_at = pl.multiple_of(r * wch, 128)
    first_down = min(ff, both)
    rest_down = ff - first_down
    loads = [
        pltpu.make_async_copy(
            src.at[:, pl.ds(share_at, wch)],
            acc.at[pl.ds(i * ks, ks), pl.ds(0, wch)],
            load_sem.at[i],
        )
        for i, src in enumerate((outer_hbm, inner_hbm, value_hbm))
    ]
    loads += [
        pltpu.make_async_copy(
            mix_hbm.at[pl.ds(share_at, wch)], own.at[0, pl.ds(0, wch)], load_sem.at[3]
        ),
        pltpu.make_async_copy(
            up_hbm.at[:, pl.ds(mine, ff)],
            acc.at[pl.ds(3 * ks, ks), pl.ds(0, ff)],
            load_sem.at[4],
        ),
        pltpu.make_async_copy(
            down_hbm.at[pl.ds(mine, first_down)],
            own.at[1, pl.ds(0, first_down)],
            load_sem.at[5],
        ),
        pltpu.make_async_copy(tokens_hbm, tok.at[pl.ds(0, rows)], load_sem.at[6]),
    ]
    if rest_down:
        loads.append(
            pltpu.make_async_copy(
                down_hbm.at[pl.ds(mine + first_down, rest_down)],
                own.at[2, pl.ds(0, rest_down)],
                load_sem.at[7],
            )
        )
    for load in loads[:3]:
        load.start()

    barrier = pltpu.get_barrier_semaphore()
    for device in (right, left, across, mate):
        pl.semaphore_signal(barrier, inc=1, device_id=device, device_id_type=MESH)
    pl.semaphore_wait(barrier, 4)

    mate_copies = {}
    across_copies = {}

    def mate_copy(key, src, dst):
        if key not in mate_copies:
            i = len(mate_copies)
            mate_copies[key] = pltpu.make_async_remote_copy(
                src_ref=src,
                dst_ref=dst,
                send_sem=tp_send.at[i],
                recv_sem=tp_recv.at[i],
                device_id=mate,
                device_id_type=MESH,
            )
        return mate_copies[key]

    def across_copy(key, src, dst):
        if key not in across_copies:
            i = len(across_copies)
            across_copies[key] = pltpu.make_async_remote_copy(
                src_ref=src,
                dst_ref=dst,
                send_sem=x_send.at[i],
                recv_sem=x_recv.at[i],
                device_id=across,
                device_id_type=MESH,
            )
        return across_copies[key]

    def piece(ti, which, owner):
        if ti == 0:
            u = ks // 2
            return wa.at[pl.ds(pl.multiple_of(owner * ks + which * u, 16), u)]
        if ti == 1:
            return wb.at[owner, pl.ds(which * (wch // 2), wch // 2)]
        if ti == 2:
            u = ks // 2
            return wc.at[pl.ds(pl.multiple_of(owner * ks + which * u, 16), u)]
        return wd.at[owner, pl.ds(which * (ff // 2), ff // 2)]

    per = 4 * half - 2
    index = {}
    for h in range(1, half + 1):
        for kind in ("Rq", "Rp", "Lq", "Lp"):
            if h == half and kind in ("Rp", "Lq"):
                continue
            index[kind, h] = len(index)

    copies = {}

    def message(ti, kind, h):
        key = (ti, kind, h)
        if key not in copies:
            which = int(kind[1] == "p")
            if kind[0] == "R":
                src, device = at(pos - (h - 1)), right
            else:
                src, device = at(pos + (h - 1)), left
            i = ti * per + index[kind, h]
            ref = piece(ti, which, src)
            copies[key] = pltpu.make_async_remote_copy(
                src_ref=ref,
                dst_ref=ref,
                send_sem=ring_send.at[i],
                recv_sem=ring_recv.at[i],
                device_id=device,
                device_id_type=MESH,
            )
        return copies[key]

    def send(ti, kind, h):
        if ti < 4 and (kind, h) in index:
            message(ti, kind, h).start()

    def got(ti, kind, h):
        message(ti, kind, h).wait_recv()

    def event(ti, h, which):
        if which == 0:
            got(ti, "Rq", h)
            send(ti, "Rq", h + 1)
            if h == half:
                send(ti + 1, "Rp", 1)
            got(ti, "Lp", h)
            send(ti, "Lp", h + 1)
            if h == half:
                send(ti + 1, "Lq", 1)
        else:
            got(ti, "Rp", h)
            if h + 1 < half:
                send(ti, "Rp", h + 1)
            else:
                send(ti + 1, "Rq", 1)
            got(ti, "Lq", h)
            if h + 1 < half:
                send(ti, "Lq", h + 1)
            else:
                send(ti + 1, "Lp", 1)

    def events(ti):
        out = []
        for h in range(1, half + 1):
            out.append((ti, h, 0))
            if h < half:
                out.append((ti, h, 1))
        return out

    def block_of(o):
        return pl.ds(pl.multiple_of(o * ks, 128), ks)

    def twin_tokens(k, o):
        return across_copy(
            ("tok", k),
            tokens_hbm.at[:, block_of(o)],
            tok.at[pl.ds(TWIN, rows), block_of(o)],
        )

    def diag_tokens(k, o):
        return mate_copy(
            ("tok", k),
            tok.at[pl.ds(TWIN, rows), block_of(o)],
            tok.at[pl.ds(DIAG, rows), block_of(o)],
        )

    share = mate_copy("share", tokens_hbm, tok.at[pl.ds(MATE, rows)])
    for k, o in every:
        twin_tokens(k, o).start()
    for i in range(3):
        loads[i].wait()
        wa[pl.ds(pl.multiple_of(f * ks, 16), ks), pl.ds(i * wch, wch)] = acc[
            pl.ds(i * ks, ks), pl.ds(0, wch)
        ].astype(BF)
    send(0, "Rq", 1)
    send(0, "Lp", 1)
    send(0, "Rp", 1)
    send(0, "Lq", 1)
    for load in loads[3:]:
        load.start()
    share.start()
    loads[3].wait()
    wb[f] = own[0, pl.ds(0, wch)].astype(BF)
    loads[4].wait()
    wc[pl.ds(pl.multiple_of(f * ks, 16), ks), :] = acc[
        pl.ds(3 * ks, ks), pl.ds(0, ff)
    ].astype(BF)
    loads[5].wait()
    wd[f, pl.ds(0, first_down)] = own[1, pl.ds(0, first_down)].astype(BF)
    if rest_down:
        loads[7].wait()
        wd[f, pl.ds(first_down, rest_down)] = own[2, pl.ds(0, rest_down)].astype(BF)
    loads[6].wait()
    share.wait_recv()

    tn = 256
    seq = SEQ
    pieces = rows // seq
    most = pieces - 1
    EARLY, LATE, ALL = (0, most * seq), (most * seq, seq), (0, rows)

    def relay_tokens(h):
        for k, o in numbered(h):
            twin_tokens(k, o).wait_recv()
            diag_tokens(k, o).start()

    def project(h, base, part):
        who = owners(h)
        start, count = part

        def unit(i, _):
            m = pl.ds(pl.multiple_of(i % 2 * MATE + base + start, 16), count)
            c = pl.ds(pl.multiple_of(i // 2 * wch, 128), wch)
            total = None
            for o in who:
                w = wa[pl.ds(pl.multiple_of(o * ks, 16), ks), c]
                term = dot(tok[m, block_of(o)], w)
                total = term if total is None else total + term
            if h == 0:
                acc[m, c] = total
            else:
                acc[m, c] += total
            return 0

        lax.fori_loop(0, 2 * 3, unit, 0)

    def project_near(h):
        project(h, OWN, ALL)

    def project_far(h, part):
        if part[0] == 0:
            for k, o in numbered(h):
                diag_tokens(k, o).wait_recv()
        project(h, TWIN, part)

    def mix(base, part):
        start, count = part
        tc = 128
        seqs = count // seq

        def unit(i, _):
            j = i % (2 * seqs)
            m = pl.ds(
                pl.multiple_of(base + j // seqs * MATE + start + j % seqs * seq, seq), seq
            )
            c = pl.multiple_of(i // (2 * seqs) * tc, tc)
            o = acc[m, pl.ds(c, tc)]
            p = (
                acc[m, pl.ds(pl.multiple_of(wch + c, tc), tc)]
                * acc[m, pl.ds(pl.multiple_of(2 * wch + c, tc), tc)]
            )
            place = lax.broadcasted_iota(jnp.int32, p.shape, 0)
            before = jnp.where(place > 0, pltpu.roll(p, 1, 0), 0.0)
            after = jnp.where(place < seq - 1, pltpu.roll(p, seq - 1, 0), 0.0)
            taps = taps_ref[:, pl.ds(pl.multiple_of(share_at + c, tc), tc)]
            conv = taps[0:1] * before + taps[1:2] * p + taps[2:3] * after
            mixed[m, pl.ds(c, tc)] = (o * conv).astype(BF)
            return 0

        lax.fori_loop(0, 2 * seqs * (wch // tc), unit, 0)

    def raise_part(size, start, x_base, acc_base, hs, new, final):
        who = [o for h in hs for o in owners(h)]
        tiles = ff // tn

        def unit(i, _):
            side = i % 2
            c = pl.ds(pl.multiple_of(i // 2 * tn, tn), tn)
            x_row = pl.multiple_of(x_base + side * MATE + start, 16)
            total = None
            for o in who:
                x = fst[pl.ds(x_row, size), block_of(o)]
                term = dot(x, wc[pl.ds(pl.multiple_of(o * ks, 16), ks), c])
                total = term if total is None else total + term
            span = pl.ds(pl.multiple_of(acc_base + side * rows + start, 16), size)
            if not new:
                total = total + acc[span, c]
            if final:
                total = jnp.maximum(total, 0.0)
                hid[pl.ds(x_row, size), c] = (total * total).astype(BF)
            else:
                acc[span, c] = total
            return 0

        lax.fori_loop(0, 2 * tiles, unit, 0)

    def raise_near(h):
        raise_part(rows, 0, OWN, 0, [h], h == 0, h == half)

    def raise_far(part):
        start, count = part
        for p in range(start // seq, (start + count) // seq):
            diag_first(p).wait_recv()
        raise_part(count, start, TWIN, both, range(half + 1), True, True)

    def far_block(kind, k, o, part):
        span = pl.ds(rows + part[0], part[1])
        return mate_copy((kind, k, part), psend.at[o, span], precv.at[o, span])

    def near_block(kind, k, o):
        span = pl.ds(0, rows)
        return mate_copy((kind, k), psend.at[o, span], precv.at[o, span])

    def across_block(kind, k, o, part):
        span = pl.ds(*part)
        return across_copy((kind, k, part), xsend.at[o, span], xrecv.at[o, span])

    used = []

    def far(kind, x_ref, w_ref, h, part):
        start, count = part
        for k, o in numbered(h):
            span = pl.ds(rows + start, count)
            psend[o, span] = dot(x_ref[pl.ds(DIAG + start, count), :], w_ref[o]).astype(BF)
            far_block(kind, k, o, part).start()
            own[o, span] = dot(x_ref[pl.ds(TWIN + start, count), :], w_ref[o])

    def pass_far(kind, h, part):
        start, count = part
        for k, o in numbered(h):
            far_block(kind, k, o, part).wait_recv()
            span = pl.ds(rows + start, count)
            xsend[o, pl.ds(start, count)] = (own[o, span] + precv[o, span].astype(F32)).astype(BF)
            across_block(kind, k, o, part).start()
            used.append((kind, k, o, part))

    def near(kind, x_ref, w_ref, h):
        span = pl.ds(0, rows)
        for k, o in numbered(h):
            psend[o, span] = dot(x_ref[pl.ds(MATE, rows), :], w_ref[o]).astype(BF)
            near_block(kind, k, o).start()
            own[o, span] = dot(x_ref[pl.ds(OWN, rows), :], w_ref[o])

    def mixout_far(h, part):
        far("mix", mixed, wb, h, part)

    def mixout_near(h):
        near("mix", mixed, wb, h)

    def lower_far(h, part):
        far("low", hid, wd, h, part)

    def lower_near(h):
        near("low", hid, wd, h)

    def mix_pass(h, part):
        pass_far("mix", h, part)

    def low_pass(h, part):
        pass_far("low", h, part)

    def norm(base_ref, gain_ref, dest_ref, start, count):
        tm = 32

        def unit(i, _):
            m = pl.multiple_of(start + i * tm, tm)
            parts = []
            for b in range(n):
                part = (
                    residual_scale
                    * base_ref[pl.ds(m, tm), pl.ds(b * nc, nc)].astype(F32)
                    + own[b, pl.ds(m, tm)]
                )
                for term in (precv, xrecv):
                    part = part + term[b, pl.ds(m, tm)].astype(F32)
                parts.append(part)
            total = parts[0]
            for b in range(1, n):
                total = total + parts[b]
            mean = jnp.sum(total, axis=-1, keepdims=True) / d
            parts = [p - mean for p in parts]
            square = parts[0] * parts[0]
            for b in range(1, n):
                square = square + parts[b] * parts[b]
            spread = jnp.sum(square, axis=-1, keepdims=True) / d
            scale = lax.rsqrt(spread + norm_epsilon)
            for b in range(n):
                cols = pl.ds(b * nc, nc)
                dest_ref[pl.ds(m, tm), cols] = (
                    parts[b] * scale * gain_ref[:, cols]
                ).astype(BF)
            return 0

        lax.fori_loop(0, count // tm, unit, 0)

    def near_first(p):
        return mate_copy(
            ("near", p), fst.at[pl.ds(p * seq, seq)], fst.at[pl.ds(MATE + p * seq, seq)]
        )

    def twin_first(p):
        return across_copy(
            ("twin", p), fst.at[pl.ds(p * seq, seq)], fst.at[pl.ds(TWIN + p * seq, seq)]
        )

    def diag_first(p):
        return mate_copy(
            ("diag", p),
            fst.at[pl.ds(TWIN + p * seq, seq)],
            fst.at[pl.ds(DIAG + p * seq, seq)],
        )

    def take_near_sums(kind):
        for k, o in every:
            near_block(kind, k, o).wait_recv()

    def make_first(part):
        for k, o in every:
            across_block("mix", k, o, part).wait_recv()
        start, count = part
        for p in range(start // seq, (start + count) // seq):
            norm(tok, norm1_ref, fst, p * seq, seq)
            twin_first(p).start()
            near_first(p).start()

    def take_near():
        for p in range(pieces):
            near_first(p).wait_recv()

    def relay_first(p):
        twin_first(p).wait_recv()
        diag_first(p).start()

    def free_sends():
        for k, o in every:
            near_block("mix", k, o).wait_send()
            for part in (EARLY, LATE):
                far_block("mix", k, o, part).wait_send()
                across_block("mix", k, o, part).wait_send()

    plan = {}

    def after(ti, h, which, *work):
        plan.setdefault((ti, h, which), []).extend(work)

    def do(function, *values):
        return lambda: function(*values)

    last = half - 1

    after(0, 1, 0, do(relay_tokens, 0), do(project_near, 0), do(project_far, 0, ALL))
    for h in range(1, last):
        after(0, h, 1, do(relay_tokens, h))
        after(0, h + 1, 0, do(project_near, h), do(project_far, h, ALL))
    after(0, last, 1, do(relay_tokens, last), do(relay_tokens, half))
    after(0, last, 1, do(project_near, last), do(project_far, last, ALL))
    after(0, half, 0, do(project_far, half, EARLY), do(mix, TWIN, EARLY))
    after(0, half, 0, do(mixout_far, 0, EARLY))
    after(1, 1, 0, do(project_far, half, LATE), do(mix_pass, 0, EARLY), do(mix, TWIN, LATE))
    after(1, 1, 1, do(mixout_far, 1, EARLY))
    after(1, 2, 0, do(mix_pass, 1, EARLY))
    after(1, 2, 1, do(mixout_far, 2, EARLY))
    after(1, 3, 0, do(mix_pass, 2, EARLY), do(project_near, half))
    for h in range(3, half):
        after(1, h, 1, do(mixout_far, h, EARLY))
        after(1, h + 1, 0, do(mix_pass, h, EARLY))
    after(1, half, 0, do(mixout_far, half, EARLY), do(mixout_far, 0, LATE))
    after(1, half, 0, do(mix_pass, half, EARLY))
    for h in range(1, half + 1):
        after(1, half, 0, do(mixout_far, h, LATE), do(mix_pass, h - 1, LATE))
    after(1, half, 0, do(mix, OWN, ALL), do(mix_pass, half, LATE))
    after(2, 1, 0, *[do(mixout_near, h) for h in range(half + 1)])
    after(2, 1, 1, do(take_near_sums, "mix"), do(make_first, EARLY))
    after(2, 2, 1, do(make_first, LATE), do(take_near))
    after(2, 2, 1, do(raise_near, 0), do(raise_near, 1))
    after(2, 3, 0, do(raise_near, 2), do(free_sends))
    for h in range(3, half):
        after(2, h, 1, do(raise_near, h))
    after(2, half, 0, do(relay_first, 0), do(raise_near, half))
    for p in range(1, most):
        after(3, 1, 0, do(relay_first, p))
    after(3, 1, 0, do(lower_near, 0), do(raise_far, EARLY))
    after(3, 1, 1, do(lower_far, 0, EARLY), do(lower_far, 1, EARLY), do(low_pass, 0, EARLY))
    after(3, 1, 1, do(low_pass, 1, EARLY), do(relay_first, most), do(raise_far, LATE))
    after(3, 2, 0, do(lower_far, 0, LATE), do(lower_far, 1, LATE))
    after(3, 2, 0, do(low_pass, 0, LATE), do(low_pass, 1, LATE), do(lower_near, 1))
    for h in range(2, half):
        after(3, h, 1, do(lower_far, h, ALL), do(low_pass, h, ALL), do(lower_near, h))
    after(3, half, 0, do(lower_far, half, ALL), do(low_pass, half, ALL), do(lower_near, half))

    for ti in range(4):
        for e in events(ti):
            event(*e)
            for work in plan.get(e, ()):
                work()

    take_near_sums("low")
    for kind, k, o, part in used:
        if kind == "low":
            across_block(kind, k, o, part).wait_recv()
    outs = []
    for p in range(pieces):
        span = pl.ds(p * seq, seq)
        norm(fst, norm2_ref, stage, p * seq, seq)
        outs.append(pltpu.make_async_copy(stage.at[span], out_ref.at[span], load_sem.at[p]))
        outs[p].start()

    for key, copy in mate_copies.items():
        if key[0] != "mix":
            copy.wait_send()
    for key, copy in across_copies.items():
        if key[0] != "mix":
            copy.wait_send()
    for key in copies:
        copies[key].wait_send()
    for copy in outs:
        copy.wait()


def fits(mesh, args):
    n = mesh.shape["fs"]
    rows, d = args[0].shape
    ks = args[1].shape[0]
    wch = args[1].shape[1] // 2
    nc = args[5].shape[1]
    ff = args[7].shape[1] // 2
    return (
        mesh.shape["rep"] == 2
        and mesh.shape["tp"] == 2
        and n % 2 == 0
        and n >= 8
        and ks % 128 == 0
        and nc == 256
        and wch % 128 == 0
        and ff % 256 == 0
        and wch <= 2 * rows
        and ff <= 4 * rows
        and ff <= 3 * wch
        and ks <= rows
        and rows % SEQ == 0
        and 2 * SEQ <= rows <= 8 * SEQ
    )


def fused(mesh, *args):
    (
        tokens,
        outer_weight,
        inner_weight,
        value_weight,
        conv_taps,
        mix_out,
        norm_first,
        up_weight,
        down_weight,
        norm_second,
    ) = args
    n = mesh.shape["fs"]
    rows, d = tokens.shape
    ks = outer_weight.shape[0]
    wch = outer_weight.shape[1] // 2
    ff = up_weight.shape[1] // 2
    nc = mix_out.shape[1]
    both = 2 * rows
    anywhere = pl.BlockSpec(memory_space=pl.ANY)
    vmem = pl.BlockSpec(memory_space=pltpu.VMEM)
    messages = 4 * (2 * n - 2)
    pairs = 1 + n + 6 * n + 2 * (rows // SEQ)
    crosses = n + 4 * n + rows // SEQ
    return pl.pallas_call(
        functools.partial(layer_kernel, n),
        out_shape=jax.ShapeDtypeStruct((rows, d), BF),
        in_specs=[
            anywhere,
            anywhere,
            anywhere,
            anywhere,
            vmem,
            anywhere,
            vmem,
            anywhere,
            anywhere,
            vmem,
        ],
        out_specs=anywhere,
        scratch_shapes=[
            pltpu.VMEM((n * ks, 3 * wch), BF),
            pltpu.VMEM((n, wch, nc), BF),
            pltpu.VMEM((n * ks, ff), BF),
            pltpu.VMEM((n, ff, nc), BF),
            pltpu.VMEM((2 * both, d), BF),
            pltpu.VMEM((2 * both, 3 * wch), F32),
            pltpu.VMEM((2 * both, wch), BF),
            pltpu.VMEM((n, both, nc), F32),
            pltpu.VMEM((n, both, nc), BF),
            pltpu.VMEM((n, both, nc), BF),
            pltpu.VMEM((n, rows, nc), BF),
            pltpu.VMEM((n, rows, nc), BF),
            pltpu.VMEM((2 * both, d), BF),
            pltpu.VMEM((2 * both, ff), BF),
            pltpu.VMEM((rows, d), BF),
            pltpu.SemaphoreType.DMA((8,)),
            pltpu.SemaphoreType.DMA((messages,)),
            pltpu.SemaphoreType.DMA((messages,)),
            pltpu.SemaphoreType.DMA((pairs,)),
            pltpu.SemaphoreType.DMA((pairs,)),
            pltpu.SemaphoreType.DMA((crosses,)),
            pltpu.SemaphoreType.DMA((crosses,)),
        ],
        compiler_params=pltpu.CompilerParams(
            collective_id=0, has_side_effects=True, vmem_limit_bytes=67043328
        ),
        name="layer",
    )(
        tokens,
        outer_weight,
        inner_weight,
        value_weight,
        conv_taps,
        mix_out,
        norm_first.reshape(1, d),
        up_weight,
        down_weight,
        norm_second.reshape(1, d),
    )


def solution(mesh):
    def body(*args):
        return fused(mesh, *args) if fits(mesh, args) else local(*args)

    return jax.shard_map(
        body,
        mesh=mesh,
        in_specs=(
            P(("rep", "fs", "tp"), None),
            P("fs", "tp"),
            P("fs", "tp"),
            P("fs", "tp"),
            P(None, "tp"),
            P("tp", "fs"),
            P(),
            P("fs", "tp"),
            P("tp", "fs"),
            P(),
        ),
        out_specs=P(("rep", "fs", "tp"), None),
        check_vma=False,
    )
```

```python
import functools

import jax
import jax.numpy as jnp
from jax import lax
from jax.experimental import pallas as pl
from jax.experimental.pallas import tpu as pltpu
from jax.sharding import PartitionSpec as P

SEQ = 128


residual_scale = 2.0**0.25
norm_epsilon = 1e-05


def layer_norm(values, scaling):
    center = values - jnp.mean(values, axis=-1, keepdims=True)
    spread = jnp.mean(center * center, axis=-1, keepdims=True)
    return center * lax.rsqrt(spread + norm_epsilon) * scaling


def short_conv(product, conv_taps):
    places = jnp.arange(product.shape[0], dtype=jnp.int32) % SEQ
    blank = jnp.zeros((1, product.shape[1]), jnp.float32)
    before = jnp.concatenate([blank, product[:-1]], axis=0)
    after = jnp.concatenate([product[1:], blank], axis=0)
    before = jnp.where((places > 0)[:, None], before, 0.0)
    after = jnp.where((places < SEQ - 1)[:, None], after, 0.0)
    return conv_taps[0] * before + conv_taps[1] * product + conv_taps[2] * after


def local(
    tokens,
    outer_weight,
    inner_weight,
    value_weight,
    conv_taps,
    mix_out,
    norm_first,
    up_weight,
    down_weight,
    norm_second,
):
    grouped = lax.all_gather(tokens, "tp", axis=0, tiled=True)
    outer_bf = outer_weight.astype(jnp.bfloat16)
    inner_bf = inner_weight.astype(jnp.bfloat16)
    value_bf = value_weight.astype(jnp.bfloat16)
    outer_full, inner_full, value_full = (
        lax.all_gather(outer_bf, "fs", axis=0, tiled=True),
        lax.all_gather(inner_bf, "fs", axis=0, tiled=True),
        lax.all_gather(value_bf, "fs", axis=0, tiled=True),
    )
    outer = jnp.dot(grouped, outer_full, preferred_element_type=jnp.float32)
    inner = jnp.dot(grouped, inner_full, preferred_element_type=jnp.float32)
    value = jnp.dot(grouped, value_full, preferred_element_type=jnp.float32)
    mixed = (outer * short_conv(inner * value, conv_taps)).astype(jnp.bfloat16)
    mixout_full = lax.all_gather(mix_out.astype(jnp.bfloat16), "fs", axis=1, tiled=True)
    selected = mixed
    mixing = lax.psum_scatter(
        jnp.dot(selected, mixout_full, preferred_element_type=jnp.float32).astype(jnp.bfloat16),
        "tp",
        scatter_dimension=0,
        tiled=True,
    ).astype(jnp.float32)
    first = layer_norm(residual_scale * tokens.astype(jnp.float32) + mixing, norm_first).astype(
        jnp.bfloat16
    )
    grouped_first = lax.all_gather(first, "tp", axis=0, tiled=True)
    upward_bf = up_weight.astype(jnp.bfloat16)
    upward_full = lax.all_gather(upward_bf, "fs", axis=0, tiled=True)
    raised = jnp.dot(grouped_first, upward_full, preferred_element_type=jnp.float32)
    raised = jax.nn.relu(raised)
    hidden = (raised * raised).astype(jnp.bfloat16)
    down_full = lax.all_gather(down_weight.astype(jnp.bfloat16), "fs", axis=1, tiled=True)
    selected = hidden
    lowered = lax.psum_scatter(
        jnp.dot(selected, down_full, preferred_element_type=jnp.float32).astype(jnp.bfloat16),
        "tp",
        scatter_dimension=0,
        tiled=True,
    ).astype(jnp.float32)
    return layer_norm(residual_scale * first.astype(jnp.float32) + lowered, norm_second).astype(
        jnp.bfloat16
    )


MESH = pl.DeviceIdType.MESH
BF = jnp.bfloat16
F32 = jnp.float32


def dot(a, b):
    return jnp.dot(a, b, preferred_element_type=F32)


def layer_kernel(
    n,
    tokens_hbm,
    outer_hbm,
    inner_hbm,
    value_hbm,
    taps_ref,
    mix_hbm,
    norm1_ref,
    up_hbm,
    down_hbm,
    norm2_ref,
    out_ref,
    wa,
    wb,
    wc,
    wd,
    tok,
    acc,
    mixed,
    own,
    psend,
    precv,
    xsend,
    xrecv,
    fst,
    hid,
    stats,
    load_sem,
    ring_send,
    ring_recv,
    tp_send,
    tp_recv,
    x_send,
    x_recv,
):
    half = n // 2
    r = lax.axis_index("rep")
    f = lax.axis_index("fs")
    t = lax.axis_index("tp")
    rows = tokens_hbm.shape[0]
    both = 2 * rows
    d = tokens_hbm.shape[1]
    ks = outer_hbm.shape[0]
    wch = wb.shape[1]
    ff = wc.shape[1]
    nc = wb.shape[2]
    OWN, TWIN, MATE, DIAG = 0, rows, 2 * rows, 3 * rows

    odd = f % 2
    pos = (1 - odd) * (f // 2) + odd * (n - 1 - f // 2)

    def at(place):
        p = (place + 2 * n) % n
        hi = p // half
        return (1 - hi) * (2 * p) + hi * (2 * (n - 1 - p) + 1)

    right = {"fs": at(pos + 1)}
    left = {"fs": at(pos - 1)}
    across = {"rep": 1 - r}
    mate = {"tp": 1 - t}

    def owners(h):
        if h == 0:
            return [f]
        if h == half:
            return [at(pos + half)]
        return [at(pos - h), at(pos + h)]

    def numbered(h):
        return [(0 if h == 0 else 2 * h - 1 + k, o) for k, o in enumerate(owners(h))]

    every = [item for h in range(half + 1) for item in numbered(h)]

    mine = pl.multiple_of(r * ff, 128)
    share_at = pl.multiple_of(r * wch, 128)
    first_down = min(ff, both)
    rest_down = ff - first_down
    loads = [
        pltpu.make_async_copy(
            src.at[:, pl.ds(share_at, wch)],
            acc.at[pl.ds(i * ks, ks), pl.ds(0, wch)],
            load_sem.at[i],
        )
        for i, src in enumerate((outer_hbm, inner_hbm, value_hbm))
    ]
    loads += [
        pltpu.make_async_copy(
            mix_hbm.at[pl.ds(share_at, wch)], own.at[0, pl.ds(0, wch)], load_sem.at[3]
        ),
        pltpu.make_async_copy(
            up_hbm.at[:, pl.ds(mine, ff)],
            acc.at[pl.ds(3 * ks, ks), pl.ds(0, ff)],
            load_sem.at[4],
        ),
        pltpu.make_async_copy(
            down_hbm.at[pl.ds(mine, first_down)],
            own.at[1, pl.ds(0, first_down)],
            load_sem.at[5],
        ),
        pltpu.make_async_copy(tokens_hbm, tok.at[pl.ds(0, rows)], load_sem.at[6]),
    ]
    if rest_down:
        loads.append(
            pltpu.make_async_copy(
                down_hbm.at[pl.ds(mine + first_down, rest_down)],
                own.at[2, pl.ds(0, rest_down)],
                load_sem.at[7],
            )
        )
    for load in loads[:3]:
        load.start()

    barrier = pltpu.get_barrier_semaphore()
    for device in (right, left, across, mate):
        pl.semaphore_signal(barrier, inc=1, device_id=device, device_id_type=MESH)
    pl.semaphore_wait(barrier, 4)

    def copier(device, send_sems, recv_sems):
        made, arrivals, groups = {}, {}, {}

        def copy(key, src, dst, group, arrival=None):
            if key not in made:
                place = arrival or key
                made[key] = pltpu.make_async_remote_copy(
                    src_ref=src,
                    dst_ref=dst,
                    send_sem=send_sems.at[groups.setdefault(group, len(groups))],
                    recv_sem=recv_sems.at[arrivals.setdefault(place, len(arrivals))],
                    device_id=device,
                    device_id_type=MESH,
                )
            return made[key]

        def whole(ref, group, arrival=None):
            return pltpu.make_async_remote_copy(
                src_ref=ref,
                dst_ref=ref,
                send_sem=send_sems.at[groups.get(group, 0)],
                recv_sem=recv_sems.at[arrivals.get(arrival, 0)],
                device_id=device,
                device_id_type=MESH,
            )

        return copy, whole

    mate_copy, mate_whole = copier(mate, tp_send, tp_recv)
    across_copy, across_whole = copier(across, x_send, x_recv)

    def piece(ti, which, owner):
        if ti == 0:
            u = ks // 2
            return wa.at[pl.ds(pl.multiple_of(owner * ks + which * u, 16), u)]
        if ti == 1:
            return wb.at[owner, pl.ds(which * (wch // 2), wch // 2)]
        if ti == 2:
            u = ks // 2
            return wc.at[pl.ds(pl.multiple_of(owner * ks + which * u, 16), u)]
        return wd.at[owner, pl.ds(which * (ff // 2), ff // 2)]

    per = 4 * half - 2
    index = {}
    for h in range(1, half + 1):
        for kind in ("Rq", "Rp", "Lq", "Lp"):
            if h == half and kind in ("Rp", "Lq"):
                continue
            index[kind, h] = len(index)

    copies = {}

    def message(ti, kind, h):
        key = (ti, kind, h)
        if key not in copies:
            which = int(kind[1] == "p")
            if kind[0] == "R":
                src, device = at(pos - (h - 1)), right
            else:
                src, device = at(pos + (h - 1)), left
            i = ti * per + index[kind, h]
            ref = piece(ti, which, src)
            copies[key] = pltpu.make_async_remote_copy(
                src_ref=ref,
                dst_ref=ref,
                send_sem=ring_send.at[ti],
                recv_sem=ring_recv.at[i],
                device_id=device,
                device_id_type=MESH,
            )
        return copies[key]

    def send(ti, kind, h):
        if ti < 4 and (kind, h) in index:
            message(ti, kind, h).start()

    def got(ti, kind, h):
        message(ti, kind, h).wait_recv()

    def event(ti, h, which):
        if which == 0:
            got(ti, "Rq", h)
            send(ti, "Rq", h + 1)
            if h == half:
                send(ti + 1, "Rp", 1)
            got(ti, "Lp", h)
            send(ti, "Lp", h + 1)
            if h == half:
                send(ti + 1, "Lq", 1)
        else:
            got(ti, "Rp", h)
            if h + 1 < half:
                send(ti, "Rp", h + 1)
            else:
                send(ti + 1, "Rq", 1)
            got(ti, "Lq", h)
            if h + 1 < half:
                send(ti, "Lq", h + 1)
            else:
                send(ti + 1, "Lp", 1)

    def events(ti):
        out = []
        for h in range(1, half + 1):
            out.append((ti, h, 0))
            if h < half:
                out.append((ti, h, 1))
        return out

    def block_of(o):
        return pl.ds(pl.multiple_of(o * ks, 128), ks)

    def twin_tokens(k, o):
        return across_copy(
            ("tok", k),
            tokens_hbm.at[:, block_of(o)],
            tok.at[pl.ds(TWIN, rows), block_of(o)],
            "tok",
        )

    def diag_tokens(k, o):
        return mate_copy(
            ("tok", k),
            tok.at[pl.ds(TWIN, rows), block_of(o)],
            tok.at[pl.ds(DIAG, rows), block_of(o)],
            "tok",
        )

    share = mate_copy("share", tokens_hbm, tok.at[pl.ds(MATE, rows)], "tok")
    for k, o in every:
        twin_tokens(k, o).start()
    for i in range(3):
        loads[i].wait()
        wa[pl.ds(pl.multiple_of(f * ks, 16), ks), pl.ds(i * wch, wch)] = acc[
            pl.ds(i * ks, ks), pl.ds(0, wch)
        ].astype(BF)
    send(0, "Rq", 1)
    send(0, "Lp", 1)
    send(0, "Rp", 1)
    send(0, "Lq", 1)
    for load in loads[3:]:
        load.start()
    share.start()
    loads[3].wait()
    wb[f] = own[0, pl.ds(0, wch)].astype(BF)
    loads[4].wait()
    wc[pl.ds(pl.multiple_of(f * ks, 16), ks), :] = acc[
        pl.ds(3 * ks, ks), pl.ds(0, ff)
    ].astype(BF)
    loads[5].wait()
    wd[f, pl.ds(0, first_down)] = own[1, pl.ds(0, first_down)].astype(BF)
    if rest_down:
        loads[7].wait()
        wd[f, pl.ds(first_down, rest_down)] = own[2, pl.ds(0, rest_down)].astype(BF)
    loads[6].wait()
    share.wait_recv()

    tn = 256
    seq = SEQ
    pieces = rows // seq
    most = pieces - 1
    EARLY, LATE, ALL = (0, most * seq), (most * seq, seq), (0, rows)

    def relay_tokens(h):
        for k, o in numbered(h):
            twin_tokens(k, o).wait_recv()
            diag_tokens(k, o).start()

    def project(h, base, part, sides=2):
        who = owners(h)
        start, count = part

        def unit(i, _):
            m = pl.ds(pl.multiple_of(i % sides * MATE + base + start, 16), count)
            c = pl.ds(pl.multiple_of(i // sides * wch, 128), wch)
            total = None
            for o in who:
                w = wa[pl.ds(pl.multiple_of(o * ks, 16), ks), c]
                term = dot(tok[m, block_of(o)], w)
                total = term if total is None else total + term
            if h == 0:
                acc[m, c] = total
            else:
                acc[m, c] += total
            return 0

        lax.fori_loop(0, sides * 3, unit, 0)

    def project_near(h):
        project(h, OWN, ALL)

    def take_diag_tokens(h):
        for k, o in numbered(h):
            diag_tokens(k, o).wait_recv()

    def project_far(h):
        take_diag_tokens(h)
        project(h, TWIN, ALL)

    def mix(base, part, sides=2):
        start, count = part
        tc = 128
        seqs = count // seq

        def unit(i, _):
            j = i % (sides * seqs)
            m = pl.ds(
                pl.multiple_of(base + j // seqs * MATE + start + j % seqs * seq, seq), seq
            )
            c = pl.multiple_of(i // (sides * seqs) * tc, tc)
            o = acc[m, pl.ds(c, tc)]
            p = (
                acc[m, pl.ds(pl.multiple_of(wch + c, tc), tc)]
                * acc[m, pl.ds(pl.multiple_of(2 * wch + c, tc), tc)]
            )
            place = lax.broadcasted_iota(jnp.int32, p.shape, 0)
            before = jnp.where(place > 0, pltpu.roll(p, 1, 0), 0.0)
            after = jnp.where(place < seq - 1, pltpu.roll(p, seq - 1, 0), 0.0)
            taps = taps_ref[:, pl.ds(pl.multiple_of(share_at + c, tc), tc)]
            conv = taps[0:1] * before + taps[1:2] * p + taps[2:3] * after
            mixed[m, pl.ds(c, tc)] = (o * conv).astype(BF)
            return 0

        lax.fori_loop(0, sides * seqs * (wch // tc), unit, 0)

    def raise_part(size, start, x_base, acc_base, hs, new, final):
        who = [o for h in hs for o in owners(h)]
        tiles = ff // tn

        def unit(i, _):
            side = i % 2
            c = pl.ds(pl.multiple_of(i // 2 * tn, tn), tn)
            x_row = pl.multiple_of(x_base + side * MATE + start, 16)
            total = None
            for o in who:
                x = fst[pl.ds(x_row, size), block_of(o)]
                term = dot(x, wc[pl.ds(pl.multiple_of(o * ks, 16), ks), c])
                total = term if total is None else total + term
            span = pl.ds(pl.multiple_of(acc_base + side * rows + start, 16), size)
            if not new:
                total = total + acc[span, c]
            if final:
                total = jnp.maximum(total, 0.0)
                hid[pl.ds(x_row, size), c] = (total * total).astype(BF)
            else:
                acc[span, c] = total
            return 0

        lax.fori_loop(0, 2 * tiles, unit, 0)

    def raise_near(h):
        raise_part(rows, 0, OWN, 0, [h], h == 0, h == half)

    def raise_far(part):
        start, count = part
        for p in range(start // seq, (start + count) // seq):
            diag_first(p).wait_recv()
        raise_part(count, start, TWIN, both, range(half + 1), True, True)

    def far_block(kind, k, o, part):
        span = pl.ds(rows + part[0], part[1])
        return mate_copy((kind, k, part), psend.at[o, span], precv.at[o, span], kind)

    def near_block(kind, k, o):
        span = pl.ds(0, rows)
        return mate_copy((kind, k), psend.at[o, span], precv.at[o, span], kind, (kind, "near"))

    def across_block(kind, k, o, part):
        span = pl.ds(*part)
        arrival = ("mix", part) if kind == "mix" else None
        return across_copy((kind, k, part), xsend.at[o, span], xrecv.at[o, span], kind, arrival)

    lowered = {h: [EARLY, LATE] if h < 2 else [ALL] for h in range(half + 1)}

    def far(kind, x_ref, w_ref, h, part, sides=(DIAG, TWIN)):
        start, count = part
        for k, o in numbered(h):
            span = pl.ds(rows + start, count)
            if DIAG in sides:
                psend[o, span] = dot(x_ref[pl.ds(DIAG + start, count), :], w_ref[o]).astype(BF)
                far_block(kind, k, o, part).start()
            if TWIN in sides:
                own[o, span] = dot(x_ref[pl.ds(TWIN + start, count), :], w_ref[o])

    def pass_far(kind, h, part):
        start, count = part
        for k, o in numbered(h):
            far_block(kind, k, o, part).wait_recv()
            span = pl.ds(rows + start, count)
            xsend[o, pl.ds(start, count)] = (own[o, span] + precv[o, span].astype(F32)).astype(BF)
            across_block(kind, k, o, part).start()

    def near(kind, x_ref, w_ref, h):
        span = pl.ds(0, rows)
        for k, o in numbered(h):
            psend[o, span] = dot(x_ref[pl.ds(MATE, rows), :], w_ref[o]).astype(BF)
            near_block(kind, k, o).start()
            own[o, span] = dot(x_ref[pl.ds(OWN, rows), :], w_ref[o])

    def mixout_far(h, part, sides=(DIAG, TWIN)):
        far("mix", mixed, wb, h, part, sides)

    def mixout_near(h):
        near("mix", mixed, wb, h)

    def lower_far(h, part):
        far("low", hid, wd, h, part)

    def lower_near(h):
        near("low", hid, wd, h)

    def mix_pass(h, part):
        pass_far("mix", h, part)

    def low_pass(h, part):
        pass_far("low", h, part)

    def norm(base_ref, gain_ref, dest_ref, start, count):
        tm = 32

        def unit(i, _):
            m = pl.multiple_of(start + i * tm, tm)
            parts = []
            for b in range(n):
                part = (
                    residual_scale
                    * base_ref[pl.ds(m, tm), pl.ds(b * nc, nc)].astype(F32)
                    + own[b, pl.ds(m, tm)]
                )
                for term in (precv, xrecv):
                    part = part + term[b, pl.ds(m, tm)].astype(F32)
                parts.append(part)
            total = parts[0]
            for b in range(1, n):
                total = total + parts[b]
            mean = jnp.sum(total, axis=-1, keepdims=True) / d
            parts = [p - mean for p in parts]
            square = parts[0] * parts[0]
            for b in range(1, n):
                square = square + parts[b] * parts[b]
            spread = jnp.sum(square, axis=-1, keepdims=True) / d
            scale = lax.rsqrt(spread + norm_epsilon)
            for b in range(n):
                cols = pl.ds(b * nc, nc)
                dest_ref[pl.ds(m, tm), cols] = (
                    parts[b] * scale * gain_ref[:, cols]
                ).astype(BF)
            return 0

        lax.fori_loop(0, count // tm, unit, 0)

    tm = SEQ
    C, D, Q, S = range(4)

    def low_parts(h):
        return [(k, o, p) for k, o in numbered(h) for p in lowered[h]]

    def add_near():
        def unit(i, _):
            m = pl.ds(pl.multiple_of(i * 32, 32), 32)
            for b in range(n):
                own[b, m] = (
                    residual_scale * fst[m, pl.ds(b * nc, nc)].astype(F32)
                    + own[b, m]
                    + precv[b, m].astype(F32)
                )
            return 0

        lax.fori_loop(0, rows // 32, unit, 0)

    def add_across(h):
        for k, o, part in low_parts(h):
            across_block("low", k, o, part).wait_recv()
        for k, o in numbered(h):

            def unit(i, _):
                m = pl.ds(pl.multiple_of(i * tm, tm), tm)
                x = own[o, m] + xrecv[o, m].astype(F32)
                own[o, m] = x
                lanes = x[:, :128] + x[:, 128:]
                stats[S, m] = lanes if k == 0 else stats[S, m] + lanes
                return 0

            lax.fori_loop(0, rows // tm, unit, 0)

    def center():
        but_last = [o for h in range(half) for o in owners(h)]

        def unit(i, _):
            m = pl.ds(pl.multiple_of(i * tm, tm), tm)
            c = jnp.sum(stats[S, m], axis=-1, keepdims=True) / ((n - 1) * nc)
            shift = square = None
            for o in but_last:
                x = own[o, m] - c
                y = x * x
                lanes, squares = x[:, :128] + x[:, 128:], y[:, :128] + y[:, 128:]
                shift = lanes if shift is None else shift + lanes
                square = squares if square is None else square + squares
            stats[C, m] = jnp.broadcast_to(c, (tm, 128))
            stats[D, m] = shift
            stats[Q, m] = square
            return 0

        lax.fori_loop(0, rows // tm, unit, 0)

    def finish():
        for k, o, part in low_parts(half):
            across_block("low", k, o, part).wait_recv()
        tail = owners(half)[0]

        def measure(i, _):
            m = pl.ds(pl.multiple_of(i * tm, tm), tm)
            value = own[tail, m] + xrecv[tail, m].astype(F32)
            own[tail, m] = value
            c = stats[C, m]
            x, y = value[:, :128] - c, value[:, 128:] - c
            shift = jnp.sum(stats[D, m] + (x + y), axis=-1, keepdims=True) / d
            square = jnp.sum(stats[Q, m] + (x * x + y * y), axis=-1, keepdims=True) / d
            spread = jnp.maximum(square - shift * shift, 0.0)
            stats[C, m] = c + shift
            stats[S, m] = jnp.broadcast_to(lax.rsqrt(spread + norm_epsilon), (tm, 128))
            return 0

        lax.fori_loop(0, rows // tm, measure, 0)

        def apply(i, _):
            m = pl.ds(pl.multiple_of(i * 32, 32), 32)
            mean, scale = stats[C, m], stats[S, m]
            for b in range(n):
                for half_block in range(nc // 128):
                    part = pl.ds(half_block * 128, 128)
                    cols = pl.ds(b * nc + half_block * 128, 128)
                    out_ref[m, cols] = (
                        (own[b, m, part] - mean) * scale * norm2_ref[:, cols]
                    ).astype(BF)
            return 0

        lax.fori_loop(0, rows // 32, apply, 0)

    def near_first(p):
        return mate_copy(
            ("near", p),
            fst.at[pl.ds(p * seq, seq)],
            fst.at[pl.ds(MATE + p * seq, seq)],
            "near",
            "near",
        )

    def twin_first(p):
        return across_copy(
            ("twin", p),
            fst.at[pl.ds(p * seq, seq)],
            fst.at[pl.ds(TWIN + p * seq, seq)],
            "first",
        )

    def diag_first(p):
        return mate_copy(
            ("diag", p),
            fst.at[pl.ds(TWIN + p * seq, seq)],
            fst.at[pl.ds(DIAG + p * seq, seq)],
            "diag",
        )

    def take_near_sums(kind):
        mate_whole(precv.at[:, pl.ds(0, rows)], kind, (kind, "near")).wait_recv()

    def make_first(part):
        across_whole(xrecv.at[:, pl.ds(*part)], "mix", ("mix", part)).wait_recv()
        start, count = part
        for p in range(start // seq, (start + count) // seq):
            norm(tok, norm1_ref, fst, p * seq, seq)
            twin_first(p).start()
            near_first(p).start()

    def take_near():
        mate_whole(fst.at[pl.ds(MATE, rows)], "near", "near").wait_recv()

    def relay_first(p):
        twin_first(p).wait_recv()
        diag_first(p).start()

    def free_sends():
        mate_whole(psend, "mix").wait_send()
        across_whole(xsend, "mix").wait_send()

    plan = {}

    def after(ti, h, which, *work):
        plan.setdefault((ti, h, which), []).extend(work)

    def do(function, *values):
        return lambda: function(*values)

    last = half - 1

    after(0, 1, 0, do(relay_tokens, 0), do(project_near, 0), do(project_far, 0))
    for h in range(1, last):
        after(0, h, 1, do(relay_tokens, h))
        after(0, h + 1, 0, do(project_near, h), do(project_far, h))
    after(0, last, 1, do(relay_tokens, last), do(relay_tokens, half))
    after(0, last, 1, do(project_near, last), do(project_far, last))
    after(0, half, 0, do(take_diag_tokens, half))
    for side in (DIAG, TWIN):
        after(0, half, 0, do(project, half, side, EARLY, 1), do(mix, side, EARLY, 1))
        after(0, half, 0, do(mixout_far, 0, EARLY, (side,)))
    after(0, half, 0, do(mix_pass, 0, EARLY))
    after(1, 1, 0, do(project, half, TWIN, LATE), do(mix, TWIN, LATE), do(mixout_far, 0, LATE))
    after(1, 1, 1, do(mixout_far, 1, EARLY), do(mix_pass, 0, LATE))
    after(1, 2, 0, do(mix_pass, 1, EARLY))
    after(1, 2, 1, do(mixout_far, 2, EARLY))
    after(1, 3, 0, do(mix_pass, 2, EARLY), do(project_near, half))
    for h in range(3, half):
        after(1, h, 1, do(mixout_far, h, EARLY))
        after(1, h + 1, 0, do(mix_pass, h, EARLY))
    after(1, half, 0, do(mixout_far, half, EARLY), do(mixout_far, 1, LATE))
    after(1, half, 0, do(mix_pass, half, EARLY))
    for h in range(2, half + 1):
        after(1, half, 0, do(mixout_far, h, LATE), do(mix_pass, h - 1, LATE))
    after(1, half, 0, do(mix, OWN, ALL), do(mix_pass, half, LATE))
    after(2, 1, 0, *[do(mixout_near, h) for h in range(half + 1)])
    after(2, 1, 1, do(take_near_sums, "mix"), do(make_first, EARLY))
    after(2, 2, 1, do(make_first, LATE), do(take_near))
    after(2, 2, 1, do(raise_near, 0), do(raise_near, 1))
    after(2, 3, 0, do(raise_near, 2), do(free_sends))
    for h in range(3, half):
        after(2, h, 1, do(raise_near, h))
    after(2, half, 0, do(relay_first, 0), do(raise_near, half))
    for p in range(1, most):
        after(3, 1, 0, do(relay_first, p))
    after(3, 1, 0, do(lower_near, 0), do(raise_far, EARLY))
    after(3, 1, 1, do(lower_far, 0, EARLY), do(lower_far, 1, EARLY), do(low_pass, 0, EARLY))
    after(3, 1, 1, do(low_pass, 1, EARLY), do(relay_first, most), do(raise_far, LATE))
    after(3, 2, 0, do(lower_far, 0, LATE), do(lower_far, 1, LATE))
    after(3, 2, 0, do(low_pass, 0, LATE), do(low_pass, 1, LATE), do(lower_near, 1))
    for h in range(2, half):
        after(3, h, 1, do(lower_far, h, ALL), do(low_pass, h, ALL), do(lower_near, h))
    after(3, half, 0, do(lower_far, half, ALL), do(low_pass, half, ALL), do(lower_near, half))

    for ti in range(4):
        for e in events(ti):
            event(*e)
            for work in plan.get(e, ()):
                work()

    take_near_sums("low")
    add_near()
    for h in range(half):
        add_across(h)
    center()
    finish()

    mate_whole(tok.at[pl.ds(0, both)], "tok").wait_send()
    for group in ("near", "diag"):
        mate_whole(fst.at[pl.ds(0, rows)], group).wait_send()
    mate_whole(psend, "low").wait_send()
    across_whole(tok.at[pl.ds(0, rows)], "tok").wait_send()
    across_whole(fst.at[pl.ds(0, rows)], "first").wait_send()
    across_whole(xsend, "low").wait_send()
    for ti, ref in enumerate(
        (
            wa.at[pl.ds(0, (n - 1) * ks)],
            wb.at[pl.ds(0, n - 1)],
            wc.at[pl.ds(0, (n - 1) * ks)],
            wd.at[pl.ds(0, n - 1)],
        )
    ):
        pltpu.make_async_remote_copy(
            src_ref=ref,
            dst_ref=ref,
            send_sem=ring_send.at[ti],
            recv_sem=ring_recv.at[0],
            device_id=right,
            device_id_type=MESH,
        ).wait_send()


def fits(mesh, args):
    n = mesh.shape["fs"]
    rows, d = args[0].shape
    ks = args[1].shape[0]
    wch = args[1].shape[1] // 2
    nc = args[5].shape[1]
    ff = args[7].shape[1] // 2
    return (
        mesh.shape["rep"] == 2
        and mesh.shape["tp"] == 2
        and n % 2 == 0
        and n >= 8
        and ks % 128 == 0
        and nc == 256
        and wch % 128 == 0
        and ff % 256 == 0
        and wch <= 2 * rows
        and ff <= 4 * rows
        and ff <= 3 * wch
        and ks <= rows
        and rows % SEQ == 0
        and 2 * SEQ <= rows <= 8 * SEQ
    )


def fused(mesh, *args):
    (
        tokens,
        outer_weight,
        inner_weight,
        value_weight,
        conv_taps,
        mix_out,
        norm_first,
        up_weight,
        down_weight,
        norm_second,
    ) = args
    n = mesh.shape["fs"]
    rows, d = tokens.shape
    ks = outer_weight.shape[0]
    wch = outer_weight.shape[1] // 2
    ff = up_weight.shape[1] // 2
    nc = mix_out.shape[1]
    both = 2 * rows
    anywhere = pl.BlockSpec(memory_space=pl.ANY)
    vmem = pl.BlockSpec(memory_space=pltpu.VMEM)
    messages = 4 * (2 * n - 2)
    pairs = 4 * n + 7 + rows // SEQ
    crosses = 2 + n + n + 3 + rows // SEQ
    return pl.pallas_call(
        functools.partial(layer_kernel, n),
        out_shape=pltpu.VMEM((rows, d), BF),
        in_specs=[
            anywhere,
            anywhere,
            anywhere,
            anywhere,
            vmem,
            anywhere,
            vmem,
            anywhere,
            anywhere,
            vmem,
        ],
        out_specs=vmem,
        scratch_shapes=[
            pltpu.VMEM((n * ks, 3 * wch), BF),
            pltpu.VMEM((n, wch, nc), BF),
            pltpu.VMEM((n * ks, ff), BF),
            pltpu.VMEM((n, ff, nc), BF),
            pltpu.VMEM((2 * both, d), BF),
            pltpu.VMEM((2 * both, 3 * wch), F32),
            pltpu.VMEM((2 * both, wch), BF),
            pltpu.VMEM((n, both, nc), F32),
            pltpu.VMEM((n, both, nc), BF),
            pltpu.VMEM((n, both, nc), BF),
            pltpu.VMEM((n, rows, nc), BF),
            pltpu.VMEM((n, rows, nc), BF),
            pltpu.VMEM((2 * both, d), BF),
            pltpu.VMEM((2 * both, ff), BF),
            pltpu.VMEM((4, rows, 128), F32),
            pltpu.SemaphoreType.DMA((8,)),
            pltpu.SemaphoreType.DMA((4,)),
            pltpu.SemaphoreType.DMA((messages,)),
            pltpu.SemaphoreType.DMA((5,)),
            pltpu.SemaphoreType.DMA((pairs,)),
            pltpu.SemaphoreType.DMA((4,)),
            pltpu.SemaphoreType.DMA((crosses,)),
        ],
        compiler_params=pltpu.CompilerParams(
            collective_id=0, has_side_effects=True, vmem_limit_bytes=62 * 2**20
        ),
        name="layer",
    )(
        tokens,
        outer_weight,
        inner_weight,
        value_weight,
        conv_taps,
        mix_out,
        norm_first.reshape(1, d),
        up_weight,
        down_weight,
        norm_second.reshape(1, d),
    )


def solution(mesh):
    def body(*args):
        return fused(mesh, *args) if fits(mesh, args) else local(*args)

    return jax.shard_map(
        body,
        mesh=mesh,
        in_specs=(
            P(("rep", "fs", "tp"), None),
            P("fs", "tp"),
            P("fs", "tp"),
            P("fs", "tp"),
            P(None, "tp"),
            P("tp", "fs"),
            P(),
            P("fs", "tp"),
            P("tp", "fs"),
            P(),
        ),
        out_specs=P(("rep", "fs", "tp"), None),
        check_vma=False,
    )
```

```python
import functools

import jax
import jax.numpy as jnp
from jax import lax
from jax.experimental import pallas as pl
from jax.experimental.pallas import tpu as pltpu
from jax.sharding import PartitionSpec as P

SEQ = 128


residual_scale = 2.0**0.25
norm_epsilon = 1e-05


def layer_norm(values, scaling):
    center = values - jnp.mean(values, axis=-1, keepdims=True)
    spread = jnp.mean(center * center, axis=-1, keepdims=True)
    return center * lax.rsqrt(spread + norm_epsilon) * scaling


def short_conv(product, conv_taps):
    places = jnp.arange(product.shape[0], dtype=jnp.int32) % SEQ
    blank = jnp.zeros((1, product.shape[1]), jnp.float32)
    before = jnp.concatenate([blank, product[:-1]], axis=0)
    after = jnp.concatenate([product[1:], blank], axis=0)
    before = jnp.where((places > 0)[:, None], before, 0.0)
    after = jnp.where((places < SEQ - 1)[:, None], after, 0.0)
    return conv_taps[0] * before + conv_taps[1] * product + conv_taps[2] * after


def local(
    tokens,
    outer_weight,
    inner_weight,
    value_weight,
    conv_taps,
    mix_out,
    norm_first,
    up_weight,
    down_weight,
    norm_second,
):
    grouped = lax.all_gather(tokens, "tp", axis=0, tiled=True)
    outer_bf = outer_weight.astype(jnp.bfloat16)
    inner_bf = inner_weight.astype(jnp.bfloat16)
    value_bf = value_weight.astype(jnp.bfloat16)
    outer_full, inner_full, value_full = (
        lax.all_gather(outer_bf, "fs", axis=0, tiled=True),
        lax.all_gather(inner_bf, "fs", axis=0, tiled=True),
        lax.all_gather(value_bf, "fs", axis=0, tiled=True),
    )
    outer = jnp.dot(grouped, outer_full, preferred_element_type=jnp.float32)
    inner = jnp.dot(grouped, inner_full, preferred_element_type=jnp.float32)
    value = jnp.dot(grouped, value_full, preferred_element_type=jnp.float32)
    mixed = (outer * short_conv(inner * value, conv_taps)).astype(jnp.bfloat16)
    mixout_full = lax.all_gather(mix_out.astype(jnp.bfloat16), "fs", axis=1, tiled=True)
    selected = mixed
    mixing = lax.psum_scatter(
        jnp.dot(selected, mixout_full, preferred_element_type=jnp.float32).astype(jnp.bfloat16),
        "tp",
        scatter_dimension=0,
        tiled=True,
    ).astype(jnp.float32)
    first = layer_norm(residual_scale * tokens.astype(jnp.float32) + mixing, norm_first).astype(
        jnp.bfloat16
    )
    grouped_first = lax.all_gather(first, "tp", axis=0, tiled=True)
    upward_bf = up_weight.astype(jnp.bfloat16)
    upward_full = lax.all_gather(upward_bf, "fs", axis=0, tiled=True)
    raised = jnp.dot(grouped_first, upward_full, preferred_element_type=jnp.float32)
    raised = jax.nn.relu(raised)
    hidden = (raised * raised).astype(jnp.bfloat16)
    down_full = lax.all_gather(down_weight.astype(jnp.bfloat16), "fs", axis=1, tiled=True)
    selected = hidden
    lowered = lax.psum_scatter(
        jnp.dot(selected, down_full, preferred_element_type=jnp.float32).astype(jnp.bfloat16),
        "tp",
        scatter_dimension=0,
        tiled=True,
    ).astype(jnp.float32)
    return layer_norm(residual_scale * first.astype(jnp.float32) + lowered, norm_second).astype(
        jnp.bfloat16
    )


MESH = pl.DeviceIdType.MESH
BF = jnp.bfloat16
F32 = jnp.float32


def dot(a, b):
    return jnp.dot(a, b, preferred_element_type=F32)


def layer_kernel(
    n,
    tokens_hbm,
    outer_hbm,
    inner_hbm,
    value_hbm,
    taps_ref,
    mix_hbm,
    norm1_ref,
    up_hbm,
    down_hbm,
    norm2_ref,
    out_ref,
    wa,
    wb,
    wc,
    wd,
    tok,
    acc,
    mixed,
    own,
    psend,
    precv,
    xsend,
    xrecv,
    fst,
    hid,
    stats,
    load_sem,
    ring_send,
    ring_recv,
    tp_send,
    tp_recv,
    x_send,
    x_recv,
):
    half = n // 2
    r = lax.axis_index("rep")
    f = lax.axis_index("fs")
    t = lax.axis_index("tp")
    rows = tokens_hbm.shape[0]
    both = 2 * rows
    d = tokens_hbm.shape[1]
    ks = outer_hbm.shape[0]
    wch = wb.shape[1] // 2
    ff = wc.shape[1]
    nc = wb.shape[2]
    OWN, TWIN, MATE, DIAG = 0, rows, 2 * rows, 3 * rows

    odd = f % 2
    pos = (1 - odd) * (f // 2) + odd * (n - 1 - f // 2)

    def at(place):
        p = (place + 2 * n) % n
        hi = p // half
        return (1 - hi) * (2 * p) + hi * (2 * (n - 1 - p) + 1)

    right = {"fs": at(pos + 1)}
    left = {"fs": at(pos - 1)}
    across = {"rep": 1 - r}
    mate = {"tp": 1 - t}

    def owners(h):
        if h == 0:
            return [f]
        if h == half:
            return [at(pos + half)]
        return [at(pos - h), at(pos + h)]

    def numbered(h):
        return [(0 if h == 0 else 2 * h - 1 + k, o) for k, o in enumerate(owners(h))]

    every = [item for h in range(half + 1) for item in numbered(h)]

    units = [((f, 0), (f, 1))]
    for h in range(1, half):
        a, b = owners(h)
        units += [((a, 0), (b, 1)), ((a, 1), (b, 0))]
    units.append(tuple((o, j) for o in owners(half) for j in range(2)))
    lane = nc // 2

    def columns(o, j):
        return pl.ds(pl.multiple_of(o * nc + j * lane, lane), lane)

    mine = pl.multiple_of(r * ff, 128)
    share_at = pl.multiple_of(r * wch, 128)
    first_down = min(ff, both)
    rest_down = ff - first_down
    loads = [
        pltpu.make_async_copy(
            src.at[:, pl.ds(share_at, wch)],
            acc.at[pl.ds(i * ks, ks), pl.ds(0, wch)],
            load_sem.at[i],
        )
        for i, src in enumerate((outer_hbm, inner_hbm, value_hbm))
    ]
    loads += [
        pltpu.make_async_copy(
            mix_hbm, own.at[0, pl.ds(0, 2 * wch)], load_sem.at[3]
        ),
        pltpu.make_async_copy(
            up_hbm.at[:, pl.ds(mine, ff)],
            acc.at[pl.ds(3 * ks, ks), pl.ds(0, ff)],
            load_sem.at[4],
        ),
        pltpu.make_async_copy(
            down_hbm.at[pl.ds(mine, first_down)],
            own.at[1, pl.ds(0, first_down)],
            load_sem.at[5],
        ),
        pltpu.make_async_copy(tokens_hbm, tok.at[pl.ds(0, rows)], load_sem.at[6]),
    ]
    if rest_down:
        loads.append(
            pltpu.make_async_copy(
                down_hbm.at[pl.ds(mine + first_down, rest_down)],
                own.at[2, pl.ds(0, rest_down)],
                load_sem.at[7],
            )
        )
    for i in (3, 0, 1, 2):
        loads[i].start()

    barrier = pltpu.get_barrier_semaphore()
    for device in (right, left, across, mate):
        pl.semaphore_signal(barrier, inc=1, device_id=device, device_id_type=MESH)
    pl.semaphore_wait(barrier, 4)

    def copier(device, send_sems, recv_sems):
        made, arrivals, groups = {}, {}, {}

        def copy(key, src, dst, group, arrival=None):
            if key not in made:
                place = arrival or key
                made[key] = pltpu.make_async_remote_copy(
                    src_ref=src,
                    dst_ref=dst,
                    send_sem=send_sems.at[groups.setdefault(group, len(groups))],
                    recv_sem=recv_sems.at[arrivals.setdefault(place, len(arrivals))],
                    device_id=device,
                    device_id_type=MESH,
                )
            return made[key]

        def whole(ref, group, arrival=None):
            return pltpu.make_async_remote_copy(
                src_ref=ref,
                dst_ref=ref,
                send_sem=send_sems.at[groups.get(group, 0)],
                recv_sem=recv_sems.at[arrivals.get(arrival, 0)],
                device_id=device,
                device_id_type=MESH,
            )

        return copy, whole

    mate_copy, mate_whole = copier(mate, tp_send, tp_recv)
    across_copy, across_whole = copier(across, x_send, x_recv)

    def piece(ti, which, owner):
        if ti == 0:
            u = wch // 2
            return wb.at[owner, pl.ds(pl.multiple_of(share_at + which * u, 16), u)]
        u = ks // 2
        if ti < 3:
            return (wa, wc)[ti - 1].at[pl.ds(pl.multiple_of(owner * ks + which * u, 16), u)]
        return wd.at[owner, which]

    per = 4 * half - 2
    index = {}
    for h in range(1, half + 1):
        for kind in ("Rq", "Rp", "Lq", "Lp"):
            if h == half and kind in ("Rp", "Lq"):
                continue
            index[kind, h] = len(index)

    copies = {}

    def message(ti, kind, h):
        key = (ti, kind, h)
        if key not in copies:
            which = int(kind[1] == "p")
            if kind[0] == "R":
                src, device = at(pos - (h - 1)), right
            else:
                src, device = at(pos + (h - 1)), left
            i = ti * per + index[kind, h]
            ref = piece(ti, which, src)
            copies[key] = pltpu.make_async_remote_copy(
                src_ref=ref,
                dst_ref=ref,
                send_sem=ring_send.at[ti],
                recv_sem=ring_recv.at[i],
                device_id=device,
                device_id_type=MESH,
            )
        return copies[key]

    def send(ti, kind, h):
        if ti < 4 and (kind, h) in index:
            message(ti, kind, h).start()

    def got(ti, kind, h):
        message(ti, kind, h).wait_recv()

    def event(ti, h, which):
        if which == 0:
            got(ti, "Rq", h)
            send(ti, "Rq", h + 1)
            if h == half:
                send(ti + 1, "Rp", 1)
            got(ti, "Lp", h)
            send(ti, "Lp", h + 1)
            if h == half:
                send(ti + 1, "Lq", 1)
        else:
            got(ti, "Rp", h)
            if h + 1 < half:
                send(ti, "Rp", h + 1)
            else:
                send(ti + 1, "Rq", 1)
            got(ti, "Lq", h)
            if h + 1 < half:
                send(ti, "Lq", h + 1)
            else:
                send(ti + 1, "Lp", 1)

    def events(ti):
        out = []
        for h in range(1, half + 1):
            out.append((ti, h, 0))
            if h < half:
                out.append((ti, h, 1))
        return out

    def block_of(o):
        return pl.ds(pl.multiple_of(o * ks, 128), ks)

    def twin_tokens(k, o):
        return across_copy(
            ("tok", k),
            tokens_hbm.at[:, block_of(o)],
            tok.at[pl.ds(TWIN, rows), block_of(o)],
            "tok",
        )

    def diag_tokens(k, o):
        return mate_copy(
            ("tok", k),
            tok.at[pl.ds(TWIN, rows), block_of(o)],
            tok.at[pl.ds(DIAG, rows), block_of(o)],
            "tok",
        )

    share = mate_copy("share", tokens_hbm, tok.at[pl.ds(MATE, rows)], "tok")
    for k, o in every:
        twin_tokens(k, o).start()
    loads[3].wait()
    wb[f] = own[0, pl.ds(0, 2 * wch)].astype(BF)
    send(0, "Rq", 1)
    send(0, "Lp", 1)
    send(0, "Rp", 1)
    send(0, "Lq", 1)
    for load in loads[4:]:
        load.start()
    share.start()
    for i in range(3):
        loads[i].wait()
        wa[pl.ds(pl.multiple_of(f * ks, 16), ks), pl.ds(i * wch, wch)] = acc[
            pl.ds(i * ks, ks), pl.ds(0, wch)
        ].astype(BF)
    loads[4].wait()
    wc[pl.ds(pl.multiple_of(f * ks, 16), ks), :] = acc[
        pl.ds(3 * ks, ks), pl.ds(0, ff)
    ].astype(BF)
    loads[5].wait()
    for j in range(2):
        wd[f, j, pl.ds(0, first_down)] = own[
            1, pl.ds(0, first_down), pl.ds(j * lane, lane)
        ].astype(BF)
    if rest_down:
        loads[7].wait()
        for j in range(2):
            wd[f, j, pl.ds(first_down, rest_down)] = own[
                2, pl.ds(0, rest_down), pl.ds(j * lane, lane)
            ].astype(BF)
    loads[6].wait()
    share.wait_recv()

    tn = 256
    seq = SEQ
    pieces = rows // seq
    most = pieces - 1
    EARLY, LATE, ALL = (0, most * seq), (most * seq, seq), (0, rows)

    def cross_wb(h):
        for k, o in numbered(h):
            ref = wb.at[o, pl.ds(share_at, wch)]
            across_copy(("wb", k), ref, ref, "wb", "wb").start()

    def relay_tokens(h):
        for k, o in numbered(h):
            twin_tokens(k, o).wait_recv()
            diag_tokens(k, o).start()

    def project(h, base, part, sides=2):
        who = owners(h)
        start, count = part

        def unit(i, _):
            m = pl.ds(pl.multiple_of(i % sides * MATE + base + start, 16), count)
            c = pl.ds(pl.multiple_of(i // sides * wch, 128), wch)
            total = None
            for o in who:
                w = wa[pl.ds(pl.multiple_of(o * ks, 16), ks), c]
                term = dot(tok[m, block_of(o)], w)
                total = term if total is None else total + term
            if h == 0:
                acc[m, c] = total
            else:
                acc[m, c] += total
            return 0

        lax.fori_loop(0, sides * 3, unit, 0)

    def project_near(h):
        project(h, OWN, ALL)

    def take_diag_tokens(h):
        for k, o in numbered(h):
            diag_tokens(k, o).wait_recv()

    def project_far(h):
        take_diag_tokens(h)
        project(h, TWIN, ALL)

    def mix(base, part, sides=2):
        start, count = part
        tc = 128
        seqs = count // seq

        def unit(i, _):
            j = i % (sides * seqs)
            m = pl.ds(
                pl.multiple_of(base + j // seqs * MATE + start + j % seqs * seq, seq), seq
            )
            c = pl.multiple_of(i // (sides * seqs) * tc, tc)
            o = acc[m, pl.ds(c, tc)]
            p = (
                acc[m, pl.ds(pl.multiple_of(wch + c, tc), tc)]
                * acc[m, pl.ds(pl.multiple_of(2 * wch + c, tc), tc)]
            )
            place = lax.broadcasted_iota(jnp.int32, p.shape, 0)
            before = jnp.where(place > 0, pltpu.roll(p, 1, 0), 0.0)
            after = jnp.where(place < seq - 1, pltpu.roll(p, seq - 1, 0), 0.0)
            taps = taps_ref[:, pl.ds(pl.multiple_of(share_at + c, tc), tc)]
            conv = taps[0:1] * before + taps[1:2] * p + taps[2:3] * after
            mixed[m, pl.ds(pl.multiple_of(share_at + c, tc), tc)] = (o * conv).astype(BF)
            return 0

        lax.fori_loop(0, sides * seqs * (wch // tc), unit, 0)

    def raise_part(size, start, x_base, acc_base, hs, new, final):
        who = [o for h in hs for o in owners(h)]
        tiles = ff // tn

        def unit(i, _):
            side = i % 2
            c = pl.ds(pl.multiple_of(i // 2 * tn, tn), tn)
            x_row = pl.multiple_of(x_base + side * MATE + start, 16)
            total = None
            for o in who:
                x = fst[pl.ds(x_row, size), block_of(o)]
                term = dot(x, wc[pl.ds(pl.multiple_of(o * ks, 16), ks), c])
                total = term if total is None else total + term
            span = pl.ds(pl.multiple_of(acc_base + side * rows + start, 16), size)
            if not new:
                total = total + acc[span, c]
            if final:
                total = jnp.maximum(total, 0.0)
                hid[pl.ds(x_row, size), c] = (total * total).astype(BF)
            else:
                acc[span, c] = total
            return 0

        lax.fori_loop(0, 2 * tiles, unit, 0)

    def raise_near(h):
        raise_part(rows, 0, OWN, 0, [h], h == 0, h == half)

    def raise_far(part):
        start, count = part
        for p in range(start // seq, (start + count) // seq):
            diag_first(p).wait_recv()
        raise_part(count, start, TWIN, both, range(half + 1), True, True)

    def send_mixed(p):
        for there, here in ((TWIN, OWN), (DIAG, MATE)):
            across_copy(
                ("mixed", there, p),
                mixed.at[pl.ds(there + p * seq, seq), pl.ds(share_at, wch)],
                mixed.at[pl.ds(here + p * seq, seq), pl.ds(share_at, wch)],
                "mixed",
                ("mixed", p),
            ).start()

    def mix_sums(p):
        span = pl.ds(p * seq, seq)
        return mate_copy(("mix", p), psend.at[:, span], precv.at[:, span], "mix")

    def mixout(p):
        span = pl.ds(p * seq, seq)
        if p == 0:
            across_whole(wb.at[pl.ds(0, n - 1), pl.ds(0, wch)], "wb", "wb").wait_recv()
        across_whole(
            mixed.at[pl.ds(0, 2 * seq), pl.ds(0, wch)], "mixed", ("mixed", p)
        ).wait_recv()

        def theirs(b, _):
            psend[b, span] = dot(mixed[pl.ds(MATE + p * seq, seq), :], wb[b]).astype(BF)
            return 0

        lax.fori_loop(0, n, theirs, 0)
        mix_sums(p).start()

        def ours(b, _):
            own[b, span] = dot(mixed[pl.ds(OWN + p * seq, seq), :], wb[b])
            return 0

        lax.fori_loop(0, n, ours, 0)

    def far_block(u, part):
        span = pl.ds(rows + part[0], part[1])
        return mate_copy(("low", u, part), psend.at[u, span], precv.at[u, span], "low")

    def near_block(u):
        span = pl.ds(0, rows)
        return mate_copy(
            ("low", u), psend.at[u, span], precv.at[u, span], "low", ("low", "near")
        )

    def across_block(u, part):
        span = pl.ds(*part)
        return across_copy(("low", u, part), xsend.at[u, span], xrecv.at[u, span], "low")

    def down(u):
        return jnp.concatenate([wd[o, j] for o, j in units[u]], axis=1)

    def lower_far(u, part):
        start, count = part
        span = pl.ds(rows + start, count)
        psend[u, span] = dot(hid[pl.ds(DIAG + start, count), :], down(u)).astype(BF)
        far_block(u, part).start()
        own[u, span] = dot(hid[pl.ds(TWIN + start, count), :], down(u))

    def low_pass(u, part):
        start, count = part
        far_block(u, part).wait_recv()
        span = pl.ds(rows + start, count)
        xsend[u, pl.ds(start, count)] = (own[u, span] + precv[u, span].astype(F32)).astype(BF)
        across_block(u, part).start()

    def lower_near(u):
        span = pl.ds(0, rows)
        psend[u, span] = dot(hid[pl.ds(MATE, rows), :], down(u)).astype(BF)
        near_block(u).start()
        own[u, span] = dot(hid[pl.ds(OWN, rows), :], down(u))

    lowered = [[EARLY, LATE] if u < 3 else [ALL] for u in range(n)]

    def norm(base_ref, gain_ref, dest_ref, start, count):
        tm = 32

        def unit(i, _):
            m = pl.multiple_of(start + i * tm, tm)
            parts = []
            for b in range(n):
                part = (
                    residual_scale
                    * base_ref[pl.ds(m, tm), pl.ds(b * nc, nc)].astype(F32)
                    + own[b, pl.ds(m, tm)]
                )
                parts.append(part + precv[b, pl.ds(m, tm)].astype(F32))
            total = parts[0]
            for b in range(1, n):
                total = total + parts[b]
            mean = jnp.sum(total, axis=-1, keepdims=True) / d
            parts = [p - mean for p in parts]
            square = parts[0] * parts[0]
            for b in range(1, n):
                square = square + parts[b] * parts[b]
            spread = jnp.sum(square, axis=-1, keepdims=True) / d
            scale = lax.rsqrt(spread + norm_epsilon)
            for b in range(n):
                cols = pl.ds(b * nc, nc)
                dest_ref[pl.ds(m, tm), cols] = (
                    parts[b] * scale * gain_ref[:, cols]
                ).astype(BF)
            return 0

        lax.fori_loop(0, count // tm, unit, 0)

    tm = SEQ
    C, D, Q, S = range(4)

    def add_near():
        def unit(i, _):
            m = pl.ds(pl.multiple_of(i * 32, 32), 32)
            for u in range(n):
                for i, place in enumerate(units[u]):
                    part = pl.ds(i * lane, lane)
                    own[u, m, part] = (
                        residual_scale * fst[m, columns(*place)].astype(F32)
                        + own[u, m, part]
                        + precv[u, m, part].astype(F32)
                    )
            return 0

        lax.fori_loop(0, rows // 32, unit, 0)

    def add_across(u):
        for part in lowered[u]:
            across_block(u, part).wait_recv()

        def unit(i, _):
            m = pl.ds(pl.multiple_of(i * tm, tm), tm)
            x = own[u, m] + xrecv[u, m].astype(F32)
            own[u, m] = x
            lanes = x[:, :lane] + x[:, lane:]
            stats[S, m] = lanes if u == 0 else stats[S, m] + lanes
            return 0

        lax.fori_loop(0, rows // tm, unit, 0)

    def center():
        def unit(i, _):
            m = pl.ds(pl.multiple_of(i * tm, tm), tm)
            c = jnp.sum(stats[S, m], axis=-1, keepdims=True) / ((n - 1) * nc)
            shift = square = None
            for u in range(n - 1):
                x = own[u, m] - c
                y = x * x
                lanes, squares = x[:, :lane] + x[:, lane:], y[:, :lane] + y[:, lane:]
                shift = lanes if shift is None else shift + lanes
                square = squares if square is None else square + squares
            stats[C, m] = jnp.broadcast_to(c, (tm, lane))
            stats[D, m] = shift
            stats[Q, m] = square
            return 0

        lax.fori_loop(0, rows // tm, unit, 0)

    def finish():
        tail = n - 1
        for part in lowered[tail]:
            across_block(tail, part).wait_recv()

        def measure(i, _):
            m = pl.ds(pl.multiple_of(i * tm, tm), tm)
            value = own[tail, m] + xrecv[tail, m].astype(F32)
            own[tail, m] = value
            c = stats[C, m]
            x, y = value[:, :lane] - c, value[:, lane:] - c
            shift = jnp.sum(stats[D, m] + (x + y), axis=-1, keepdims=True) / d
            square = jnp.sum(stats[Q, m] + (x * x + y * y), axis=-1, keepdims=True) / d
            spread = jnp.maximum(square - shift * shift, 0.0)
            stats[C, m] = c + shift
            stats[S, m] = jnp.broadcast_to(lax.rsqrt(spread + norm_epsilon), (tm, lane))
            return 0

        lax.fori_loop(0, rows // tm, measure, 0)

        def apply(i, _):
            m = pl.ds(pl.multiple_of(i * 32, 32), 32)
            mean, scale = stats[C, m], stats[S, m]
            for u in range(n):
                for i, place in enumerate(units[u]):
                    cols = columns(*place)
                    value = own[u, m, pl.ds(i * lane, lane)]
                    out_ref[m, cols] = ((value - mean) * scale * norm2_ref[:, cols]).astype(BF)
            return 0

        lax.fori_loop(0, rows // 32, apply, 0)

    def near_first(p):
        return mate_copy(
            ("near", p),
            fst.at[pl.ds(p * seq, seq)],
            fst.at[pl.ds(MATE + p * seq, seq)],
            "near",
            "near",
        )

    def twin_first(p):
        return across_copy(
            ("twin", p),
            fst.at[pl.ds(p * seq, seq)],
            fst.at[pl.ds(TWIN + p * seq, seq)],
            "first",
        )

    def diag_first(p):
        return mate_copy(
            ("diag", p),
            fst.at[pl.ds(TWIN + p * seq, seq)],
            fst.at[pl.ds(DIAG + p * seq, seq)],
            "diag",
        )

    def take_near_sums():
        mate_whole(precv.at[:, pl.ds(0, rows)], "low", ("low", "near")).wait_recv()

    def make_first(p):
        mix_sums(p).wait_recv()
        norm(tok, norm1_ref, fst, p * seq, seq)
        twin_first(p).start()
        near_first(p).start()

    def take_near():
        mate_whole(fst.at[pl.ds(MATE, rows)], "near", "near").wait_recv()

    def relay_first(p):
        twin_first(p).wait_recv()
        diag_first(p).start()

    def free_sends():
        mate_whole(psend.at[:, pl.ds(0, rows)], "mix").wait_send()

    plan = {}

    def after(ti, h, which, *work):
        plan.setdefault((ti, h, which), []).extend(work)

    def do(function, *values):
        return lambda: function(*values)

    last = half - 1

    for h in range(1, half):
        after(0, h, 1, do(cross_wb, h))
    after(0, half, 0, do(cross_wb, half))
    after(0, half, 0, do(relay_tokens, 0), do(project_near, 0), do(project_far, 0))
    for h in range(1, half):
        after(1, h, 0, do(relay_tokens, h))
        after(1, h, 1, do(project_near, h), do(project_far, h))
    after(1, last, 0, do(relay_tokens, half))
    after(1, half, 0, do(take_diag_tokens, half))
    after(1, half, 0, do(project, half, TWIN, EARLY), do(mix, TWIN, EARLY))
    for p in range(most):
        after(1, half, 0, do(send_mixed, p))
    after(1, half, 0, do(project, half, TWIN, LATE), do(mix, TWIN, LATE), do(send_mixed, most))
    after(1, half, 0, do(project_near, half), do(mix, OWN, ALL))
    after(2, 1, 0, do(mixout, 0))
    after(2, 1, 1, do(make_first, 0), do(mixout, 1), do(make_first, 1))
    for p in range(2, pieces):
        after(2, 2, 0, do(mixout, p), do(make_first, p))
    after(2, 2, 1, do(take_near), do(raise_near, 0), do(raise_near, 1))
    after(2, 3, 0, do(raise_near, 2), do(free_sends))
    for h in range(3, half):
        after(2, h, 1, do(raise_near, h))
    after(2, last, 1, do(relay_first, 0))
    after(2, half, 0, do(raise_near, half), do(lower_near, 0))
    for p in range(1, most):
        after(2, half, 0, do(relay_first, p))
    after(2, half, 0, do(raise_far, EARLY))
    after(3, 1, 0, do(lower_far, 0, EARLY), do(lower_far, 1, EARLY))
    after(3, 1, 0, do(low_pass, 0, EARLY), do(low_pass, 1, EARLY), do(relay_first, most))
    after(3, 1, 1, do(lower_far, 2, EARLY), do(low_pass, 2, EARLY), do(raise_far, LATE))
    for u in range(3):
        after(3, 1, 1, do(lower_far, u, LATE))
    for u in range(3):
        after(3, 1, 1, do(low_pass, u, LATE))
    for u in range(3, n):
        e = (3, half, 0) if u == n - 1 else (3, (u + 1) // 2, (u + 1) % 2)
        after(*e, do(lower_far, u, ALL), do(lower_near, u - 2), do(low_pass, u, ALL))
    after(3, half, 0, do(lower_near, n - 2), do(lower_near, n - 1))

    for ti in range(4):
        for e in events(ti):
            event(*e)
            for work in plan.get(e, ()):
                work()

    take_near_sums()
    add_near()
    for u in range(n - 1):
        add_across(u)
    center()
    finish()

    mate_whole(tok.at[pl.ds(0, both)], "tok").wait_send()
    for group in ("near", "diag"):
        mate_whole(fst.at[pl.ds(0, rows)], group).wait_send()
    mate_whole(psend, "low").wait_send()
    across_whole(tok.at[pl.ds(0, rows)], "tok").wait_send()
    across_whole(wb.at[pl.ds(0, n - 1), pl.ds(0, wch)], "wb").wait_send()
    across_whole(mixed.at[pl.ds(0, both), pl.ds(0, wch)], "mixed").wait_send()
    across_whole(fst.at[pl.ds(0, rows)], "first").wait_send()
    across_whole(xsend, "low").wait_send()
    for ti, ref in enumerate(
        (
            wb.at[pl.ds(0, n - 1), pl.ds(0, wch)],
            wa.at[pl.ds(0, (n - 1) * ks)],
            wc.at[pl.ds(0, (n - 1) * ks)],
            wd.at[pl.ds(0, n - 1)],
        )
    ):
        pltpu.make_async_remote_copy(
            src_ref=ref,
            dst_ref=ref,
            send_sem=ring_send.at[ti],
            recv_sem=ring_recv.at[0],
            device_id=right,
            device_id_type=MESH,
        ).wait_send()


def fits(mesh, args):
    n = mesh.shape["fs"]
    rows, d = args[0].shape
    ks = args[1].shape[0]
    wch = args[1].shape[1] // 2
    nc = args[5].shape[1]
    ff = args[7].shape[1] // 2
    return (
        mesh.shape["rep"] == 2
        and mesh.shape["tp"] == 2
        and n % 2 == 0
        and n >= 8
        and ks % 128 == 0
        and nc == 256
        and wch % 128 == 0
        and ff % 256 == 0
        and wch <= rows
        and ff <= 4 * rows
        and ff <= 3 * wch
        and ks <= rows
        and rows % SEQ == 0
        and 2 * SEQ <= rows <= 8 * SEQ
    )


def fused(mesh, *args):
    (
        tokens,
        outer_weight,
        inner_weight,
        value_weight,
        conv_taps,
        mix_out,
        norm_first,
        up_weight,
        down_weight,
        norm_second,
    ) = args
    n = mesh.shape["fs"]
    rows, d = tokens.shape
    ks = outer_weight.shape[0]
    wch = outer_weight.shape[1] // 2
    ff = up_weight.shape[1] // 2
    nc = mix_out.shape[1]
    both = 2 * rows
    anywhere = pl.BlockSpec(memory_space=pl.ANY)
    vmem = pl.BlockSpec(memory_space=pltpu.VMEM)
    messages = 4 * (2 * n - 2)
    pairs = 2 * n + 6 + 2 * (rows // SEQ)
    crosses = 2 * n + 4 + 2 * (rows // SEQ)
    return pl.pallas_call(
        functools.partial(layer_kernel, n),
        out_shape=pltpu.VMEM((rows, d), BF),
        in_specs=[
            anywhere,
            anywhere,
            anywhere,
            anywhere,
            vmem,
            anywhere,
            vmem,
            anywhere,
            anywhere,
            vmem,
        ],
        out_specs=vmem,
        scratch_shapes=[
            pltpu.VMEM((n * ks, 3 * wch), BF),
            pltpu.VMEM((n, 2 * wch, nc), BF),
            pltpu.VMEM((n * ks, ff), BF),
            pltpu.VMEM((n, 2, ff, nc // 2), BF),
            pltpu.VMEM((2 * both, d), BF),
            pltpu.VMEM((2 * both, 3 * wch), F32),
            pltpu.VMEM((2 * both, 2 * wch), BF),
            pltpu.VMEM((n, both, nc), F32),
            pltpu.VMEM((n, both, nc), BF),
            pltpu.VMEM((n, both, nc), BF),
            pltpu.VMEM((n, rows, nc), BF),
            pltpu.VMEM((n, rows, nc), BF),
            pltpu.VMEM((2 * both, d), BF),
            pltpu.VMEM((2 * both, ff), BF),
            pltpu.VMEM((4, rows, 128), F32),
            pltpu.SemaphoreType.DMA((8,)),
            pltpu.SemaphoreType.DMA((4,)),
            pltpu.SemaphoreType.DMA((messages,)),
            pltpu.SemaphoreType.DMA((5,)),
            pltpu.SemaphoreType.DMA((pairs,)),
            pltpu.SemaphoreType.DMA((5,)),
            pltpu.SemaphoreType.DMA((crosses,)),
        ],
        compiler_params=pltpu.CompilerParams(
            collective_id=0, has_side_effects=True, vmem_limit_bytes=62 * 2**20
        ),
        name="layer",
    )(
        tokens,
        outer_weight,
        inner_weight,
        value_weight,
        conv_taps,
        mix_out,
        norm_first.reshape(1, d),
        up_weight,
        down_weight,
        norm_second.reshape(1, d),
    )


def solution(mesh):
    def body(*args):
        return fused(mesh, *args) if fits(mesh, args) else local(*args)

    return jax.shard_map(
        body,
        mesh=mesh,
        in_specs=(
            P(("rep", "fs", "tp"), None),
            P("fs", "tp"),
            P("fs", "tp"),
            P("fs", "tp"),
            P(None, "tp"),
            P("tp", "fs"),
            P(),
            P("fs", "tp"),
            P("tp", "fs"),
            P(),
        ),
        out_specs=P(("rep", "fs", "tp"), None),
        check_vma=False,
    )
```

```python
import functools

import jax
import jax.numpy as jnp
from jax import lax
from jax.experimental import pallas as pl
from jax.experimental.pallas import tpu as pltpu
from jax.sharding import PartitionSpec as P

SEQ = 128


residual_scale = 2.0**0.25
norm_epsilon = 1e-05


def layer_norm(values, scaling):
    center = values - jnp.mean(values, axis=-1, keepdims=True)
    spread = jnp.mean(center * center, axis=-1, keepdims=True)
    return center * lax.rsqrt(spread + norm_epsilon) * scaling


def short_conv(product, conv_taps):
    places = jnp.arange(product.shape[0], dtype=jnp.int32) % SEQ
    blank = jnp.zeros((1, product.shape[1]), jnp.float32)
    before = jnp.concatenate([blank, product[:-1]], axis=0)
    after = jnp.concatenate([product[1:], blank], axis=0)
    before = jnp.where((places > 0)[:, None], before, 0.0)
    after = jnp.where((places < SEQ - 1)[:, None], after, 0.0)
    return conv_taps[0] * before + conv_taps[1] * product + conv_taps[2] * after


def local(
    tokens,
    outer_weight,
    inner_weight,
    value_weight,
    conv_taps,
    mix_out,
    norm_first,
    up_weight,
    down_weight,
    norm_second,
):
    grouped = lax.all_gather(tokens, "tp", axis=0, tiled=True)
    outer_bf = outer_weight.astype(jnp.bfloat16)
    inner_bf = inner_weight.astype(jnp.bfloat16)
    value_bf = value_weight.astype(jnp.bfloat16)
    outer_full, inner_full, value_full = (
        lax.all_gather(outer_bf, "fs", axis=0, tiled=True),
        lax.all_gather(inner_bf, "fs", axis=0, tiled=True),
        lax.all_gather(value_bf, "fs", axis=0, tiled=True),
    )
    outer = jnp.dot(grouped, outer_full, preferred_element_type=jnp.float32)
    inner = jnp.dot(grouped, inner_full, preferred_element_type=jnp.float32)
    value = jnp.dot(grouped, value_full, preferred_element_type=jnp.float32)
    mixed = (outer * short_conv(inner * value, conv_taps)).astype(jnp.bfloat16)
    mixout_full = lax.all_gather(mix_out.astype(jnp.bfloat16), "fs", axis=1, tiled=True)
    selected = mixed
    mixing = lax.psum_scatter(
        jnp.dot(selected, mixout_full, preferred_element_type=jnp.float32).astype(jnp.bfloat16),
        "tp",
        scatter_dimension=0,
        tiled=True,
    ).astype(jnp.float32)
    first = layer_norm(residual_scale * tokens.astype(jnp.float32) + mixing, norm_first).astype(
        jnp.bfloat16
    )
    grouped_first = lax.all_gather(first, "tp", axis=0, tiled=True)
    upward_bf = up_weight.astype(jnp.bfloat16)
    upward_full = lax.all_gather(upward_bf, "fs", axis=0, tiled=True)
    raised = jnp.dot(grouped_first, upward_full, preferred_element_type=jnp.float32)
    raised = jax.nn.relu(raised)
    hidden = (raised * raised).astype(jnp.bfloat16)
    down_full = lax.all_gather(down_weight.astype(jnp.bfloat16), "fs", axis=1, tiled=True)
    selected = hidden
    lowered = lax.psum_scatter(
        jnp.dot(selected, down_full, preferred_element_type=jnp.float32).astype(jnp.bfloat16),
        "tp",
        scatter_dimension=0,
        tiled=True,
    ).astype(jnp.float32)
    return layer_norm(residual_scale * first.astype(jnp.float32) + lowered, norm_second).astype(
        jnp.bfloat16
    )


MESH = pl.DeviceIdType.MESH
BF = jnp.bfloat16
F32 = jnp.float32


def dot(a, b):
    return jnp.dot(a, b, preferred_element_type=F32)


def layer_kernel(
    n,
    tokens_hbm,
    outer_hbm,
    inner_hbm,
    value_hbm,
    taps_ref,
    mix_hbm,
    norm1_ref,
    up_hbm,
    down_hbm,
    norm2_ref,
    out_ref,
    wa,
    wb,
    wc,
    wd,
    tok,
    acc,
    mixed,
    own,
    psend,
    precv,
    xsend,
    xrecv,
    fst,
    hid,
    stats,
    load_sem,
    ring_send,
    ring_recv,
    tp_send,
    tp_recv,
    x_send,
    x_recv,
):
    half = n // 2
    r = lax.axis_index("rep")
    f = lax.axis_index("fs")
    t = lax.axis_index("tp")
    rows = tokens_hbm.shape[0]
    both = 2 * rows
    d = tokens_hbm.shape[1]
    ks = outer_hbm.shape[0]
    wch = wb.shape[1] // 2
    ff = wc.shape[1]
    nc = wb.shape[2]
    OWN, TWIN, MATE, DIAG = 0, rows, 2 * rows, 3 * rows

    odd = f % 2
    pos = (1 - odd) * (f // 2) + odd * (n - 1 - f // 2)

    def at(place):
        p = (place + 2 * n) % n
        hi = p // half
        return (1 - hi) * (2 * p) + hi * (2 * (n - 1 - p) + 1)

    right = {"fs": at(pos + 1)}
    left = {"fs": at(pos - 1)}
    across = {"rep": 1 - r}
    mate = {"tp": 1 - t}

    def owners(h):
        if h == 0:
            return [f]
        if h == half:
            return [at(pos + half)]
        return [at(pos - h), at(pos + h)]

    def numbered(h):
        return [(0 if h == 0 else 2 * h - 1 + k, o) for k, o in enumerate(owners(h))]

    every = [item for h in range(half + 1) for item in numbered(h)]

    units = [((f, 0), (f, 1))]
    for h in range(1, half):
        a, b = owners(h)
        units += [((a, 0), (b, 1)), ((a, 1), (b, 0))]
    units.append(tuple((o, j) for o in owners(half) for j in range(2)))
    lane = nc // 2

    def columns(o, j):
        return pl.ds(pl.multiple_of(o * nc + j * lane, lane), lane)

    mine = pl.multiple_of(r * ff, 128)
    share_at = pl.multiple_of(r * wch, 128)
    first_down = min(ff, both)
    rest_down = ff - first_down
    loads = [
        pltpu.make_async_copy(
            src.at[:, pl.ds(share_at, wch)],
            acc.at[pl.ds(i * ks, ks), pl.ds(0, wch)],
            load_sem.at[i],
        )
        for i, src in enumerate((outer_hbm, inner_hbm, value_hbm))
    ]
    loads += [
        pltpu.make_async_copy(
            mix_hbm, own.at[0, pl.ds(0, 2 * wch)], load_sem.at[3]
        ),
        pltpu.make_async_copy(
            up_hbm.at[:, pl.ds(mine, ff)],
            acc.at[pl.ds(3 * ks, ks), pl.ds(0, ff)],
            load_sem.at[4],
        ),
        pltpu.make_async_copy(
            down_hbm.at[pl.ds(mine, first_down)],
            own.at[1, pl.ds(0, first_down)],
            load_sem.at[5],
        ),
        pltpu.make_async_copy(tokens_hbm, tok.at[pl.ds(0, rows)], load_sem.at[6]),
    ]
    if rest_down:
        loads.append(
            pltpu.make_async_copy(
                down_hbm.at[pl.ds(mine + first_down, rest_down)],
                own.at[2, pl.ds(0, rest_down)],
                load_sem.at[7],
            )
        )
    for i in (3, 0, 1, 2):
        loads[i].start()

    barrier = pltpu.get_barrier_semaphore()
    for device in (right, left, across, mate):
        pl.semaphore_signal(barrier, inc=1, device_id=device, device_id_type=MESH)
    pl.semaphore_wait(barrier, 4)

    def copier(device, send_sems, recv_sems):
        made, arrivals, groups = {}, {}, {}

        def copy(key, src, dst, group, arrival=None):
            if key not in made:
                place = arrival or key
                made[key] = pltpu.make_async_remote_copy(
                    src_ref=src,
                    dst_ref=dst,
                    send_sem=send_sems.at[groups.setdefault(group, len(groups))],
                    recv_sem=recv_sems.at[arrivals.setdefault(place, len(arrivals))],
                    device_id=device,
                    device_id_type=MESH,
                )
            return made[key]

        def whole(ref, group, arrival=None):
            return pltpu.make_async_remote_copy(
                src_ref=ref,
                dst_ref=ref,
                send_sem=send_sems.at[groups.get(group, 0)],
                recv_sem=recv_sems.at[arrivals.get(arrival, 0)],
                device_id=device,
                device_id_type=MESH,
            )

        return copy, whole

    mate_copy, mate_whole = copier(mate, tp_send, tp_recv)
    across_copy, across_whole = copier(across, x_send, x_recv)

    def piece(ti, which, owner):
        if ti == 0:
            u = wch // 2
            return wb.at[owner, pl.ds(pl.multiple_of(share_at + which * u, 16), u)]
        u = ks // 2
        if ti < 3:
            return (wa, wc)[ti - 1].at[pl.ds(pl.multiple_of(owner * ks + which * u, 16), u)]
        return wd.at[owner, which]

    per = 4 * half - 2
    index = {}
    for h in range(1, half + 1):
        for kind in ("Rq", "Rp", "Lq", "Lp"):
            if h == half and kind in ("Rp", "Lq"):
                continue
            index[kind, h] = len(index)

    copies = {}

    def message(ti, kind, h):
        key = (ti, kind, h)
        if key not in copies:
            which = int(kind[1] == "p")
            if kind[0] == "R":
                src, device = at(pos - (h - 1)), right
            else:
                src, device = at(pos + (h - 1)), left
            i = ti * per + index[kind, h]
            ref = piece(ti, which, src)
            copies[key] = pltpu.make_async_remote_copy(
                src_ref=ref,
                dst_ref=ref,
                send_sem=ring_send.at[ti],
                recv_sem=ring_recv.at[i],
                device_id=device,
                device_id_type=MESH,
            )
        return copies[key]

    def send(ti, kind, h):
        if ti < 4 and (kind, h) in index:
            message(ti, kind, h).start()

    def got(ti, kind, h):
        message(ti, kind, h).wait_recv()

    def event(ti, h, which):
        if which == 0:
            got(ti, "Rq", h)
            send(ti, "Rq", h + 1)
            if h == half:
                send(ti + 1, "Rp", 1)
            got(ti, "Lp", h)
            send(ti, "Lp", h + 1)
            if h == half:
                send(ti + 1, "Lq", 1)
        else:
            got(ti, "Rp", h)
            if h + 1 < half:
                send(ti, "Rp", h + 1)
            else:
                send(ti + 1, "Rq", 1)
            got(ti, "Lq", h)
            if h + 1 < half:
                send(ti, "Lq", h + 1)
            else:
                send(ti + 1, "Lp", 1)

    def events(ti):
        out = []
        for h in range(1, half + 1):
            out.append((ti, h, 0))
            if h < half:
                out.append((ti, h, 1))
        return out

    def block_of(o):
        return pl.ds(pl.multiple_of(o * ks, 128), ks)

    def twin_tokens(k, o):
        return across_copy(
            ("tok", k),
            tokens_hbm.at[:, block_of(o)],
            tok.at[pl.ds(TWIN, rows), block_of(o)],
            "tok",
        )

    def diag_tokens(k, o):
        return mate_copy(
            ("tok", k),
            tok.at[pl.ds(TWIN, rows), block_of(o)],
            tok.at[pl.ds(DIAG, rows), block_of(o)],
            "tok",
        )

    share = mate_copy("share", tokens_hbm, tok.at[pl.ds(MATE, rows)], "tok")
    for k, o in every:
        twin_tokens(k, o).start()
    loads[3].wait()
    wb[f] = own[0, pl.ds(0, 2 * wch)].astype(BF)
    send(0, "Rq", 1)
    send(0, "Lp", 1)
    send(0, "Rp", 1)
    send(0, "Lq", 1)
    for load in loads[4:]:
        load.start()
    share.start()
    for i in range(3):
        loads[i].wait()
        wa[pl.ds(pl.multiple_of(f * ks, 16), ks), pl.ds(i * wch, wch)] = acc[
            pl.ds(i * ks, ks), pl.ds(0, wch)
        ].astype(BF)
    loads[4].wait()
    wc[pl.ds(pl.multiple_of(f * ks, 16), ks), :] = acc[
        pl.ds(3 * ks, ks), pl.ds(0, ff)
    ].astype(BF)
    loads[5].wait()
    for j in range(2):
        wd[f, j, pl.ds(0, first_down)] = own[
            1, pl.ds(0, first_down), pl.ds(j * lane, lane)
        ].astype(BF)
    if rest_down:
        loads[7].wait()
        for j in range(2):
            wd[f, j, pl.ds(first_down, rest_down)] = own[
                2, pl.ds(0, rest_down), pl.ds(j * lane, lane)
            ].astype(BF)
    loads[6].wait()
    share.wait_recv()

    tn = 256
    seq = SEQ
    pieces = rows // seq
    most = pieces - 1
    EARLY, LATE, ALL = (0, most * seq), (most * seq, seq), (0, rows)

    def cross_wb(h):
        for k, o in numbered(h):
            ref = wb.at[o, pl.ds(share_at, wch)]
            across_copy(("wb", k), ref, ref, "wb", "wb").start()

    def relay_tokens(h):
        for k, o in numbered(h):
            twin_tokens(k, o).wait_recv()
            diag_tokens(k, o).start()

    def project(h, base, part, sides=2):
        who = owners(h)
        start, count = part

        def unit(i, _):
            m = pl.ds(pl.multiple_of(i % sides * MATE + base + start, 16), count)
            c = pl.ds(pl.multiple_of(i // sides * wch, 128), wch)
            total = None
            for o in who:
                w = wa[pl.ds(pl.multiple_of(o * ks, 16), ks), c]
                term = dot(tok[m, block_of(o)], w)
                total = term if total is None else total + term
            if h == 0:
                acc[m, c] = total
            else:
                acc[m, c] += total
            return 0

        lax.fori_loop(0, sides * 3, unit, 0)

    def project_near(h):
        project(h, OWN, ALL)

    def take_diag_tokens(h):
        for k, o in numbered(h):
            diag_tokens(k, o).wait_recv()

    def project_far(h):
        take_diag_tokens(h)
        project(h, TWIN, ALL)

    def mix(base, part, sides=2):
        start, count = part
        tc = 128
        seqs = count // seq

        def unit(i, _):
            j = i % (sides * seqs)
            m = pl.ds(
                pl.multiple_of(base + j // seqs * MATE + start + j % seqs * seq, seq), seq
            )
            c = pl.multiple_of(i // (sides * seqs) * tc, tc)
            o = acc[m, pl.ds(c, tc)]
            p = (
                acc[m, pl.ds(pl.multiple_of(wch + c, tc), tc)]
                * acc[m, pl.ds(pl.multiple_of(2 * wch + c, tc), tc)]
            )
            place = lax.broadcasted_iota(jnp.int32, p.shape, 0)
            before = jnp.where(place > 0, pltpu.roll(p, 1, 0), 0.0)
            after = jnp.where(place < seq - 1, pltpu.roll(p, seq - 1, 0), 0.0)
            taps = taps_ref[:, pl.ds(pl.multiple_of(share_at + c, tc), tc)]
            conv = taps[0:1] * before + taps[1:2] * p + taps[2:3] * after
            mixed[m, pl.ds(pl.multiple_of(share_at + c, tc), tc)] = (o * conv).astype(BF)
            return 0

        lax.fori_loop(0, sides * seqs * (wch // tc), unit, 0)

    def raise_part(size, start, x_base, acc_base, hs, new, final):
        who = [o for h in hs for o in owners(h)]
        tiles = ff // tn

        def unit(i, _):
            side = i % 2
            c = pl.ds(pl.multiple_of(i // 2 * tn, tn), tn)
            x_row = pl.multiple_of(x_base + side * MATE + start, 16)
            total = None
            for o in who:
                x = fst[pl.ds(x_row, size), block_of(o)]
                term = dot(x, wc[pl.ds(pl.multiple_of(o * ks, 16), ks), c])
                total = term if total is None else total + term
            span = pl.ds(pl.multiple_of(acc_base + side * rows + start, 16), size)
            if not new:
                total = total + acc[span, c]
            if final:
                total = jnp.maximum(total, 0.0)
                hid[pl.ds(x_row, size), c] = (total * total).astype(BF)
            else:
                acc[span, c] = total
            return 0

        lax.fori_loop(0, 2 * tiles, unit, 0)

    def raise_near(h):
        raise_part(rows, 0, OWN, 0, [h], h == 0, h == half)

    def raise_far(part):
        start, count = part
        for p in range(start // seq, (start + count) // seq):
            diag_first(p).wait_recv()
        raise_part(count, start, TWIN, both, range(half + 1), True, True)

    def send_mixed(p):
        for there, here in ((TWIN, OWN), (DIAG, MATE)):
            across_copy(
                ("mixed", there, p),
                mixed.at[pl.ds(there + p * seq, seq), pl.ds(share_at, wch)],
                mixed.at[pl.ds(here + p * seq, seq), pl.ds(share_at, wch)],
                "mixed",
                ("mixed", p),
            ).start()

    def mix_sums(p):
        span = pl.ds(p * seq, seq)
        return mate_copy(("mix", p), psend.at[:, span], precv.at[:, span], "mix")

    def mixout(p):
        span = pl.ds(p * seq, seq)
        if p == 0:
            across_whole(wb.at[pl.ds(0, n - 1), pl.ds(0, wch)], "wb", "wb").wait_recv()
        across_whole(
            mixed.at[pl.ds(0, 2 * seq), pl.ds(0, wch)], "mixed", ("mixed", p)
        ).wait_recv()

        def theirs(b, _):
            psend[b, span] = dot(mixed[pl.ds(MATE + p * seq, seq), :], wb[b]).astype(BF)
            return 0

        lax.fori_loop(0, n, theirs, 0)
        mix_sums(p).start()

        def ours(b, _):
            own[b, span] = dot(mixed[pl.ds(OWN + p * seq, seq), :], wb[b])
            return 0

        lax.fori_loop(0, n, ours, 0)

    def far_block(u, part):
        span = pl.ds(rows + part[0], part[1])
        return mate_copy(("low", u, part), psend.at[u, span], precv.at[u, span], "low")

    def near_group(u):
        return max(u - (n - 3), 0)

    def near_block(u):
        span = pl.ds(0, rows)
        return mate_copy(
            ("low", u), psend.at[u, span], precv.at[u, span], "low", ("low", near_group(u))
        )

    def across_block(u, part):
        span = pl.ds(*part)
        return across_copy(("low", u, part), xsend.at[u, span], xrecv.at[u, span], "low")

    def down(u):
        return jnp.concatenate([wd[o, j] for o, j in units[u]], axis=1)

    def lower_far(u, part):
        start, count = part
        span = pl.ds(rows + start, count)
        psend[u, span] = dot(hid[pl.ds(DIAG + start, count), :], down(u)).astype(BF)
        far_block(u, part).start()
        own[u, span] = dot(hid[pl.ds(TWIN + start, count), :], down(u))

    def low_pass(u, part):
        start, count = part
        far_block(u, part).wait_recv()
        span = pl.ds(rows + start, count)
        xsend[u, pl.ds(start, count)] = (own[u, span] + precv[u, span].astype(F32)).astype(BF)
        across_block(u, part).start()

    def lower_near(u):
        span = pl.ds(0, rows)
        psend[u, span] = dot(hid[pl.ds(MATE, rows), :], down(u)).astype(BF)
        near_block(u).start()
        own[u, span] = dot(hid[pl.ds(OWN, rows), :], down(u))

    lowered = [[ALL] if 3 <= u < n - 1 else [EARLY, LATE] for u in range(n)]

    def norm(base_ref, gain_ref, dest_ref, start, count):
        tm = 32

        def unit(i, _):
            m = pl.multiple_of(start + i * tm, tm)
            parts = []
            for b in range(n):
                part = (
                    residual_scale
                    * base_ref[pl.ds(m, tm), pl.ds(b * nc, nc)].astype(F32)
                    + own[b, pl.ds(m, tm)]
                )
                parts.append(part + precv[b, pl.ds(m, tm)].astype(F32))
            total = parts[0]
            for b in range(1, n):
                total = total + parts[b]
            mean = jnp.sum(total, axis=-1, keepdims=True) / d
            parts = [p - mean for p in parts]
            square = parts[0] * parts[0]
            for b in range(1, n):
                square = square + parts[b] * parts[b]
            spread = jnp.sum(square, axis=-1, keepdims=True) / d
            scale = lax.rsqrt(spread + norm_epsilon)
            for b in range(n):
                cols = pl.ds(b * nc, nc)
                dest_ref[pl.ds(m, tm), cols] = (
                    parts[b] * scale * gain_ref[:, cols]
                ).astype(BF)
            return 0

        lax.fori_loop(0, count // tm, unit, 0)

    tm = SEQ
    C, D, Q, S = range(4)

    def add_near(first, count):
        def unit(i, _):
            m = pl.ds(pl.multiple_of(i * 32, 32), 32)
            for u in range(first, first + count):
                for i, place in enumerate(units[u]):
                    part = pl.ds(i * lane, lane)
                    own[u, m, part] = (
                        residual_scale * fst[m, columns(*place)].astype(F32)
                        + own[u, m, part]
                        + precv[u, m, part].astype(F32)
                    )
            return 0

        lax.fori_loop(0, rows // 32, unit, 0)

    def add_across(u):
        for part in lowered[u]:
            across_block(u, part).wait_recv()

        def unit(i, _):
            m = pl.ds(pl.multiple_of(i * tm, tm), tm)
            x = own[u, m] + xrecv[u, m].astype(F32)
            own[u, m] = x
            lanes = x[:, :lane] + x[:, lane:]
            stats[S, m] = lanes if u == 0 else stats[S, m] + lanes
            return 0

        lax.fori_loop(0, rows // tm, unit, 0)

    def center():
        def unit(i, _):
            m = pl.ds(pl.multiple_of(i * tm, tm), tm)
            c = jnp.sum(stats[S, m], axis=-1, keepdims=True) / ((n - 1) * nc)
            shift = square = None
            for u in range(n - 1):
                x = own[u, m] - c
                y = x * x
                lanes, squares = x[:, :lane] + x[:, lane:], y[:, :lane] + y[:, lane:]
                shift = lanes if shift is None else shift + lanes
                square = squares if square is None else square + squares
            stats[C, m] = jnp.broadcast_to(c, (tm, lane))
            stats[D, m] = shift
            stats[Q, m] = square
            return 0

        lax.fori_loop(0, rows // tm, unit, 0)

    def finish(part):
        start, count = part
        tail = n - 1
        across_block(tail, part).wait_recv()

        def measure(i, _):
            m = pl.ds(pl.multiple_of(start + i * tm, tm), tm)
            value = own[tail, m] + xrecv[tail, m].astype(F32)
            own[tail, m] = value
            c = stats[C, m]
            x, y = value[:, :lane] - c, value[:, lane:] - c
            shift = jnp.sum(stats[D, m] + (x + y), axis=-1, keepdims=True) / d
            square = jnp.sum(stats[Q, m] + (x * x + y * y), axis=-1, keepdims=True) / d
            spread = jnp.maximum(square - shift * shift, 0.0)
            stats[C, m] = c + shift
            stats[S, m] = jnp.broadcast_to(lax.rsqrt(spread + norm_epsilon), (tm, lane))
            return 0

        lax.fori_loop(0, count // tm, measure, 0)

        def apply(i, _):
            m = pl.ds(pl.multiple_of(start + i * 32, 32), 32)
            mean, scale = stats[C, m], stats[S, m]
            for u in range(n):
                for i, place in enumerate(units[u]):
                    cols = columns(*place)
                    value = own[u, m, pl.ds(i * lane, lane)]
                    out_ref[m, cols] = ((value - mean) * scale * norm2_ref[:, cols]).astype(BF)
            return 0

        lax.fori_loop(0, count // 32, apply, 0)

    def near_first(p):
        return mate_copy(
            ("near", p),
            fst.at[pl.ds(p * seq, seq)],
            fst.at[pl.ds(MATE + p * seq, seq)],
            "near",
            "near",
        )

    def twin_first(p):
        return across_copy(
            ("twin", p),
            fst.at[pl.ds(p * seq, seq)],
            fst.at[pl.ds(TWIN + p * seq, seq)],
            "first",
        )

    def diag_first(p):
        return mate_copy(
            ("diag", p),
            fst.at[pl.ds(TWIN + p * seq, seq)],
            fst.at[pl.ds(DIAG + p * seq, seq)],
            "diag",
        )

    def take_near_sums(first, count):
        mate_whole(
            precv.at[pl.ds(first, count), pl.ds(0, rows)], "low", ("low", near_group(first))
        ).wait_recv()
        add_near(first, count)

    def make_first(p):
        mix_sums(p).wait_recv()
        norm(tok, norm1_ref, fst, p * seq, seq)
        twin_first(p).start()
        near_first(p).start()

    def take_near():
        mate_whole(fst.at[pl.ds(MATE, rows)], "near", "near").wait_recv()

    def relay_first(p):
        twin_first(p).wait_recv()
        diag_first(p).start()

    def free_sends():
        mate_whole(psend.at[:, pl.ds(0, rows)], "mix").wait_send()

    plan = {}

    def after(ti, h, which, *work):
        plan.setdefault((ti, h, which), []).extend(work)

    def do(function, *values):
        return lambda: function(*values)

    last = half - 1

    for h in range(1, half):
        after(0, h, 1, do(cross_wb, h))
    after(0, half, 0, do(cross_wb, half))
    after(0, half, 0, do(relay_tokens, 0), do(project_near, 0), do(project_far, 0))
    for h in range(1, half):
        after(1, h, 0, do(relay_tokens, h))
        after(1, h, 1, do(project_near, h), do(project_far, h))
    after(1, last, 0, do(relay_tokens, half))
    after(1, half, 0, do(take_diag_tokens, half))
    after(1, half, 0, do(project, half, TWIN, EARLY), do(mix, TWIN, EARLY))
    for p in range(most):
        after(1, half, 0, do(send_mixed, p))
    after(1, half, 0, do(project, half, TWIN, LATE), do(mix, TWIN, LATE), do(send_mixed, most))
    after(1, half, 0, do(project_near, half), do(mix, OWN, ALL))
    after(2, 1, 0, do(mixout, 0))
    after(2, 1, 1, do(make_first, 0), do(mixout, 1), do(make_first, 1))
    for p in range(2, pieces):
        after(2, 2, 0, do(mixout, p), do(make_first, p))
    after(2, 2, 1, do(take_near), do(raise_near, 0), do(raise_near, 1))
    after(2, 3, 0, do(raise_near, 2), do(free_sends))
    for h in range(3, half):
        after(2, h, 1, do(raise_near, h))
    after(2, last, 1, do(relay_first, 0))
    after(2, half, 0, do(raise_near, half), do(lower_near, 0))
    for p in range(1, most):
        after(2, half, 0, do(relay_first, p))
    after(2, half, 0, do(raise_far, EARLY))
    after(3, 1, 0, do(lower_far, 0, EARLY), do(lower_far, 1, EARLY))
    after(3, 1, 0, do(low_pass, 0, EARLY), do(low_pass, 1, EARLY), do(relay_first, most))
    after(3, 1, 1, do(lower_far, 2, EARLY), do(low_pass, 2, EARLY), do(raise_far, LATE))
    for u in range(3):
        after(3, 1, 1, do(lower_far, u, LATE))
    for u in range(3):
        after(3, 1, 1, do(low_pass, u, LATE))
    for u in range(3, n - 1):
        e = (3, (u + 1) // 2, (u + 1) % 2)
        near = u - 2 if u < n - 2 else n - 3
        after(*e, do(lower_far, u, ALL), do(lower_near, near), do(low_pass, u, ALL))
    after(3, last, 0, do(lower_near, n - 4))
    after(3, last, 1, do(lower_near, n - 2))
    after(3, last, 1, do(take_near_sums, 0, n - 2))
    for u in range(n - 3):
        after(3, last, 1, do(add_across, u))
    for work in (lower_far, low_pass):
        after(3, half, 0, do(work, n - 1, EARLY), do(work, n - 1, LATE))
    after(3, half, 0, do(lower_near, n - 1), do(take_near_sums, n - 2, 1))
    for u in range(n - 3, n - 1):
        after(3, half, 0, do(add_across, u))
    after(3, half, 0, do(center), do(take_near_sums, n - 1, 1), do(finish, EARLY))
    after(3, half, 0, do(finish, LATE))

    for ti in range(4):
        for e in events(ti):
            event(*e)
            for work in plan.get(e, ()):
                work()

    mate_whole(tok.at[pl.ds(0, both)], "tok").wait_send()
    for group in ("near", "diag"):
        mate_whole(fst.at[pl.ds(0, rows)], group).wait_send()
    mate_whole(psend, "low").wait_send()
    across_whole(tok.at[pl.ds(0, rows)], "tok").wait_send()
    across_whole(wb.at[pl.ds(0, n - 1), pl.ds(0, wch)], "wb").wait_send()
    across_whole(mixed.at[pl.ds(0, both), pl.ds(0, wch)], "mixed").wait_send()
    across_whole(fst.at[pl.ds(0, rows)], "first").wait_send()
    across_whole(xsend, "low").wait_send()
    for ti, ref in enumerate(
        (
            wb.at[pl.ds(0, n - 1), pl.ds(0, wch)],
            wa.at[pl.ds(0, (n - 1) * ks)],
            wc.at[pl.ds(0, (n - 1) * ks)],
            wd.at[pl.ds(0, n - 1)],
        )
    ):
        pltpu.make_async_remote_copy(
            src_ref=ref,
            dst_ref=ref,
            send_sem=ring_send.at[ti],
            recv_sem=ring_recv.at[0],
            device_id=right,
            device_id_type=MESH,
        ).wait_send()


def fits(mesh, args):
    n = mesh.shape["fs"]
    rows, d = args[0].shape
    ks = args[1].shape[0]
    wch = args[1].shape[1] // 2
    nc = args[5].shape[1]
    ff = args[7].shape[1] // 2
    return (
        mesh.shape["rep"] == 2
        and mesh.shape["tp"] == 2
        and n % 2 == 0
        and n >= 8
        and ks % 128 == 0
        and nc == 256
        and wch % 128 == 0
        and ff % 256 == 0
        and wch <= rows
        and ff <= 4 * rows
        and ff <= 3 * wch
        and ks <= rows
        and rows % SEQ == 0
        and 2 * SEQ <= rows <= 8 * SEQ
    )


def fused(mesh, *args):
    (
        tokens,
        outer_weight,
        inner_weight,
        value_weight,
        conv_taps,
        mix_out,
        norm_first,
        up_weight,
        down_weight,
        norm_second,
    ) = args
    n = mesh.shape["fs"]
    rows, d = tokens.shape
    ks = outer_weight.shape[0]
    wch = outer_weight.shape[1] // 2
    ff = up_weight.shape[1] // 2
    nc = mix_out.shape[1]
    both = 2 * rows
    anywhere = pl.BlockSpec(memory_space=pl.ANY)
    vmem = pl.BlockSpec(memory_space=pltpu.VMEM)
    messages = 4 * (2 * n - 2)
    pairs = 2 * n + 9 + 2 * (rows // SEQ)
    crosses = 2 * n + 5 + 2 * (rows // SEQ)
    return pl.pallas_call(
        functools.partial(layer_kernel, n),
        out_shape=pltpu.VMEM((rows, d), BF),
        in_specs=[
            anywhere,
            anywhere,
            anywhere,
            anywhere,
            vmem,
            anywhere,
            vmem,
            anywhere,
            anywhere,
            vmem,
        ],
        out_specs=vmem,
        scratch_shapes=[
            pltpu.VMEM((n * ks, 3 * wch), BF),
            pltpu.VMEM((n, 2 * wch, nc), BF),
            pltpu.VMEM((n * ks, ff), BF),
            pltpu.VMEM((n, 2, ff, nc // 2), BF),
            pltpu.VMEM((2 * both, d), BF),
            pltpu.VMEM((2 * both, 3 * wch), F32),
            pltpu.VMEM((2 * both, 2 * wch), BF),
            pltpu.VMEM((n, both, nc), F32),
            pltpu.VMEM((n, both, nc), BF),
            pltpu.VMEM((n, both, nc), BF),
            pltpu.VMEM((n, rows, nc), BF),
            pltpu.VMEM((n, rows, nc), BF),
            pltpu.VMEM((2 * both, d), BF),
            pltpu.VMEM((2 * both, ff), BF),
            pltpu.VMEM((4, rows, 128), F32),
            pltpu.SemaphoreType.DMA((8,)),
            pltpu.SemaphoreType.DMA((4,)),
            pltpu.SemaphoreType.DMA((messages,)),
            pltpu.SemaphoreType.DMA((5,)),
            pltpu.SemaphoreType.DMA((pairs,)),
            pltpu.SemaphoreType.DMA((5,)),
            pltpu.SemaphoreType.DMA((crosses,)),
        ],
        compiler_params=pltpu.CompilerParams(
            collective_id=0, has_side_effects=True, vmem_limit_bytes=62 * 2**20
        ),
        name="layer",
    )(
        tokens,
        outer_weight,
        inner_weight,
        value_weight,
        conv_taps,
        mix_out,
        norm_first.reshape(1, d),
        up_weight,
        down_weight,
        norm_second.reshape(1, d),
    )


def solution(mesh):
    def body(*args):
        return fused(mesh, *args) if fits(mesh, args) else local(*args)

    return jax.shard_map(
        body,
        mesh=mesh,
        in_specs=(
            P(("rep", "fs", "tp"), None),
            P("fs", "tp"),
            P("fs", "tp"),
            P("fs", "tp"),
            P(None, "tp"),
            P("tp", "fs"),
            P(),
            P("fs", "tp"),
            P("tp", "fs"),
            P(),
        ),
        out_specs=P(("rep", "fs", "tp"), None),
        check_vma=False,
    )
```

```python
import functools

import jax
import jax.numpy as jnp
from jax import lax
from jax.experimental import pallas as pl
from jax.experimental.pallas import tpu as pltpu
from jax.sharding import PartitionSpec as P

SEQ = 128


residual_scale = 2.0**0.25
norm_epsilon = 1e-05


def layer_norm(values, scaling):
    center = values - jnp.mean(values, axis=-1, keepdims=True)
    spread = jnp.mean(center * center, axis=-1, keepdims=True)
    return center * lax.rsqrt(spread + norm_epsilon) * scaling


def short_conv(product, conv_taps):
    places = jnp.arange(product.shape[0], dtype=jnp.int32) % SEQ
    blank = jnp.zeros((1, product.shape[1]), jnp.float32)
    before = jnp.concatenate([blank, product[:-1]], axis=0)
    after = jnp.concatenate([product[1:], blank], axis=0)
    before = jnp.where((places > 0)[:, None], before, 0.0)
    after = jnp.where((places < SEQ - 1)[:, None], after, 0.0)
    return conv_taps[0] * before + conv_taps[1] * product + conv_taps[2] * after


def local(
    tokens,
    outer_weight,
    inner_weight,
    value_weight,
    conv_taps,
    mix_out,
    norm_first,
    up_weight,
    down_weight,
    norm_second,
):
    grouped = lax.all_gather(tokens, "tp", axis=0, tiled=True)
    outer_bf = outer_weight.astype(jnp.bfloat16)
    inner_bf = inner_weight.astype(jnp.bfloat16)
    value_bf = value_weight.astype(jnp.bfloat16)
    outer_full, inner_full, value_full = (
        lax.all_gather(outer_bf, "fs", axis=0, tiled=True),
        lax.all_gather(inner_bf, "fs", axis=0, tiled=True),
        lax.all_gather(value_bf, "fs", axis=0, tiled=True),
    )
    outer = jnp.dot(grouped, outer_full, preferred_element_type=jnp.float32)
    inner = jnp.dot(grouped, inner_full, preferred_element_type=jnp.float32)
    value = jnp.dot(grouped, value_full, preferred_element_type=jnp.float32)
    mixed = (outer * short_conv(inner * value, conv_taps)).astype(jnp.bfloat16)
    mixout_full = lax.all_gather(mix_out.astype(jnp.bfloat16), "fs", axis=1, tiled=True)
    selected = mixed
    mixing = lax.psum_scatter(
        jnp.dot(selected, mixout_full, preferred_element_type=jnp.float32).astype(jnp.bfloat16),
        "tp",
        scatter_dimension=0,
        tiled=True,
    ).astype(jnp.float32)
    first = layer_norm(residual_scale * tokens.astype(jnp.float32) + mixing, norm_first).astype(
        jnp.bfloat16
    )
    grouped_first = lax.all_gather(first, "tp", axis=0, tiled=True)
    upward_bf = up_weight.astype(jnp.bfloat16)
    upward_full = lax.all_gather(upward_bf, "fs", axis=0, tiled=True)
    raised = jnp.dot(grouped_first, upward_full, preferred_element_type=jnp.float32)
    raised = jax.nn.relu(raised)
    hidden = (raised * raised).astype(jnp.bfloat16)
    down_full = lax.all_gather(down_weight.astype(jnp.bfloat16), "fs", axis=1, tiled=True)
    selected = hidden
    lowered = lax.psum_scatter(
        jnp.dot(selected, down_full, preferred_element_type=jnp.float32).astype(jnp.bfloat16),
        "tp",
        scatter_dimension=0,
        tiled=True,
    ).astype(jnp.float32)
    return layer_norm(residual_scale * first.astype(jnp.float32) + lowered, norm_second).astype(
        jnp.bfloat16
    )


MESH = pl.DeviceIdType.MESH
BF = jnp.bfloat16
F32 = jnp.float32


def dot(a, b):
    return jnp.dot(a, b, preferred_element_type=F32)


def layer_kernel(
    n,
    tokens_hbm,
    outer_hbm,
    inner_hbm,
    value_hbm,
    taps_hbm,
    mix_hbm,
    norm1_hbm,
    up_hbm,
    down_hbm,
    norm2_hbm,
    out_ref,
    wa,
    wb,
    wc,
    wd,
    tok,
    acc,
    mixed,
    own,
    psend,
    precv,
    xsend,
    xrecv,
    fst,
    hid,
    stats,
    taps_ref,
    norm1_ref,
    norm2_ref,
    load_sem,
    ring_send,
    ring_recv,
    tp_send,
    tp_recv,
    x_send,
    x_recv,
):
    half = n // 2
    r = lax.axis_index("rep")
    f = lax.axis_index("fs")
    t = lax.axis_index("tp")
    rows = tokens_hbm.shape[0]
    both = 2 * rows
    d = tokens_hbm.shape[1]
    ks = outer_hbm.shape[0]
    wch = wb.shape[1] // 2
    ff = wc.shape[1]
    nc = wb.shape[2]
    OWN, TWIN, MATE, DIAG = 0, rows, 2 * rows, 3 * rows

    odd = f % 2
    pos = (1 - odd) * (f // 2) + odd * (n - 1 - f // 2)

    def at(place):
        p = (place + 2 * n) % n
        hi = p // half
        return (1 - hi) * (2 * p) + hi * (2 * (n - 1 - p) + 1)

    right = {"fs": at(pos + 1)}
    left = {"fs": at(pos - 1)}
    across = {"rep": 1 - r}
    mate = {"tp": 1 - t}

    def owners(h):
        if h == 0:
            return [f]
        if h == half:
            return [at(pos + half)]
        return [at(pos - h), at(pos + h)]

    def numbered(h):
        return [(0 if h == 0 else 2 * h - 1 + k, o) for k, o in enumerate(owners(h))]

    every = [item for h in range(half + 1) for item in numbered(h)]

    units = [((f, 0), (f, 1))]
    for h in range(1, half):
        a, b = owners(h)
        units += [((a, 0), (b, 1)), ((a, 1), (b, 0))]
    units.append(tuple((o, j) for o in owners(half) for j in range(2)))
    lane = nc // 2

    def columns(o, j):
        return pl.ds(pl.multiple_of(o * nc + j * lane, lane), lane)

    mine = pl.multiple_of(r * ff, 128)
    share_at = pl.multiple_of(r * wch, 128)
    first_down = min(ff, both)
    rest_down = ff - first_down
    loads = [
        pltpu.make_async_copy(
            src.at[:, pl.ds(share_at, wch)],
            acc.at[pl.ds(i * ks, ks), pl.ds(0, wch)],
            load_sem.at[i],
        )
        for i, src in enumerate((outer_hbm, inner_hbm, value_hbm))
    ]
    loads += [
        pltpu.make_async_copy(
            mix_hbm, own.at[0, pl.ds(0, 2 * wch)], load_sem.at[3]
        ),
        pltpu.make_async_copy(
            up_hbm.at[:, pl.ds(mine, ff)],
            acc.at[pl.ds(3 * ks, ks), pl.ds(0, ff)],
            load_sem.at[4],
        ),
        pltpu.make_async_copy(
            down_hbm.at[pl.ds(mine, first_down)],
            own.at[1, pl.ds(0, first_down)],
            load_sem.at[5],
        ),
        pltpu.make_async_copy(tokens_hbm, tok.at[pl.ds(0, rows)], load_sem.at[6]),
    ]
    smalls = [
        pltpu.make_async_copy(src, dst, load_sem.at[8 + i])
        for i, (src, dst) in enumerate(
            ((taps_hbm, taps_ref), (norm1_hbm, norm1_ref), (norm2_hbm, norm2_ref))
        )
    ]
    if rest_down:
        loads.append(
            pltpu.make_async_copy(
                down_hbm.at[pl.ds(mine + first_down, rest_down)],
                own.at[2, pl.ds(0, rest_down)],
                load_sem.at[7],
            )
        )
    for i in (3, 0, 1, 2):
        loads[i].start()

    barrier = pltpu.get_barrier_semaphore()
    for device in (right, left, across, mate):
        pl.semaphore_signal(barrier, inc=1, device_id=device, device_id_type=MESH)
    pl.semaphore_wait(barrier, 4)

    def copier(device, send_sems, recv_sems):
        made, arrivals, groups = {}, {}, {}

        def copy(key, src, dst, group, arrival=None):
            if key not in made:
                place = arrival or key
                made[key] = pltpu.make_async_remote_copy(
                    src_ref=src,
                    dst_ref=dst,
                    send_sem=send_sems.at[groups.setdefault(group, len(groups))],
                    recv_sem=recv_sems.at[arrivals.setdefault(place, len(arrivals))],
                    device_id=device,
                    device_id_type=MESH,
                )
            return made[key]

        def whole(ref, group, arrival=None):
            return pltpu.make_async_remote_copy(
                src_ref=ref,
                dst_ref=ref,
                send_sem=send_sems.at[groups.get(group, 0)],
                recv_sem=recv_sems.at[arrivals.get(arrival, 0)],
                device_id=device,
                device_id_type=MESH,
            )

        return copy, whole

    mate_copy, mate_whole = copier(mate, tp_send, tp_recv)
    across_copy, across_whole = copier(across, x_send, x_recv)

    def piece(ti, which, owner):
        if ti == 0:
            u = wch // 2
            return wb.at[owner, pl.ds(pl.multiple_of(share_at + which * u, 16), u)]
        u = ks // 2
        if ti < 3:
            return (wa, wc)[ti - 1].at[pl.ds(pl.multiple_of(owner * ks + which * u, 16), u)]
        return wd.at[owner, which]

    per = 4 * half - 2
    index = {}
    for h in range(1, half + 1):
        for kind in ("Rq", "Rp", "Lq", "Lp"):
            if h == half and kind in ("Rp", "Lq"):
                continue
            index[kind, h] = len(index)

    copies = {}

    def message(ti, kind, h):
        key = (ti, kind, h)
        if key not in copies:
            which = int(kind[1] == "p")
            if kind[0] == "R":
                src, device = at(pos - (h - 1)), right
            else:
                src, device = at(pos + (h - 1)), left
            i = ti * per + index[kind, h]
            ref = piece(ti, which, src)
            copies[key] = pltpu.make_async_remote_copy(
                src_ref=ref,
                dst_ref=ref,
                send_sem=ring_send.at[ti],
                recv_sem=ring_recv.at[i],
                device_id=device,
                device_id_type=MESH,
            )
        return copies[key]

    def send(ti, kind, h):
        if ti < 4 and (kind, h) in index:
            message(ti, kind, h).start()

    def got(ti, kind, h):
        message(ti, kind, h).wait_recv()

    def event(ti, h, which):
        if which == 0:
            got(ti, "Rq", h)
            send(ti, "Rq", h + 1)
            if h == half:
                send(ti + 1, "Rp", 1)
            got(ti, "Lp", h)
            send(ti, "Lp", h + 1)
            if h == half:
                send(ti + 1, "Lq", 1)
        else:
            got(ti, "Rp", h)
            if h + 1 < half:
                send(ti, "Rp", h + 1)
            else:
                send(ti + 1, "Rq", 1)
            got(ti, "Lq", h)
            if h + 1 < half:
                send(ti, "Lq", h + 1)
            else:
                send(ti + 1, "Lp", 1)

    def events(ti):
        out = []
        for h in range(1, half + 1):
            out.append((ti, h, 0))
            if h < half:
                out.append((ti, h, 1))
        return out

    def block_of(o):
        return pl.ds(pl.multiple_of(o * ks, 128), ks)

    def twin_tokens(k, o):
        return across_copy(
            ("tok", k),
            tokens_hbm.at[:, block_of(o)],
            tok.at[pl.ds(TWIN, rows), block_of(o)],
            "tok",
        )

    def diag_tokens(k, o):
        return mate_copy(
            ("tok", k),
            tok.at[pl.ds(TWIN, rows), block_of(o)],
            tok.at[pl.ds(DIAG, rows), block_of(o)],
            "tok",
        )

    share = mate_copy("share", tokens_hbm, tok.at[pl.ds(MATE, rows)], "tok")
    for k, o in every:
        twin_tokens(k, o).start()
    loads[3].wait()
    wb[f] = own[0, pl.ds(0, 2 * wch)].astype(BF)
    send(0, "Rq", 1)
    send(0, "Lp", 1)
    send(0, "Rp", 1)
    send(0, "Lq", 1)
    for load in loads[4:] + smalls:
        load.start()
    share.start()
    for i in range(3):
        loads[i].wait()
        wa[pl.ds(pl.multiple_of(f * ks, 16), ks), pl.ds(i * wch, wch)] = acc[
            pl.ds(i * ks, ks), pl.ds(0, wch)
        ].astype(BF)
    loads[4].wait()
    wc[pl.ds(pl.multiple_of(f * ks, 16), ks), :] = acc[
        pl.ds(3 * ks, ks), pl.ds(0, ff)
    ].astype(BF)
    loads[5].wait()
    for j in range(2):
        wd[f, j, pl.ds(0, first_down)] = own[
            1, pl.ds(0, first_down), pl.ds(j * lane, lane)
        ].astype(BF)
    if rest_down:
        loads[7].wait()
        for j in range(2):
            wd[f, j, pl.ds(first_down, rest_down)] = own[
                2, pl.ds(0, rest_down), pl.ds(j * lane, lane)
            ].astype(BF)
    for load in [loads[6]] + smalls:
        load.wait()
    share.wait_recv()

    tn = 256
    seq = SEQ
    pieces = rows // seq
    most = pieces - 1
    EARLY, LATE, ALL = (0, most * seq), (most * seq, seq), (0, rows)

    def cross_wb(h):
        for k, o in numbered(h):
            ref = wb.at[o, pl.ds(share_at, wch)]
            across_copy(("wb", k), ref, ref, "wb", "wb").start()

    def relay_tokens(h):
        for k, o in numbered(h):
            twin_tokens(k, o).wait_recv()
            diag_tokens(k, o).start()

    def project(h, base, part, sides=2):
        who = owners(h)
        start, count = part

        def unit(i, _):
            m = pl.ds(pl.multiple_of(i % sides * MATE + base + start, 16), count)
            c = pl.ds(pl.multiple_of(i // sides * wch, 128), wch)
            total = None
            for o in who:
                w = wa[pl.ds(pl.multiple_of(o * ks, 16), ks), c]
                term = dot(tok[m, block_of(o)], w)
                total = term if total is None else total + term
            if h == 0:
                acc[m, c] = total
            else:
                acc[m, c] += total
            return 0

        lax.fori_loop(0, sides * 3, unit, 0)

    def project_near(h):
        project(h, OWN, ALL)

    def take_diag_tokens(h):
        for k, o in numbered(h):
            diag_tokens(k, o).wait_recv()

    def project_far(h):
        take_diag_tokens(h)
        project(h, TWIN, ALL)

    def mix(base, part, sides=2):
        start, count = part
        tc = 128
        seqs = count // seq

        def unit(i, _):
            j = i % (sides * seqs)
            m = pl.ds(
                pl.multiple_of(base + j // seqs * MATE + start + j % seqs * seq, seq), seq
            )
            c = pl.multiple_of(i // (sides * seqs) * tc, tc)
            o = acc[m, pl.ds(c, tc)]
            p = (
                acc[m, pl.ds(pl.multiple_of(wch + c, tc), tc)]
                * acc[m, pl.ds(pl.multiple_of(2 * wch + c, tc), tc)]
            )
            place = lax.broadcasted_iota(jnp.int32, p.shape, 0)
            before = jnp.where(place > 0, pltpu.roll(p, 1, 0), 0.0)
            after = jnp.where(place < seq - 1, pltpu.roll(p, seq - 1, 0), 0.0)
            taps = taps_ref[:, pl.ds(pl.multiple_of(share_at + c, tc), tc)]
            conv = taps[0:1] * before + taps[1:2] * p + taps[2:3] * after
            mixed[m, pl.ds(pl.multiple_of(share_at + c, tc), tc)] = (o * conv).astype(BF)
            return 0

        lax.fori_loop(0, sides * seqs * (wch // tc), unit, 0)

    def raise_part(size, start, x_base, acc_base, hs, new, final):
        who = [o for h in hs for o in owners(h)]
        tiles = ff // tn

        def unit(i, _):
            side = i % 2
            c = pl.ds(pl.multiple_of(i // 2 * tn, tn), tn)
            x_row = pl.multiple_of(x_base + side * MATE + start, 16)
            total = None
            for o in who:
                x = fst[pl.ds(x_row, size), block_of(o)]
                term = dot(x, wc[pl.ds(pl.multiple_of(o * ks, 16), ks), c])
                total = term if total is None else total + term
            span = pl.ds(pl.multiple_of(acc_base + side * rows + start, 16), size)
            if not new:
                total = total + acc[span, c]
            if final:
                total = jnp.maximum(total, 0.0)
                hid[pl.ds(x_row, size), c] = (total * total).astype(BF)
            else:
                acc[span, c] = total
            return 0

        lax.fori_loop(0, 2 * tiles, unit, 0)

    def raise_near(h):
        raise_part(rows, 0, OWN, 0, [h], h == 0, h == half)

    def raise_far(part):
        start, count = part
        for p in range(start // seq, (start + count) // seq):
            diag_first(p).wait_recv()
        raise_part(count, start, TWIN, both, range(half + 1), True, True)

    def send_mixed(p):
        for there, here in ((TWIN, OWN), (DIAG, MATE)):
            across_copy(
                ("mixed", there, p),
                mixed.at[pl.ds(there + p * seq, seq), pl.ds(share_at, wch)],
                mixed.at[pl.ds(here + p * seq, seq), pl.ds(share_at, wch)],
                "mixed",
                ("mixed", p),
            ).start()

    def mix_sums(p):
        span = pl.ds(p * seq, seq)
        return mate_copy(("mix", p), psend.at[:, span], precv.at[:, span], "mix")

    def mixout(p):
        span = pl.ds(p * seq, seq)
        if p == 0:
            across_whole(wb.at[pl.ds(0, n - 1), pl.ds(0, wch)], "wb", "wb").wait_recv()
        across_whole(
            mixed.at[pl.ds(0, 2 * seq), pl.ds(0, wch)], "mixed", ("mixed", p)
        ).wait_recv()

        def theirs(b, _):
            psend[b, span] = dot(mixed[pl.ds(MATE + p * seq, seq), :], wb[b]).astype(BF)
            return 0

        lax.fori_loop(0, n, theirs, 0)
        mix_sums(p).start()

        def ours(b, _):
            own[b, span] = dot(mixed[pl.ds(OWN + p * seq, seq), :], wb[b])
            return 0

        lax.fori_loop(0, n, ours, 0)

    def far_block(u, part):
        span = pl.ds(rows + part[0], part[1])
        return mate_copy(("low", u, part), psend.at[u, span], precv.at[u, span], "low")

    def near_group(u):
        return max(u - (n - 3), 0)

    def near_block(u):
        span = pl.ds(0, rows)
        return mate_copy(
            ("low", u), psend.at[u, span], precv.at[u, span], "low", ("low", near_group(u))
        )

    def across_block(u, part):
        span = pl.ds(*part)
        return across_copy(("low", u, part), xsend.at[u, span], xrecv.at[u, span], "low")

    def down(u):
        return jnp.concatenate([wd[o, j] for o, j in units[u]], axis=1)

    def lower_far(u, part):
        start, count = part
        span = pl.ds(rows + start, count)
        psend[u, span] = dot(hid[pl.ds(DIAG + start, count), :], down(u)).astype(BF)
        far_block(u, part).start()
        own[u, span] = dot(hid[pl.ds(TWIN + start, count), :], down(u))

    def low_pass(u, part):
        start, count = part
        far_block(u, part).wait_recv()
        span = pl.ds(rows + start, count)
        xsend[u, pl.ds(start, count)] = (own[u, span] + precv[u, span].astype(F32)).astype(BF)
        across_block(u, part).start()

    def lower_near(u):
        span = pl.ds(0, rows)
        psend[u, span] = dot(hid[pl.ds(MATE, rows), :], down(u)).astype(BF)
        near_block(u).start()
        own[u, span] = dot(hid[pl.ds(OWN, rows), :], down(u))

    lowered = [[ALL] if 3 <= u < n - 1 else [EARLY, LATE] for u in range(n)]

    def norm(base_ref, gain_ref, dest_ref, start, count):
        tm = 32

        def unit(i, _):
            m = pl.multiple_of(start + i * tm, tm)
            parts = []
            for b in range(n):
                part = (
                    residual_scale
                    * base_ref[pl.ds(m, tm), pl.ds(b * nc, nc)].astype(F32)
                    + own[b, pl.ds(m, tm)]
                )
                parts.append(part + precv[b, pl.ds(m, tm)].astype(F32))
            total = parts[0]
            for b in range(1, n):
                total = total + parts[b]
            mean = jnp.sum(total, axis=-1, keepdims=True) / d
            parts = [p - mean for p in parts]
            square = parts[0] * parts[0]
            for b in range(1, n):
                square = square + parts[b] * parts[b]
            spread = jnp.sum(square, axis=-1, keepdims=True) / d
            scale = lax.rsqrt(spread + norm_epsilon)
            for b in range(n):
                cols = pl.ds(b * nc, nc)
                dest_ref[pl.ds(m, tm), cols] = (
                    parts[b] * scale * gain_ref[:, cols]
                ).astype(BF)
            return 0

        lax.fori_loop(0, count // tm, unit, 0)

    tm = SEQ
    C, D, Q, S = range(4)

    def add_near(first, count):
        def unit(i, _):
            m = pl.ds(pl.multiple_of(i * 32, 32), 32)
            for u in range(first, first + count):
                for i, place in enumerate(units[u]):
                    part = pl.ds(i * lane, lane)
                    own[u, m, part] = (
                        residual_scale * fst[m, columns(*place)].astype(F32)
                        + own[u, m, part]
                        + precv[u, m, part].astype(F32)
                    )
            return 0

        lax.fori_loop(0, rows // 32, unit, 0)

    def add_across(u):
        for part in lowered[u]:
            across_block(u, part).wait_recv()

        def unit(i, _):
            m = pl.ds(pl.multiple_of(i * tm, tm), tm)
            x = own[u, m] + xrecv[u, m].astype(F32)
            own[u, m] = x
            lanes = x[:, :lane] + x[:, lane:]
            stats[S, m] = lanes if u == 0 else stats[S, m] + lanes
            return 0

        lax.fori_loop(0, rows // tm, unit, 0)

    def center():
        def unit(i, _):
            m = pl.ds(pl.multiple_of(i * tm, tm), tm)
            c = jnp.sum(stats[S, m], axis=-1, keepdims=True) / ((n - 1) * nc)
            shift = square = None
            for u in range(n - 1):
                x = own[u, m] - c
                y = x * x
                lanes, squares = x[:, :lane] + x[:, lane:], y[:, :lane] + y[:, lane:]
                shift = lanes if shift is None else shift + lanes
                square = squares if square is None else square + squares
            stats[C, m] = jnp.broadcast_to(c, (tm, lane))
            stats[D, m] = shift
            stats[Q, m] = square
            return 0

        lax.fori_loop(0, rows // tm, unit, 0)

    def finish(part):
        start, count = part
        tail = n - 1
        across_block(tail, part).wait_recv()

        def measure(i, _):
            m = pl.ds(pl.multiple_of(start + i * tm, tm), tm)
            value = own[tail, m] + xrecv[tail, m].astype(F32)
            own[tail, m] = value
            c = stats[C, m]
            x, y = value[:, :lane] - c, value[:, lane:] - c
            shift = jnp.sum(stats[D, m] + (x + y), axis=-1, keepdims=True) / d
            square = jnp.sum(stats[Q, m] + (x * x + y * y), axis=-1, keepdims=True) / d
            spread = jnp.maximum(square - shift * shift, 0.0)
            stats[C, m] = c + shift
            stats[S, m] = jnp.broadcast_to(lax.rsqrt(spread + norm_epsilon), (tm, lane))
            return 0

        lax.fori_loop(0, count // tm, measure, 0)

        def apply(i, _):
            m = pl.ds(pl.multiple_of(start + i * 32, 32), 32)
            mean, scale = stats[C, m], stats[S, m]
            for u in range(n):
                for i, place in enumerate(units[u]):
                    cols = columns(*place)
                    value = own[u, m, pl.ds(i * lane, lane)]
                    out_ref[m, cols] = ((value - mean) * scale * norm2_ref[:, cols]).astype(BF)
            return 0

        lax.fori_loop(0, count // 32, apply, 0)

    def near_first(p):
        return mate_copy(
            ("near", p),
            fst.at[pl.ds(p * seq, seq)],
            fst.at[pl.ds(MATE + p * seq, seq)],
            "near",
            "near",
        )

    def twin_first(p):
        return across_copy(
            ("twin", p),
            fst.at[pl.ds(p * seq, seq)],
            fst.at[pl.ds(TWIN + p * seq, seq)],
            "first",
        )

    def diag_first(p):
        return mate_copy(
            ("diag", p),
            fst.at[pl.ds(TWIN + p * seq, seq)],
            fst.at[pl.ds(DIAG + p * seq, seq)],
            "diag",
        )

    def take_near_sums(first, count):
        mate_whole(
            precv.at[pl.ds(first, count), pl.ds(0, rows)], "low", ("low", near_group(first))
        ).wait_recv()
        add_near(first, count)

    def make_first(p):
        mix_sums(p).wait_recv()
        norm(tok, norm1_ref, fst, p * seq, seq)
        twin_first(p).start()
        near_first(p).start()

    def take_near():
        mate_whole(fst.at[pl.ds(MATE, rows)], "near", "near").wait_recv()

    def relay_first(p):
        twin_first(p).wait_recv()
        diag_first(p).start()

    def free_sends():
        mate_whole(psend.at[:, pl.ds(0, rows)], "mix").wait_send()

    plan = {}

    def after(ti, h, which, *work):
        plan.setdefault((ti, h, which), []).extend(work)

    def do(function, *values):
        return lambda: function(*values)

    last = half - 1

    for h in range(1, half):
        after(0, h, 1, do(cross_wb, h))
    after(0, half, 0, do(cross_wb, half))
    after(0, half, 0, do(relay_tokens, 0), do(project_near, 0), do(project_far, 0))
    for h in range(1, half):
        after(1, h, 0, do(relay_tokens, h))
        after(1, h, 1, do(project_near, h), do(project_far, h))
    after(1, last, 0, do(relay_tokens, half))
    after(1, half, 0, do(take_diag_tokens, half))
    after(1, half, 0, do(project, half, TWIN, EARLY), do(mix, TWIN, EARLY))
    for p in range(most):
        after(1, half, 0, do(send_mixed, p))
    after(1, half, 0, do(project, half, TWIN, LATE), do(mix, TWIN, LATE), do(send_mixed, most))
    after(1, half, 0, do(project_near, half), do(mix, OWN, ALL))
    after(2, 1, 0, do(mixout, 0))
    after(2, 1, 1, do(make_first, 0), do(mixout, 1), do(make_first, 1))
    for p in range(2, pieces):
        after(2, 2, 0, do(mixout, p), do(make_first, p))
    after(2, 2, 1, do(take_near), do(raise_near, 0), do(raise_near, 1))
    after(2, 3, 0, do(raise_near, 2), do(free_sends))
    for h in range(3, half):
        after(2, h, 1, do(raise_near, h))
    after(2, last, 1, do(relay_first, 0))
    after(2, half, 0, do(raise_near, half), do(lower_near, 0))
    for p in range(1, most):
        after(2, half, 0, do(relay_first, p))
    after(2, half, 0, do(raise_far, EARLY))
    after(3, 1, 0, do(lower_far, 0, EARLY), do(lower_far, 1, EARLY))
    after(3, 1, 0, do(low_pass, 0, EARLY), do(low_pass, 1, EARLY), do(relay_first, most))
    after(3, 1, 1, do(lower_far, 2, EARLY), do(low_pass, 2, EARLY), do(raise_far, LATE))
    for u in range(3):
        after(3, 1, 1, do(lower_far, u, LATE))
    for u in range(3):
        after(3, 1, 1, do(low_pass, u, LATE))
    for u in range(3, n - 1):
        e = (3, (u + 1) // 2, (u + 1) % 2)
        near = u - 2 if u < n - 2 else n - 3
        after(*e, do(lower_far, u, ALL), do(lower_near, near), do(low_pass, u, ALL))
    after(3, last, 0, do(lower_near, n - 4))
    after(3, last, 1, do(lower_near, n - 2))
    after(3, last, 1, do(take_near_sums, 0, n - 2))
    for u in range(n - 3):
        after(3, last, 1, do(add_across, u))
    for work in (lower_far, low_pass):
        after(3, half, 0, do(work, n - 1, EARLY), do(work, n - 1, LATE))
    after(3, half, 0, do(lower_near, n - 1), do(take_near_sums, n - 2, 1))
    for u in range(n - 3, n - 1):
        after(3, half, 0, do(add_across, u))
    after(3, half, 0, do(center), do(take_near_sums, n - 1, 1), do(finish, EARLY))
    after(3, half, 0, do(finish, LATE))

    for ti in range(4):
        for e in events(ti):
            event(*e)
            for work in plan.get(e, ()):
                work()

    mate_whole(tok.at[pl.ds(0, both)], "tok").wait_send()
    for group in ("near", "diag"):
        mate_whole(fst.at[pl.ds(0, rows)], group).wait_send()
    mate_whole(psend, "low").wait_send()
    across_whole(tok.at[pl.ds(0, rows)], "tok").wait_send()
    across_whole(wb.at[pl.ds(0, n - 1), pl.ds(0, wch)], "wb").wait_send()
    across_whole(mixed.at[pl.ds(0, both), pl.ds(0, wch)], "mixed").wait_send()
    across_whole(fst.at[pl.ds(0, rows)], "first").wait_send()
    across_whole(xsend, "low").wait_send()
    for ti, ref in enumerate(
        (
            wb.at[pl.ds(0, n - 1), pl.ds(0, wch)],
            wa.at[pl.ds(0, (n - 1) * ks)],
            wc.at[pl.ds(0, (n - 1) * ks)],
            wd.at[pl.ds(0, n - 1)],
        )
    ):
        pltpu.make_async_remote_copy(
            src_ref=ref,
            dst_ref=ref,
            send_sem=ring_send.at[ti],
            recv_sem=ring_recv.at[0],
            device_id=right,
            device_id_type=MESH,
        ).wait_send()


def fits(mesh, args):
    n = mesh.shape["fs"]
    rows, d = args[0].shape
    ks = args[1].shape[0]
    wch = args[1].shape[1] // 2
    nc = args[5].shape[1]
    ff = args[7].shape[1] // 2
    return (
        mesh.shape["rep"] == 2
        and mesh.shape["tp"] == 2
        and n % 2 == 0
        and n >= 8
        and ks % 128 == 0
        and nc == 256
        and wch % 128 == 0
        and ff % 256 == 0
        and wch <= rows
        and ff <= 4 * rows
        and ff <= 3 * wch
        and ks <= rows
        and rows % SEQ == 0
        and 2 * SEQ <= rows <= 8 * SEQ
    )


def fused(mesh, *args):
    (
        tokens,
        outer_weight,
        inner_weight,
        value_weight,
        conv_taps,
        mix_out,
        norm_first,
        up_weight,
        down_weight,
        norm_second,
    ) = args
    n = mesh.shape["fs"]
    rows, d = tokens.shape
    ks = outer_weight.shape[0]
    wch = outer_weight.shape[1] // 2
    ff = up_weight.shape[1] // 2
    nc = mix_out.shape[1]
    both = 2 * rows
    anywhere = pl.BlockSpec(memory_space=pl.ANY)
    vmem = pl.BlockSpec(memory_space=pltpu.VMEM)
    messages = 4 * (2 * n - 2)
    pairs = 2 * n + 9 + 2 * (rows // SEQ)
    crosses = 2 * n + 5 + 2 * (rows // SEQ)
    return pl.pallas_call(
        functools.partial(layer_kernel, n),
        out_shape=pltpu.VMEM((rows, d), BF),
        in_specs=[anywhere] * 10,
        out_specs=vmem,
        scratch_shapes=[
            pltpu.VMEM((n * ks, 3 * wch), BF),
            pltpu.VMEM((n, 2 * wch, nc), BF),
            pltpu.VMEM((n * ks, ff), BF),
            pltpu.VMEM((n, 2, ff, nc // 2), BF),
            pltpu.VMEM((2 * both, d), BF),
            pltpu.VMEM((2 * both, 3 * wch), F32),
            pltpu.VMEM((2 * both, 2 * wch), BF),
            pltpu.VMEM((n, both, nc), F32),
            pltpu.VMEM((n, both, nc), BF),
            pltpu.VMEM((n, both, nc), BF),
            pltpu.VMEM((n, rows, nc), BF),
            pltpu.VMEM((n, rows, nc), BF),
            pltpu.VMEM((2 * both, d), BF),
            pltpu.VMEM((2 * both, ff), BF),
            pltpu.VMEM((4, rows, 128), F32),
            pltpu.VMEM(conv_taps.shape, F32),
            pltpu.VMEM((1, d), F32),
            pltpu.VMEM((1, d), F32),
            pltpu.SemaphoreType.DMA((11,)),
            pltpu.SemaphoreType.DMA((4,)),
            pltpu.SemaphoreType.DMA((messages,)),
            pltpu.SemaphoreType.DMA((5,)),
            pltpu.SemaphoreType.DMA((pairs,)),
            pltpu.SemaphoreType.DMA((5,)),
            pltpu.SemaphoreType.DMA((crosses,)),
        ],
        compiler_params=pltpu.CompilerParams(
            collective_id=0, has_side_effects=True, vmem_limit_bytes=62 * 2**20
        ),
        name="layer",
    )(
        tokens,
        outer_weight,
        inner_weight,
        value_weight,
        conv_taps,
        mix_out,
        norm_first.reshape(1, d),
        up_weight,
        down_weight,
        norm_second.reshape(1, d),
    )


def solution(mesh):
    def body(*args):
        return fused(mesh, *args) if fits(mesh, args) else local(*args)

    return jax.shard_map(
        body,
        mesh=mesh,
        in_specs=(
            P(("rep", "fs", "tp"), None),
            P("fs", "tp"),
            P("fs", "tp"),
            P("fs", "tp"),
            P(None, "tp"),
            P("tp", "fs"),
            P(),
            P("fs", "tp"),
            P("tp", "fs"),
            P(),
        ),
        out_specs=P(("rep", "fs", "tp"), None),
        check_vma=False,
    )
```

```python
import functools

import jax
import jax.numpy as jnp
from jax import lax
from jax.experimental import pallas as pl
from jax.experimental.pallas import tpu as pltpu
from jax.sharding import PartitionSpec as P

SEQ = 128


residual_scale = 2.0**0.25
norm_epsilon = 1e-05


def layer_norm(values, scaling):
    center = values - jnp.mean(values, axis=-1, keepdims=True)
    spread = jnp.mean(center * center, axis=-1, keepdims=True)
    return center * lax.rsqrt(spread + norm_epsilon) * scaling


def short_conv(product, conv_taps):
    places = jnp.arange(product.shape[0], dtype=jnp.int32) % SEQ
    blank = jnp.zeros((1, product.shape[1]), jnp.float32)
    before = jnp.concatenate([blank, product[:-1]], axis=0)
    after = jnp.concatenate([product[1:], blank], axis=0)
    before = jnp.where((places > 0)[:, None], before, 0.0)
    after = jnp.where((places < SEQ - 1)[:, None], after, 0.0)
    return conv_taps[0] * before + conv_taps[1] * product + conv_taps[2] * after


def local(
    tokens,
    outer_weight,
    inner_weight,
    value_weight,
    conv_taps,
    mix_out,
    norm_first,
    up_weight,
    down_weight,
    norm_second,
):
    grouped = lax.all_gather(tokens, "tp", axis=0, tiled=True)
    outer_bf = outer_weight.astype(jnp.bfloat16)
    inner_bf = inner_weight.astype(jnp.bfloat16)
    value_bf = value_weight.astype(jnp.bfloat16)
    outer_full, inner_full, value_full = (
        lax.all_gather(outer_bf, "fs", axis=0, tiled=True),
        lax.all_gather(inner_bf, "fs", axis=0, tiled=True),
        lax.all_gather(value_bf, "fs", axis=0, tiled=True),
    )
    outer = jnp.dot(grouped, outer_full, preferred_element_type=jnp.float32)
    inner = jnp.dot(grouped, inner_full, preferred_element_type=jnp.float32)
    value = jnp.dot(grouped, value_full, preferred_element_type=jnp.float32)
    mixed = (outer * short_conv(inner * value, conv_taps)).astype(jnp.bfloat16)
    mixout_full = lax.all_gather(mix_out.astype(jnp.bfloat16), "fs", axis=1, tiled=True)
    selected = mixed
    mixing = lax.psum_scatter(
        jnp.dot(selected, mixout_full, preferred_element_type=jnp.float32).astype(jnp.bfloat16),
        "tp",
        scatter_dimension=0,
        tiled=True,
    ).astype(jnp.float32)
    first = layer_norm(residual_scale * tokens.astype(jnp.float32) + mixing, norm_first).astype(
        jnp.bfloat16
    )
    grouped_first = lax.all_gather(first, "tp", axis=0, tiled=True)
    upward_bf = up_weight.astype(jnp.bfloat16)
    upward_full = lax.all_gather(upward_bf, "fs", axis=0, tiled=True)
    raised = jnp.dot(grouped_first, upward_full, preferred_element_type=jnp.float32)
    raised = jax.nn.relu(raised)
    hidden = (raised * raised).astype(jnp.bfloat16)
    down_full = lax.all_gather(down_weight.astype(jnp.bfloat16), "fs", axis=1, tiled=True)
    selected = hidden
    lowered = lax.psum_scatter(
        jnp.dot(selected, down_full, preferred_element_type=jnp.float32).astype(jnp.bfloat16),
        "tp",
        scatter_dimension=0,
        tiled=True,
    ).astype(jnp.float32)
    return layer_norm(residual_scale * first.astype(jnp.float32) + lowered, norm_second).astype(
        jnp.bfloat16
    )


MESH = pl.DeviceIdType.MESH
BF = jnp.bfloat16
F32 = jnp.float32


def dot(a, b):
    return jnp.dot(a, b, preferred_element_type=F32)


def layer_kernel(
    n,
    tokens_hbm,
    outer_hbm,
    inner_hbm,
    value_hbm,
    taps_hbm,
    mix_hbm,
    norm1_hbm,
    up_hbm,
    down_hbm,
    norm2_hbm,
    out_ref,
    wa,
    wb,
    wc,
    wd,
    tok,
    acc,
    mixed,
    own,
    psend,
    precv,
    xsend,
    xrecv,
    fst,
    hid,
    stats,
    taps_ref,
    norm1_ref,
    norm2_ref,
    load_sem,
    ring_send,
    ring_recv,
    tp_send,
    tp_recv,
    x_send,
    x_recv,
):
    half = n // 2
    r = lax.axis_index("rep")
    f = lax.axis_index("fs")
    t = lax.axis_index("tp")
    rows = tokens_hbm.shape[0]
    both = 2 * rows
    d = tokens_hbm.shape[1]
    ks = outer_hbm.shape[0]
    wch = wb.shape[1] // 2
    ff = wc.shape[1]
    nc = wb.shape[2]
    OWN, TWIN, MATE, DIAG = 0, rows, 2 * rows, 3 * rows

    odd = f % 2
    pos = (1 - odd) * (f // 2) + odd * (n - 1 - f // 2)

    def at(place):
        p = (place + 2 * n) % n
        hi = p // half
        return (1 - hi) * (2 * p) + hi * (2 * (n - 1 - p) + 1)

    right = {"fs": at(pos + 1)}
    left = {"fs": at(pos - 1)}
    across = {"rep": 1 - r}
    mate = {"tp": 1 - t}

    def owners(h):
        if h == 0:
            return [f]
        if h == half:
            return [at(pos + half)]
        return [at(pos - h), at(pos + h)]

    def numbered(h):
        return [(0 if h == 0 else 2 * h - 1 + k, o) for k, o in enumerate(owners(h))]

    every = [item for h in range(half + 1) for item in numbered(h)]

    units = [((f, 0), (f, 1))]
    for h in range(1, half):
        a, b = owners(h)
        units += [((a, 0), (b, 1)), ((a, 1), (b, 0))]
    units.append(tuple((o, j) for o in owners(half) for j in range(2)))
    lane = nc // 2

    def columns(o, j):
        return pl.ds(pl.multiple_of(o * nc + j * lane, lane), lane)

    mine = pl.multiple_of(r * ff, 128)
    share_at = pl.multiple_of(r * wch, 128)
    first_down = min(ff, both)
    rest_down = ff - first_down
    loads = [
        pltpu.make_async_copy(
            src.at[:, pl.ds(share_at, wch)],
            acc.at[pl.ds(i * ks, ks), pl.ds(0, wch)],
            load_sem.at[i],
        )
        for i, src in enumerate((outer_hbm, inner_hbm, value_hbm))
    ]
    loads += [
        pltpu.make_async_copy(
            mix_hbm, own.at[0, pl.ds(0, 2 * wch)], load_sem.at[3]
        ),
        pltpu.make_async_copy(
            up_hbm.at[:, pl.ds(mine, ff)],
            acc.at[pl.ds(3 * ks, ks), pl.ds(0, ff)],
            load_sem.at[4],
        ),
        pltpu.make_async_copy(
            down_hbm.at[pl.ds(mine, first_down)],
            own.at[1, pl.ds(0, first_down)],
            load_sem.at[5],
        ),
        pltpu.make_async_copy(tokens_hbm, tok.at[pl.ds(0, rows)], load_sem.at[6]),
    ]
    smalls = [
        pltpu.make_async_copy(src, dst, load_sem.at[8 + i])
        for i, (src, dst) in enumerate(
            ((taps_hbm, taps_ref), (norm1_hbm, norm1_ref), (norm2_hbm, norm2_ref))
        )
    ]
    if rest_down:
        loads.append(
            pltpu.make_async_copy(
                down_hbm.at[pl.ds(mine + first_down, rest_down)],
                own.at[2, pl.ds(0, rest_down)],
                load_sem.at[7],
            )
        )
    for i in (3, 0, 1, 2):
        loads[i].start()

    barrier = pltpu.get_barrier_semaphore()
    for device in (right, left, across, mate):
        pl.semaphore_signal(barrier, inc=1, device_id=device, device_id_type=MESH)
    loads[3].wait()
    wb[f] = own[0, pl.ds(0, 2 * wch)].astype(BF)
    pl.semaphore_wait(barrier, 4)

    def copier(device, send_sems, recv_sems):
        made, arrivals, groups = {}, {}, {}

        def copy(key, src, dst, group, arrival=None):
            if key not in made:
                place = arrival or key
                made[key] = pltpu.make_async_remote_copy(
                    src_ref=src,
                    dst_ref=dst,
                    send_sem=send_sems.at[groups.setdefault(group, len(groups))],
                    recv_sem=recv_sems.at[arrivals.setdefault(place, len(arrivals))],
                    device_id=device,
                    device_id_type=MESH,
                )
            return made[key]

        def whole(ref, group, arrival=None):
            return pltpu.make_async_remote_copy(
                src_ref=ref,
                dst_ref=ref,
                send_sem=send_sems.at[groups.get(group, 0)],
                recv_sem=recv_sems.at[arrivals.get(arrival, 0)],
                device_id=device,
                device_id_type=MESH,
            )

        return copy, whole

    mate_copy, mate_whole = copier(mate, tp_send, tp_recv)
    across_copy, across_whole = copier(across, x_send, x_recv)

    def piece(ti, which, owner):
        if ti == 0:
            u = wch // 2
            return wb.at[owner, pl.ds(pl.multiple_of(share_at + which * u, 16), u)]
        u = ks // 2
        if ti < 3:
            return (wa, wc)[ti - 1].at[pl.ds(pl.multiple_of(owner * ks + which * u, 16), u)]
        return wd.at[owner, which]

    per = 4 * half - 2
    index = {}
    for h in range(1, half + 1):
        for kind in ("Rq", "Rp", "Lq", "Lp"):
            if h == half and kind in ("Rp", "Lq"):
                continue
            index[kind, h] = len(index)

    copies = {}

    def message(ti, kind, h):
        key = (ti, kind, h)
        if key not in copies:
            which = int(kind[1] == "p")
            if kind[0] == "R":
                src, device = at(pos - (h - 1)), right
            else:
                src, device = at(pos + (h - 1)), left
            i = ti % 2 * per + index[kind, h]
            ref = piece(ti, which, src)
            copies[key] = pltpu.make_async_remote_copy(
                src_ref=ref,
                dst_ref=ref,
                send_sem=ring_send.at[ti],
                recv_sem=ring_recv.at[i],
                device_id=device,
                device_id_type=MESH,
            )
        return copies[key]

    def send(ti, kind, h):
        if ti < 4 and (kind, h) in index:
            message(ti, kind, h).start()

    def got(ti, kind, h):
        message(ti, kind, h).wait_recv()

    def event(ti, h, which):
        if which == 0:
            got(ti, "Rq", h)
            send(ti, "Rq", h + 1)
            if h == half:
                send(ti + 1, "Rp", 1)
            got(ti, "Lp", h)
            send(ti, "Lp", h + 1)
            if h == half:
                send(ti + 1, "Lq", 1)
        else:
            got(ti, "Rp", h)
            if h + 1 < half:
                send(ti, "Rp", h + 1)
            else:
                send(ti + 1, "Rq", 1)
            got(ti, "Lq", h)
            if h + 1 < half:
                send(ti, "Lq", h + 1)
            else:
                send(ti + 1, "Lp", 1)

    def events(ti):
        out = []
        for h in range(1, half + 1):
            out.append((ti, h, 0))
            if h < half:
                out.append((ti, h, 1))
        return out

    def block_of(o):
        return pl.ds(pl.multiple_of(o * ks, 128), ks)

    def twin_tokens(k, o):
        return across_copy(
            ("tok", k),
            tokens_hbm.at[:, block_of(o)],
            tok.at[pl.ds(TWIN, rows), block_of(o)],
            "tok",
        )

    def diag_tokens(k, o):
        return mate_copy(
            ("tok", k),
            tok.at[pl.ds(TWIN, rows), block_of(o)],
            tok.at[pl.ds(DIAG, rows), block_of(o)],
            "tok",
        )

    share = mate_copy("share", tokens_hbm, tok.at[pl.ds(MATE, rows)], "tok")
    send(0, "Rq", 1)
    send(0, "Lp", 1)
    send(0, "Rp", 1)
    send(0, "Lq", 1)
    for k, o in every:
        twin_tokens(k, o).start()
    for load in loads[4:] + smalls:
        load.start()
    share.start()
    for i in range(3):
        loads[i].wait()
        wa[pl.ds(pl.multiple_of(f * ks, 16), ks), pl.ds(i * wch, wch)] = acc[
            pl.ds(i * ks, ks), pl.ds(0, wch)
        ].astype(BF)
    loads[4].wait()
    wc[pl.ds(pl.multiple_of(f * ks, 16), ks), :] = acc[
        pl.ds(3 * ks, ks), pl.ds(0, ff)
    ].astype(BF)
    loads[5].wait()
    for j in range(2):
        wd[f, j, pl.ds(0, first_down)] = own[
            1, pl.ds(0, first_down), pl.ds(j * lane, lane)
        ].astype(BF)
    if rest_down:
        loads[7].wait()
        for j in range(2):
            wd[f, j, pl.ds(first_down, rest_down)] = own[
                2, pl.ds(0, rest_down), pl.ds(j * lane, lane)
            ].astype(BF)
    for load in [loads[6]] + smalls:
        load.wait()
    share.wait_recv()

    tn = 256
    seq = SEQ
    pieces = rows // seq
    most = pieces - 1
    EARLY, LATE, ALL = (0, most * seq), (most * seq, seq), (0, rows)

    def cross_wb(h):
        for k, o in numbered(h):
            ref = wb.at[o, pl.ds(share_at, wch)]
            across_copy(("wb", k), ref, ref, "wb", "wb").start()

    def relay_tokens(h):
        for k, o in numbered(h):
            twin_tokens(k, o).wait_recv()
            diag_tokens(k, o).start()

    def project(h, base, part, sides=2):
        who = owners(h)
        start, count = part

        def unit(i, _):
            m = pl.ds(pl.multiple_of(i % sides * MATE + base + start, 16), count)
            c = pl.ds(pl.multiple_of(i // sides * wch, 128), wch)
            total = None
            for o in who:
                w = wa[pl.ds(pl.multiple_of(o * ks, 16), ks), c]
                term = dot(tok[m, block_of(o)], w)
                total = term if total is None else total + term
            if h == 0:
                acc[m, c] = total
            else:
                acc[m, c] += total
            return 0

        lax.fori_loop(0, sides * 3, unit, 0)

    def project_near(h):
        project(h, OWN, ALL)

    def take_diag_tokens(h):
        for k, o in numbered(h):
            diag_tokens(k, o).wait_recv()

    def project_far(h):
        take_diag_tokens(h)
        project(h, TWIN, ALL)

    def mix(base, part, sides=2):
        start, count = part
        tc = 128
        seqs = count // seq

        def unit(i, _):
            j = i % (sides * seqs)
            m = pl.ds(
                pl.multiple_of(base + j // seqs * MATE + start + j % seqs * seq, seq), seq
            )
            c = pl.multiple_of(i // (sides * seqs) * tc, tc)
            o = acc[m, pl.ds(c, tc)]
            p = (
                acc[m, pl.ds(pl.multiple_of(wch + c, tc), tc)]
                * acc[m, pl.ds(pl.multiple_of(2 * wch + c, tc), tc)]
            )
            place = lax.broadcasted_iota(jnp.int32, p.shape, 0)
            before = jnp.where(place > 0, pltpu.roll(p, 1, 0), 0.0)
            after = jnp.where(place < seq - 1, pltpu.roll(p, seq - 1, 0), 0.0)
            taps = taps_ref[:, pl.ds(pl.multiple_of(share_at + c, tc), tc)]
            conv = taps[0:1] * before + taps[1:2] * p + taps[2:3] * after
            mixed[m, pl.ds(pl.multiple_of(share_at + c, tc), tc)] = (o * conv).astype(BF)
            return 0

        lax.fori_loop(0, sides * seqs * (wch // tc), unit, 0)

    def raise_part(size, start, x_base, acc_base, hs, new, final):
        who = [o for h in hs for o in owners(h)]
        tiles = ff // tn

        def unit(i, _):
            side = i % 2
            c = pl.ds(pl.multiple_of(i // 2 * tn, tn), tn)
            x_row = pl.multiple_of(x_base + side * MATE + start, 16)
            total = None
            for o in who:
                x = fst[pl.ds(x_row, size), block_of(o)]
                term = dot(x, wc[pl.ds(pl.multiple_of(o * ks, 16), ks), c])
                total = term if total is None else total + term
            span = pl.ds(pl.multiple_of(acc_base + side * rows + start, 16), size)
            if not new:
                total = total + acc[span, c]
            if final:
                total = jnp.maximum(total, 0.0)
                hid[pl.ds(x_row, size), c] = (total * total).astype(BF)
            else:
                acc[span, c] = total
            return 0

        lax.fori_loop(0, 2 * tiles, unit, 0)

    def raise_near(h):
        raise_part(rows, 0, OWN, 0, [h], h == 0, h == half)

    def raise_far(part):
        start, count = part
        for p in range(start // seq, (start + count) // seq):
            diag_first(p).wait_recv()
        raise_part(count, start, TWIN, both, range(half + 1), True, True)

    def send_mixed(p):
        for there, here in ((TWIN, OWN), (DIAG, MATE)):
            across_copy(
                ("mixed", there, p),
                mixed.at[pl.ds(there + p * seq, seq), pl.ds(share_at, wch)],
                mixed.at[pl.ds(here + p * seq, seq), pl.ds(share_at, wch)],
                "mixed",
                ("mixed", p),
            ).start()

    def mix_sums(p):
        span = pl.ds(p * seq, seq)
        return mate_copy(("mix", p), psend.at[:, span], precv.at[:, span], "mix")

    def mixout(p):
        span = pl.ds(p * seq, seq)
        if p == 0:
            across_whole(wb.at[pl.ds(0, n - 1), pl.ds(0, wch)], "wb", "wb").wait_recv()
        across_whole(
            mixed.at[pl.ds(0, 2 * seq), pl.ds(0, wch)], "mixed", ("mixed", p)
        ).wait_recv()

        def theirs(b, _):
            psend[b, span] = dot(mixed[pl.ds(MATE + p * seq, seq), :], wb[b]).astype(BF)
            return 0

        lax.fori_loop(0, n, theirs, 0)
        mix_sums(p).start()

        def ours(b, _):
            own[b, span] = dot(mixed[pl.ds(OWN + p * seq, seq), :], wb[b])
            return 0

        lax.fori_loop(0, n, ours, 0)

    def far_block(u, part):
        span = pl.ds(rows + part[0], part[1])
        return mate_copy(("low", u, part), psend.at[u, span], precv.at[u, span], "low")

    def near_group(u):
        return max(u - (n - 3), 0)

    def near_block(u):
        span = pl.ds(0, rows)
        return mate_copy(
            ("low", u), psend.at[u, span], precv.at[u, span], "low", ("low", near_group(u))
        )

    def across_block(u, part):
        span = pl.ds(*part)
        return across_copy(("low", u, part), xsend.at[u, span], xrecv.at[u, span], "low")

    def down(u):
        return jnp.concatenate([wd[o, j] for o, j in units[u]], axis=1)

    def lower_far(u, part):
        start, count = part
        span = pl.ds(rows + start, count)
        psend[u, span] = dot(hid[pl.ds(DIAG + start, count), :], down(u)).astype(BF)
        far_block(u, part).start()
        own[u, span] = dot(hid[pl.ds(TWIN + start, count), :], down(u))

    def low_pass(u, part):
        start, count = part
        far_block(u, part).wait_recv()
        span = pl.ds(rows + start, count)
        xsend[u, pl.ds(start, count)] = (own[u, span] + precv[u, span].astype(F32)).astype(BF)
        across_block(u, part).start()

    def lower_near(u):
        span = pl.ds(0, rows)
        psend[u, span] = dot(hid[pl.ds(MATE, rows), :], down(u)).astype(BF)
        near_block(u).start()
        own[u, span] = dot(hid[pl.ds(OWN, rows), :], down(u))

    lowered = [[ALL] if 3 <= u < n - 1 else [EARLY, LATE] for u in range(n)]

    def norm(base_ref, gain_ref, dest_ref, start, count):
        tm = 32

        def unit(i, _):
            m = pl.multiple_of(start + i * tm, tm)
            parts = []
            for b in range(n):
                part = (
                    residual_scale
                    * base_ref[pl.ds(m, tm), pl.ds(b * nc, nc)].astype(F32)
                    + own[b, pl.ds(m, tm)]
                )
                parts.append(part + precv[b, pl.ds(m, tm)].astype(F32))
            total = parts[0]
            for b in range(1, n):
                total = total + parts[b]
            mean = jnp.sum(total, axis=-1, keepdims=True) / d
            parts = [p - mean for p in parts]
            square = parts[0] * parts[0]
            for b in range(1, n):
                square = square + parts[b] * parts[b]
            spread = jnp.sum(square, axis=-1, keepdims=True) / d
            scale = lax.rsqrt(spread + norm_epsilon)
            for b in range(n):
                cols = pl.ds(b * nc, nc)
                dest_ref[pl.ds(m, tm), cols] = (
                    parts[b] * scale * gain_ref[:, cols]
                ).astype(BF)
            return 0

        lax.fori_loop(0, count // tm, unit, 0)

    tm = SEQ
    C, D, Q, S = range(4)

    def add_near(first, count):
        def unit(i, _):
            m = pl.ds(pl.multiple_of(i * 32, 32), 32)
            for u in range(first, first + count):
                for i, place in enumerate(units[u]):
                    part = pl.ds(i * lane, lane)
                    own[u, m, part] = (
                        residual_scale * fst[m, columns(*place)].astype(F32)
                        + own[u, m, part]
                        + precv[u, m, part].astype(F32)
                    )
            return 0

        lax.fori_loop(0, rows // 32, unit, 0)

    def add_across(u):
        for part in lowered[u]:
            across_block(u, part).wait_recv()

        def unit(i, _):
            m = pl.ds(pl.multiple_of(i * tm, tm), tm)
            x = own[u, m] + xrecv[u, m].astype(F32)
            own[u, m] = x
            lanes = x[:, :lane] + x[:, lane:]
            stats[S, m] = lanes if u == 0 else stats[S, m] + lanes
            return 0

        lax.fori_loop(0, rows // tm, unit, 0)

    def center():
        def unit(i, _):
            m = pl.ds(pl.multiple_of(i * tm, tm), tm)
            c = jnp.sum(stats[S, m], axis=-1, keepdims=True) / ((n - 1) * nc)
            shift = square = None
            for u in range(n - 1):
                x = own[u, m] - c
                y = x * x
                lanes, squares = x[:, :lane] + x[:, lane:], y[:, :lane] + y[:, lane:]
                shift = lanes if shift is None else shift + lanes
                square = squares if square is None else square + squares
            stats[C, m] = jnp.broadcast_to(c, (tm, lane))
            stats[D, m] = shift
            stats[Q, m] = square
            return 0

        lax.fori_loop(0, rows // tm, unit, 0)

    def finish(part):
        start, count = part
        tail = n - 1
        across_block(tail, part).wait_recv()

        def measure(i, _):
            m = pl.ds(pl.multiple_of(start + i * tm, tm), tm)
            value = own[tail, m] + xrecv[tail, m].astype(F32)
            own[tail, m] = value
            c = stats[C, m]
            x, y = value[:, :lane] - c, value[:, lane:] - c
            shift = jnp.sum(stats[D, m] + (x + y), axis=-1, keepdims=True) / d
            square = jnp.sum(stats[Q, m] + (x * x + y * y), axis=-1, keepdims=True) / d
            spread = jnp.maximum(square - shift * shift, 0.0)
            stats[C, m] = c + shift
            stats[S, m] = jnp.broadcast_to(lax.rsqrt(spread + norm_epsilon), (tm, lane))
            return 0

        lax.fori_loop(0, count // tm, measure, 0)

        def apply(i, _):
            m = pl.ds(pl.multiple_of(start + i * 32, 32), 32)
            mean, scale = stats[C, m], stats[S, m]
            for u in range(n):
                for i, place in enumerate(units[u]):
                    cols = columns(*place)
                    value = own[u, m, pl.ds(i * lane, lane)]
                    out_ref[m, cols] = ((value - mean) * scale * norm2_ref[:, cols]).astype(BF)
            return 0

        lax.fori_loop(0, count // 32, apply, 0)

    def near_first(p):
        return mate_copy(
            ("near", p),
            fst.at[pl.ds(p * seq, seq)],
            fst.at[pl.ds(MATE + p * seq, seq)],
            "near",
            "near",
        )

    def twin_first(p):
        return across_copy(
            ("twin", p),
            fst.at[pl.ds(p * seq, seq)],
            fst.at[pl.ds(TWIN + p * seq, seq)],
            "first",
        )

    def diag_first(p):
        return mate_copy(
            ("diag", p),
            fst.at[pl.ds(TWIN + p * seq, seq)],
            fst.at[pl.ds(DIAG + p * seq, seq)],
            "diag",
        )

    def take_near_sums(first, count):
        mate_whole(
            precv.at[pl.ds(first, count), pl.ds(0, rows)], "low", ("low", near_group(first))
        ).wait_recv()
        add_near(first, count)

    def make_first(p):
        mix_sums(p).wait_recv()
        norm(tok, norm1_ref, fst, p * seq, seq)
        twin_first(p).start()
        near_first(p).start()

    def take_near():
        mate_whole(fst.at[pl.ds(MATE, rows)], "near", "near").wait_recv()

    def relay_first(p):
        twin_first(p).wait_recv()
        diag_first(p).start()

    def free_sends():
        mate_whole(psend.at[:, pl.ds(0, rows)], "mix").wait_send()

    plan = {}

    def after(ti, h, which, *work):
        plan.setdefault((ti, h, which), []).extend(work)

    def do(function, *values):
        return lambda: function(*values)

    last = half - 1

    for h in range(1, half):
        after(0, h, 1, do(cross_wb, h))
    after(0, half, 0, do(cross_wb, half))
    after(0, half, 0, do(relay_tokens, 0), do(project_near, 0), do(project_far, 0))
    for h in range(1, half):
        after(1, h, 0, do(relay_tokens, h))
        after(1, h, 1, do(project_near, h), do(project_far, h))
    after(1, last, 0, do(relay_tokens, half))
    after(1, half, 0, do(take_diag_tokens, half))
    after(1, half, 0, do(project, half, TWIN, EARLY), do(mix, TWIN, EARLY))
    for p in range(most):
        after(1, half, 0, do(send_mixed, p))
    after(1, half, 0, do(project, half, TWIN, LATE), do(mix, TWIN, LATE), do(send_mixed, most))
    after(1, half, 0, do(project_near, half), do(mix, OWN, ALL))
    after(2, 1, 0, do(mixout, 0))
    after(2, 1, 1, do(make_first, 0), do(mixout, 1), do(make_first, 1))
    for p in range(2, pieces):
        after(2, 2, 0, do(mixout, p), do(make_first, p))
    after(2, 2, 1, do(take_near), do(raise_near, 0), do(raise_near, 1))
    after(2, 3, 0, do(raise_near, 2), do(free_sends))
    for h in range(3, half):
        after(2, h, 1, do(raise_near, h))
    after(2, last, 1, do(relay_first, 0))
    after(2, half, 0, do(raise_near, half), do(lower_near, 0))
    for p in range(1, most):
        after(2, half, 0, do(relay_first, p))
    after(2, half, 0, do(raise_far, EARLY))
    after(3, 1, 0, do(lower_far, 0, EARLY), do(lower_far, 1, EARLY))
    after(3, 1, 0, do(low_pass, 0, EARLY), do(low_pass, 1, EARLY), do(relay_first, most))
    after(3, 1, 1, do(lower_far, 2, EARLY), do(low_pass, 2, EARLY), do(raise_far, LATE))
    for u in range(3):
        after(3, 1, 1, do(lower_far, u, LATE))
    for u in range(3):
        after(3, 1, 1, do(low_pass, u, LATE))
    for u in range(3, n - 1):
        e = (3, (u + 1) // 2, (u + 1) % 2)
        near = u - 2 if u < n - 2 else n - 3
        after(*e, do(lower_far, u, ALL), do(lower_near, near), do(low_pass, u, ALL))
    after(3, last, 0, do(lower_near, n - 4))
    after(3, last, 1, do(lower_near, n - 2))
    after(3, last, 1, do(take_near_sums, 0, n - 2))
    for u in range(n - 3):
        after(3, last, 1, do(add_across, u))
    for work in (lower_far, low_pass):
        after(3, half, 0, do(work, n - 1, EARLY), do(work, n - 1, LATE))
    after(3, half, 0, do(lower_near, n - 1), do(take_near_sums, n - 2, 1))
    for u in range(n - 3, n - 1):
        after(3, half, 0, do(add_across, u))
    after(3, half, 0, do(center), do(take_near_sums, n - 1, 1), do(finish, EARLY))
    after(3, half, 0, do(finish, LATE))

    for ti in range(4):
        for e in events(ti):
            event(*e)
            for work in plan.get(e, ()):
                work()

    mate_whole(tok.at[pl.ds(0, both)], "tok").wait_send()
    for group in ("near", "diag"):
        mate_whole(fst.at[pl.ds(0, rows)], group).wait_send()
    mate_whole(psend, "low").wait_send()
    across_whole(tok.at[pl.ds(0, rows)], "tok").wait_send()
    across_whole(wb.at[pl.ds(0, n - 1), pl.ds(0, wch)], "wb").wait_send()
    across_whole(mixed.at[pl.ds(0, both), pl.ds(0, wch)], "mixed").wait_send()
    across_whole(fst.at[pl.ds(0, rows)], "first").wait_send()
    across_whole(xsend, "low").wait_send()
    for ti, ref in enumerate(
        (
            wb.at[pl.ds(0, n - 1), pl.ds(0, wch)],
            wa.at[pl.ds(0, (n - 1) * ks)],
            wc.at[pl.ds(0, (n - 1) * ks)],
            wd.at[pl.ds(0, n - 1)],
        )
    ):
        pltpu.make_async_remote_copy(
            src_ref=ref,
            dst_ref=ref,
            send_sem=ring_send.at[ti],
            recv_sem=ring_recv.at[0],
            device_id=right,
            device_id_type=MESH,
        ).wait_send()


def fits(mesh, args):
    n = mesh.shape["fs"]
    rows, d = args[0].shape
    ks = args[1].shape[0]
    wch = args[1].shape[1] // 2
    nc = args[5].shape[1]
    ff = args[7].shape[1] // 2
    return (
        mesh.shape["rep"] == 2
        and mesh.shape["tp"] == 2
        and n % 2 == 0
        and n >= 8
        and ks % 128 == 0
        and nc == 256
        and wch % 128 == 0
        and ff % 256 == 0
        and wch <= rows
        and ff <= 4 * rows
        and ff <= 3 * wch
        and ks <= rows
        and rows % SEQ == 0
        and 2 * SEQ <= rows <= 8 * SEQ
    )


def fused(mesh, *args):
    (
        tokens,
        outer_weight,
        inner_weight,
        value_weight,
        conv_taps,
        mix_out,
        norm_first,
        up_weight,
        down_weight,
        norm_second,
    ) = args
    n = mesh.shape["fs"]
    rows, d = tokens.shape
    ks = outer_weight.shape[0]
    wch = outer_weight.shape[1] // 2
    ff = up_weight.shape[1] // 2
    nc = mix_out.shape[1]
    both = 2 * rows
    anywhere = pl.BlockSpec(memory_space=pl.ANY)
    vmem = pl.BlockSpec(memory_space=pltpu.VMEM)
    messages = 2 * (2 * n - 2)
    pairs = 2 * n + 9 + 2 * (rows // SEQ)
    crosses = 2 * n + 5 + 2 * (rows // SEQ)
    return pl.pallas_call(
        functools.partial(layer_kernel, n),
        out_shape=pltpu.VMEM((rows, d), BF),
        in_specs=[anywhere] * 10,
        out_specs=vmem,
        scratch_shapes=[
            pltpu.VMEM((n * ks, 3 * wch), BF),
            pltpu.VMEM((n, 2 * wch, nc), BF),
            pltpu.VMEM((n * ks, ff), BF),
            pltpu.VMEM((n, 2, ff, nc // 2), BF),
            pltpu.VMEM((2 * both, d), BF),
            pltpu.VMEM((2 * both, 3 * wch), F32),
            pltpu.VMEM((2 * both, 2 * wch), BF),
            pltpu.VMEM((n, both, nc), F32),
            pltpu.VMEM((n, both, nc), BF),
            pltpu.VMEM((n, both, nc), BF),
            pltpu.VMEM((n, rows, nc), BF),
            pltpu.VMEM((n, rows, nc), BF),
            pltpu.VMEM((2 * both, d), BF),
            pltpu.VMEM((2 * both, ff), BF),
            pltpu.VMEM((4, rows, 128), F32),
            pltpu.VMEM(conv_taps.shape, F32),
            pltpu.VMEM((1, d), F32),
            pltpu.VMEM((1, d), F32),
            pltpu.SemaphoreType.DMA((11,)),
            pltpu.SemaphoreType.DMA((4,)),
            pltpu.SemaphoreType.DMA((messages,)),
            pltpu.SemaphoreType.DMA((5,)),
            pltpu.SemaphoreType.DMA((pairs,)),
            pltpu.SemaphoreType.DMA((5,)),
            pltpu.SemaphoreType.DMA((crosses,)),
        ],
        compiler_params=pltpu.CompilerParams(
            collective_id=0, has_side_effects=True, vmem_limit_bytes=62 * 2**20
        ),
        name="layer",
    )(
        tokens,
        outer_weight,
        inner_weight,
        value_weight,
        conv_taps,
        mix_out,
        norm_first.reshape(1, d),
        up_weight,
        down_weight,
        norm_second.reshape(1, d),
    )


def solution(mesh):
    def body(*args):
        return fused(mesh, *args) if fits(mesh, args) else local(*args)

    return jax.shard_map(
        body,
        mesh=mesh,
        in_specs=(
            P(("rep", "fs", "tp"), None),
            P("fs", "tp"),
            P("fs", "tp"),
            P("fs", "tp"),
            P(None, "tp"),
            P("tp", "fs"),
            P(),
            P("fs", "tp"),
            P("tp", "fs"),
            P(),
        ),
        out_specs=P(("rep", "fs", "tp"), None),
        check_vma=False,
    )
```

```python
import functools

import jax
import jax.numpy as jnp
from jax import lax
from jax.experimental import pallas as pl
from jax.experimental.pallas import tpu as pltpu
from jax.sharding import PartitionSpec as P

SEQ = 128


residual_scale = 2.0**0.25
norm_epsilon = 1e-05


def layer_norm(values, scaling):
    center = values - jnp.mean(values, axis=-1, keepdims=True)
    spread = jnp.mean(center * center, axis=-1, keepdims=True)
    return center * lax.rsqrt(spread + norm_epsilon) * scaling


def short_conv(product, conv_taps):
    places = jnp.arange(product.shape[0], dtype=jnp.int32) % SEQ
    blank = jnp.zeros((1, product.shape[1]), jnp.float32)
    before = jnp.concatenate([blank, product[:-1]], axis=0)
    after = jnp.concatenate([product[1:], blank], axis=0)
    before = jnp.where((places > 0)[:, None], before, 0.0)
    after = jnp.where((places < SEQ - 1)[:, None], after, 0.0)
    return conv_taps[0] * before + conv_taps[1] * product + conv_taps[2] * after


def local(
    tokens,
    outer_weight,
    inner_weight,
    value_weight,
    conv_taps,
    mix_out,
    norm_first,
    up_weight,
    down_weight,
    norm_second,
):
    grouped = lax.all_gather(tokens, "tp", axis=0, tiled=True)
    outer_bf = outer_weight.astype(jnp.bfloat16)
    inner_bf = inner_weight.astype(jnp.bfloat16)
    value_bf = value_weight.astype(jnp.bfloat16)
    outer_full, inner_full, value_full = (
        lax.all_gather(outer_bf, "fs", axis=0, tiled=True),
        lax.all_gather(inner_bf, "fs", axis=0, tiled=True),
        lax.all_gather(value_bf, "fs", axis=0, tiled=True),
    )
    outer = jnp.dot(grouped, outer_full, preferred_element_type=jnp.float32)
    inner = jnp.dot(grouped, inner_full, preferred_element_type=jnp.float32)
    value = jnp.dot(grouped, value_full, preferred_element_type=jnp.float32)
    mixed = (outer * short_conv(inner * value, conv_taps)).astype(jnp.bfloat16)
    mixout_full = lax.all_gather(mix_out.astype(jnp.bfloat16), "fs", axis=1, tiled=True)
    selected = mixed
    mixing = lax.psum_scatter(
        jnp.dot(selected, mixout_full, preferred_element_type=jnp.float32).astype(jnp.bfloat16),
        "tp",
        scatter_dimension=0,
        tiled=True,
    ).astype(jnp.float32)
    first = layer_norm(residual_scale * tokens.astype(jnp.float32) + mixing, norm_first).astype(
        jnp.bfloat16
    )
    grouped_first = lax.all_gather(first, "tp", axis=0, tiled=True)
    upward_bf = up_weight.astype(jnp.bfloat16)
    upward_full = lax.all_gather(upward_bf, "fs", axis=0, tiled=True)
    raised = jnp.dot(grouped_first, upward_full, preferred_element_type=jnp.float32)
    raised = jax.nn.relu(raised)
    hidden = (raised * raised).astype(jnp.bfloat16)
    down_full = lax.all_gather(down_weight.astype(jnp.bfloat16), "fs", axis=1, tiled=True)
    selected = hidden
    lowered = lax.psum_scatter(
        jnp.dot(selected, down_full, preferred_element_type=jnp.float32).astype(jnp.bfloat16),
        "tp",
        scatter_dimension=0,
        tiled=True,
    ).astype(jnp.float32)
    return layer_norm(residual_scale * first.astype(jnp.float32) + lowered, norm_second).astype(
        jnp.bfloat16
    )


MESH = pl.DeviceIdType.MESH
BF = jnp.bfloat16
F32 = jnp.float32


def dot(a, b):
    return jnp.dot(a, b, preferred_element_type=F32)


def layer_kernel(
    n,
    tokens_hbm,
    outer_hbm,
    inner_hbm,
    value_hbm,
    taps_hbm,
    mix_hbm,
    norm1_hbm,
    up_hbm,
    down_hbm,
    norm2_hbm,
    out_ref,
    wa,
    wb,
    wc,
    wd,
    tok,
    acc,
    mixed,
    own,
    psend,
    precv,
    xsend,
    xrecv,
    fst,
    hid,
    stats,
    taps_ref,
    norm1_ref,
    norm2_ref,
    load_sem,
    ring_send,
    ring_recv,
    tp_send,
    tp_recv,
    x_send,
    x_recv,
):
    half = n // 2
    r = lax.axis_index("rep")
    f = lax.axis_index("fs")
    t = lax.axis_index("tp")
    rows = tokens_hbm.shape[0]
    both = 2 * rows
    d = tokens_hbm.shape[1]
    ks = outer_hbm.shape[0]
    wch = wb.shape[1] // 2
    ff = wc.shape[1]
    nc = wb.shape[2]
    OWN, TWIN, MATE, DIAG = 0, rows, 2 * rows, 3 * rows

    odd = f % 2
    pos = (1 - odd) * (f // 2) + odd * (n - 1 - f // 2)

    def at(place):
        p = (place + 2 * n) % n
        hi = p // half
        return (1 - hi) * (2 * p) + hi * (2 * (n - 1 - p) + 1)

    right = {"fs": at(pos + 1)}
    left = {"fs": at(pos - 1)}
    across = {"rep": 1 - r}
    mate = {"tp": 1 - t}

    def owners(h):
        if h == 0:
            return [f]
        if h == half:
            return [at(pos + half)]
        return [at(pos - h), at(pos + h)]

    def numbered(h):
        return [(0 if h == 0 else 2 * h - 1 + k, o) for k, o in enumerate(owners(h))]

    every = [item for h in range(half + 1) for item in numbered(h)]

    units = [((f, 0), (f, 1))]
    for h in range(1, half):
        a, b = owners(h)
        units += [((a, 0), (b, 1)), ((a, 1), (b, 0))]
    units.append(tuple((o, j) for o in owners(half) for j in range(2)))
    lane = nc // 2

    def columns(o, j):
        return pl.ds(pl.multiple_of(o * nc + j * lane, lane), lane)

    mine = pl.multiple_of(r * ff, 128)
    share_at = pl.multiple_of(r * wch, 128)
    first_down = min(ff, both)
    rest_down = ff - first_down
    loads = [
        pltpu.make_async_copy(
            src.at[:, pl.ds(share_at, wch)],
            acc.at[pl.ds(i * ks, ks), pl.ds(0, wch)],
            load_sem.at[i],
        )
        for i, src in enumerate((outer_hbm, inner_hbm, value_hbm))
    ]
    loads += [
        pltpu.make_async_copy(
            mix_hbm, own.at[0, pl.ds(0, 2 * wch)], load_sem.at[3]
        ),
        pltpu.make_async_copy(
            up_hbm.at[:, pl.ds(mine, ff)],
            acc.at[pl.ds(3 * ks, ks), pl.ds(0, ff)],
            load_sem.at[4],
        ),
        pltpu.make_async_copy(
            down_hbm.at[pl.ds(mine, first_down)],
            own.at[1, pl.ds(0, first_down)],
            load_sem.at[5],
        ),
        pltpu.make_async_copy(tokens_hbm, tok.at[pl.ds(0, rows)], load_sem.at[6]),
    ]
    smalls = [
        pltpu.make_async_copy(src, dst, load_sem.at[8 + i])
        for i, (src, dst) in enumerate(
            ((taps_hbm, taps_ref), (norm1_hbm, norm1_ref), (norm2_hbm, norm2_ref))
        )
    ]
    if rest_down:
        loads.append(
            pltpu.make_async_copy(
                down_hbm.at[pl.ds(mine + first_down, rest_down)],
                own.at[2, pl.ds(0, rest_down)],
                load_sem.at[7],
            )
        )
    for i in (3, 0, 1, 2):
        loads[i].start()

    barrier = pltpu.get_barrier_semaphore()
    for device in (right, left, across, mate):
        pl.semaphore_signal(barrier, inc=1, device_id=device, device_id_type=MESH)
    loads[3].wait()
    wb[f] = own[0, pl.ds(0, 2 * wch)].astype(BF)
    pl.semaphore_wait(barrier, 4)

    def copier(device, send_sems, recv_sems):
        made, arrivals, groups = {}, {}, {}

        def copy(key, src, dst, group, arrival=None):
            if key not in made:
                place = arrival or key
                made[key] = pltpu.make_async_remote_copy(
                    src_ref=src,
                    dst_ref=dst,
                    send_sem=send_sems.at[groups.setdefault(group, len(groups))],
                    recv_sem=recv_sems.at[arrivals.setdefault(place, len(arrivals))],
                    device_id=device,
                    device_id_type=MESH,
                )
            return made[key]

        def whole(ref, group, arrival=None):
            return pltpu.make_async_remote_copy(
                src_ref=ref,
                dst_ref=ref,
                send_sem=send_sems.at[groups.get(group, 0)],
                recv_sem=recv_sems.at[arrivals.get(arrival, 0)],
                device_id=device,
                device_id_type=MESH,
            )

        return copy, whole

    mate_copy, mate_whole = copier(mate, tp_send, tp_recv)
    across_copy, across_whole = copier(across, x_send, x_recv)

    def piece(ti, which, owner):
        if ti == 0:
            u = wch // 2
            return wb.at[owner, pl.ds(pl.multiple_of(share_at + which * u, 16), u)]
        u = ks // 2
        if ti < 3:
            return (wa, wc)[ti - 1].at[pl.ds(pl.multiple_of(owner * ks + which * u, 16), u)]
        return wd.at[owner, which]

    per = 4 * half - 2
    index = {}
    for h in range(1, half + 1):
        for kind in ("Rq", "Rp", "Lq", "Lp"):
            if h == half and kind in ("Rp", "Lq"):
                continue
            index[kind, h] = len(index)

    copies = {}

    def message(ti, kind, h):
        key = (ti, kind, h)
        if key not in copies:
            which = int(kind[1] == "p")
            if kind[0] == "R":
                src, device = at(pos - (h - 1)), right
            else:
                src, device = at(pos + (h - 1)), left
            i = ti % 2 * per + index[kind, h]
            ref = piece(ti, which, src)
            copies[key] = pltpu.make_async_remote_copy(
                src_ref=ref,
                dst_ref=ref,
                send_sem=ring_send.at[ti],
                recv_sem=ring_recv.at[i],
                device_id=device,
                device_id_type=MESH,
            )
        return copies[key]

    def send(ti, kind, h):
        if ti < 4 and (kind, h) in index:
            message(ti, kind, h).start()

    def got(ti, kind, h):
        message(ti, kind, h).wait_recv()

    def event(ti, h, which):
        if which == 0:
            got(ti, "Rq", h)
            send(ti, "Rq", h + 1)
            if h == half:
                send(ti + 1, "Rp", 1)
            got(ti, "Lp", h)
            send(ti, "Lp", h + 1)
            if h == half:
                send(ti + 1, "Lq", 1)
        else:
            got(ti, "Rp", h)
            if h + 1 < half:
                send(ti, "Rp", h + 1)
            else:
                send(ti + 1, "Rq", 1)
            got(ti, "Lq", h)
            if h + 1 < half:
                send(ti, "Lq", h + 1)
            else:
                send(ti + 1, "Lp", 1)

    def events(ti):
        out = []
        for h in range(1, half + 1):
            out.append((ti, h, 0))
            if h < half:
                out.append((ti, h, 1))
        return out

    def block_of(o):
        return pl.ds(pl.multiple_of(o * ks, 128), ks)

    def twin_tokens(k, o):
        return across_copy(
            ("tok", k),
            tokens_hbm.at[:, block_of(o)],
            tok.at[pl.ds(TWIN, rows), block_of(o)],
            "tok",
        )

    def diag_tokens(k, o):
        return mate_copy(
            ("tok", k),
            tok.at[pl.ds(TWIN, rows), block_of(o)],
            tok.at[pl.ds(DIAG, rows), block_of(o)],
            "tok",
        )

    share = mate_copy("share", tokens_hbm, tok.at[pl.ds(MATE, rows)], "tok")
    send(0, "Rq", 1)
    send(0, "Lp", 1)
    send(0, "Rp", 1)
    send(0, "Lq", 1)
    for k, o in every:
        twin_tokens(k, o).start()
    for load in loads[4:] + smalls:
        load.start()
    share.start()
    for i in range(3):
        loads[i].wait()
        wa[pl.ds(pl.multiple_of(f * ks, 16), ks), pl.ds(i * wch, wch)] = acc[
            pl.ds(i * ks, ks), pl.ds(0, wch)
        ].astype(BF)
    loads[4].wait()
    wc[pl.ds(pl.multiple_of(f * ks, 16), ks), :] = acc[
        pl.ds(3 * ks, ks), pl.ds(0, ff)
    ].astype(BF)
    loads[5].wait()
    for j in range(2):
        wd[f, j, pl.ds(0, first_down)] = own[
            1, pl.ds(0, first_down), pl.ds(j * lane, lane)
        ].astype(BF)
    if rest_down:
        loads[7].wait()
        for j in range(2):
            wd[f, j, pl.ds(first_down, rest_down)] = own[
                2, pl.ds(0, rest_down), pl.ds(j * lane, lane)
            ].astype(BF)
    for load in [loads[6]] + smalls:
        load.wait()
    share.wait_recv()

    tn = 256
    seq = SEQ
    pieces = rows // seq
    most = pieces - 1
    EARLY, LATE, ALL = (0, most * seq), (most * seq, seq), (0, rows)

    def cross_wb(h):
        for k, o in numbered(h):
            ref = wb.at[o, pl.ds(share_at, wch)]
            across_copy(("wb", k), ref, ref, "wb", "wb").start()

    def relay_tokens(h):
        for k, o in numbered(h):
            twin_tokens(k, o).wait_recv()
            diag_tokens(k, o).start()

    def project(h, base, part, sides=2):
        who = owners(h)
        start, count = part

        def unit(i, _):
            m = pl.ds(pl.multiple_of(i % sides * MATE + base + start, 16), count)
            c = pl.ds(pl.multiple_of(i // sides * wch, 128), wch)
            total = None
            for o in who:
                w = wa[pl.ds(pl.multiple_of(o * ks, 16), ks), c]
                term = dot(tok[m, block_of(o)], w)
                total = term if total is None else total + term
            if h == 0:
                acc[m, c] = total
            else:
                acc[m, c] += total
            return 0

        lax.fori_loop(0, sides * 3, unit, 0)

    def project_near(h):
        project(h, OWN, ALL)

    def take_diag_tokens(h):
        for k, o in numbered(h):
            diag_tokens(k, o).wait_recv()

    def project_far(h):
        take_diag_tokens(h)
        project(h, TWIN, ALL)

    def mix(base, part, sides=2):
        start, count = part
        tc = 128
        seqs = count // seq

        def unit(i, _):
            j = i % (sides * seqs)
            m = pl.ds(
                pl.multiple_of(base + j // seqs * MATE + start + j % seqs * seq, seq), seq
            )
            c = pl.multiple_of(i // (sides * seqs) * tc, tc)
            o = acc[m, pl.ds(c, tc)]
            p = (
                acc[m, pl.ds(pl.multiple_of(wch + c, tc), tc)]
                * acc[m, pl.ds(pl.multiple_of(2 * wch + c, tc), tc)]
            )
            place = lax.broadcasted_iota(jnp.int32, p.shape, 0)
            before = jnp.where(place > 0, pltpu.roll(p, 1, 0), 0.0)
            after = jnp.where(place < seq - 1, pltpu.roll(p, seq - 1, 0), 0.0)
            taps = taps_ref[:, pl.ds(pl.multiple_of(share_at + c, tc), tc)]
            conv = taps[0:1] * before + taps[1:2] * p + taps[2:3] * after
            mixed[m, pl.ds(pl.multiple_of(share_at + c, tc), tc)] = (o * conv).astype(BF)
            return 0

        lax.fori_loop(0, sides * seqs * (wch // tc), unit, 0)

    def raise_part(size, start, x_base, acc_base, hs, new, final):
        who = [o for h in hs for o in owners(h)]
        tiles = ff // tn

        def unit(i, _):
            side = i % 2
            c = pl.ds(pl.multiple_of(i // 2 * tn, tn), tn)
            x_row = pl.multiple_of(x_base + side * MATE + start, 16)
            total = None
            for o in who:
                x = fst[pl.ds(x_row, size), block_of(o)]
                term = dot(x, wc[pl.ds(pl.multiple_of(o * ks, 16), ks), c])
                total = term if total is None else total + term
            span = pl.ds(pl.multiple_of(acc_base + side * rows + start, 16), size)
            if not new:
                total = total + acc[span, c]
            if final:
                total = jnp.maximum(total, 0.0)
                hid[pl.ds(x_row, size), c] = (total * total).astype(BF)
            else:
                acc[span, c] = total
            return 0

        lax.fori_loop(0, 2 * tiles, unit, 0)

    def raise_near(h):
        raise_part(rows, 0, OWN, 0, [h], h == 0, h == half)

    def raise_far(part):
        start, count = part
        for p in range(start // seq, (start + count) // seq):
            diag_first(p).wait_recv()
        raise_part(count, start, TWIN, both, range(half + 1), True, True)

    def send_mixed(p):
        for there, here in ((TWIN, OWN), (DIAG, MATE)):
            across_copy(
                ("mixed", there, p),
                mixed.at[pl.ds(there + p * seq, seq), pl.ds(share_at, wch)],
                mixed.at[pl.ds(here + p * seq, seq), pl.ds(share_at, wch)],
                "mixed",
                ("mixed", p),
            ).start()

    def mix_sums(p):
        span = pl.ds(p * seq, seq)
        return mate_copy(("mix", p), psend.at[:, span], precv.at[:, span], "mix")

    def mixout(p):
        span = pl.ds(p * seq, seq)
        if p == 0:
            across_whole(wb.at[pl.ds(0, n - 1), pl.ds(0, wch)], "wb", "wb").wait_recv()
        across_whole(
            mixed.at[pl.ds(0, 2 * seq), pl.ds(0, wch)], "mixed", ("mixed", p)
        ).wait_recv()

        def theirs(b, _):
            psend[b, span] = dot(mixed[pl.ds(MATE + p * seq, seq), :], wb[b]).astype(BF)
            return 0

        lax.fori_loop(0, n, theirs, 0)
        mix_sums(p).start()

        def ours(b, _):
            own[b, span] = dot(mixed[pl.ds(OWN + p * seq, seq), :], wb[b])
            return 0

        lax.fori_loop(0, n, ours, 0)

    def far_block(u, part):
        span = pl.ds(rows + part[0], part[1])
        return mate_copy(("low", u, part), psend.at[u, span], precv.at[u, span], "low")

    def near_group(u):
        return max(u - (n - 3), 0)

    def near_block(u):
        span = pl.ds(0, rows)
        return mate_copy(
            ("low", u), psend.at[u, span], precv.at[u, span], "low", ("low", near_group(u))
        )

    def across_block(u, part):
        span = pl.ds(*part)
        return across_copy(("low", u, part), xsend.at[u, span], xrecv.at[u, span], "low")

    def down(u):
        return jnp.concatenate([wd[o, j] for o, j in units[u]], axis=1)

    def lower_far(u, part):
        start, count = part
        span = pl.ds(rows + start, count)
        psend[u, span] = dot(hid[pl.ds(DIAG + start, count), :], down(u)).astype(BF)
        far_block(u, part).start()
        own[u, span] = dot(hid[pl.ds(TWIN + start, count), :], down(u))

    def low_pass(u, part):
        start, count = part
        far_block(u, part).wait_recv()
        span = pl.ds(rows + start, count)
        xsend[u, pl.ds(start, count)] = (own[u, span] + precv[u, span].astype(F32)).astype(BF)
        across_block(u, part).start()

    def lower_near(u):
        span = pl.ds(0, rows)
        psend[u, span] = dot(hid[pl.ds(MATE, rows), :], down(u)).astype(BF)
        near_block(u).start()
        own[u, span] = dot(hid[pl.ds(OWN, rows), :], down(u))

    def last_near(core):
        near_block(n - 1)

        @pl.when(t == core)
        def _():
            lower_near(n - 1)

    lowered = [[ALL] if 3 <= u < n - 1 else [EARLY, LATE] for u in range(n)]

    def norm(base_ref, gain_ref, dest_ref, start, count):
        tm = 32

        def unit(i, _):
            m = pl.multiple_of(start + i * tm, tm)
            parts = []
            for b in range(n):
                part = (
                    residual_scale
                    * base_ref[pl.ds(m, tm), pl.ds(b * nc, nc)].astype(F32)
                    + own[b, pl.ds(m, tm)]
                )
                parts.append(part + precv[b, pl.ds(m, tm)].astype(F32))
            total = parts[0]
            for b in range(1, n):
                total = total + parts[b]
            mean = jnp.sum(total, axis=-1, keepdims=True) / d
            parts = [p - mean for p in parts]
            square = parts[0] * parts[0]
            for b in range(1, n):
                square = square + parts[b] * parts[b]
            spread = jnp.sum(square, axis=-1, keepdims=True) / d
            scale = lax.rsqrt(spread + norm_epsilon)
            for b in range(n):
                cols = pl.ds(b * nc, nc)
                dest_ref[pl.ds(m, tm), cols] = (
                    parts[b] * scale * gain_ref[:, cols]
                ).astype(BF)
            return 0

        lax.fori_loop(0, count // tm, unit, 0)

    tm = SEQ
    C, D, Q, S = range(4)

    def add_near(first, count):
        def unit(i, _):
            m = pl.ds(pl.multiple_of(i * 32, 32), 32)
            for u in range(first, first + count):
                for i, place in enumerate(units[u]):
                    part = pl.ds(i * lane, lane)
                    own[u, m, part] = (
                        residual_scale * fst[m, columns(*place)].astype(F32)
                        + own[u, m, part]
                        + precv[u, m, part].astype(F32)
                    )
            return 0

        lax.fori_loop(0, rows // 32, unit, 0)

    def add_across(u):
        for part in lowered[u]:
            across_block(u, part).wait_recv()

        def unit(i, _):
            m = pl.ds(pl.multiple_of(i * tm, tm), tm)
            x = own[u, m] + xrecv[u, m].astype(F32)
            own[u, m] = x
            lanes = x[:, :lane] + x[:, lane:]
            stats[S, m] = lanes if u == 0 else stats[S, m] + lanes
            return 0

        lax.fori_loop(0, rows // tm, unit, 0)

    def center():
        def unit(i, _):
            m = pl.ds(pl.multiple_of(i * tm, tm), tm)
            c = jnp.sum(stats[S, m], axis=-1, keepdims=True) / ((n - 1) * nc)
            shift = square = None
            for u in range(n - 1):
                x = own[u, m] - c
                y = x * x
                lanes, squares = x[:, :lane] + x[:, lane:], y[:, :lane] + y[:, lane:]
                shift = lanes if shift is None else shift + lanes
                square = squares if square is None else square + squares
            stats[C, m] = jnp.broadcast_to(c, (tm, lane))
            stats[D, m] = shift
            stats[Q, m] = square
            return 0

        lax.fori_loop(0, rows // tm, unit, 0)

    def finish(part):
        start, count = part
        tail = n - 1
        across_block(tail, part).wait_recv()

        def measure(i, _):
            m = pl.ds(pl.multiple_of(start + i * tm, tm), tm)
            value = own[tail, m] + xrecv[tail, m].astype(F32)
            own[tail, m] = value
            c = stats[C, m]
            x, y = value[:, :lane] - c, value[:, lane:] - c
            shift = jnp.sum(stats[D, m] + (x + y), axis=-1, keepdims=True) / d
            square = jnp.sum(stats[Q, m] + (x * x + y * y), axis=-1, keepdims=True) / d
            spread = jnp.maximum(square - shift * shift, 0.0)
            stats[C, m] = c + shift
            stats[S, m] = jnp.broadcast_to(lax.rsqrt(spread + norm_epsilon), (tm, lane))
            return 0

        lax.fori_loop(0, count // tm, measure, 0)

        def apply(i, _):
            m = pl.ds(pl.multiple_of(start + i * 32, 32), 32)
            mean, scale = stats[C, m], stats[S, m]
            for u in range(n):
                for i, place in enumerate(units[u]):
                    cols = columns(*place)
                    value = own[u, m, pl.ds(i * lane, lane)]
                    out_ref[m, cols] = ((value - mean) * scale * norm2_ref[:, cols]).astype(BF)
            return 0

        lax.fori_loop(0, count // 32, apply, 0)

    def near_first(p):
        return mate_copy(
            ("near", p),
            fst.at[pl.ds(p * seq, seq)],
            fst.at[pl.ds(MATE + p * seq, seq)],
            "near",
            "near",
        )

    def twin_first(p):
        return across_copy(
            ("twin", p),
            fst.at[pl.ds(p * seq, seq)],
            fst.at[pl.ds(TWIN + p * seq, seq)],
            "first",
        )

    def diag_first(p):
        return mate_copy(
            ("diag", p),
            fst.at[pl.ds(TWIN + p * seq, seq)],
            fst.at[pl.ds(DIAG + p * seq, seq)],
            "diag",
        )

    def take_near_sums(first, count):
        mate_whole(
            precv.at[pl.ds(first, count), pl.ds(0, rows)], "low", ("low", near_group(first))
        ).wait_recv()
        add_near(first, count)

    def make_first(p):
        mix_sums(p).wait_recv()
        norm(tok, norm1_ref, fst, p * seq, seq)
        twin_first(p).start()
        near_first(p).start()

    def take_near():
        mate_whole(fst.at[pl.ds(MATE, rows)], "near", "near").wait_recv()

    def relay_first(p):
        twin_first(p).wait_recv()
        diag_first(p).start()

    def free_sends():
        mate_whole(psend.at[:, pl.ds(0, rows)], "mix").wait_send()

    plan = {}

    def after(ti, h, which, *work):
        plan.setdefault((ti, h, which), []).extend(work)

    def do(function, *values):
        return lambda: function(*values)

    last = half - 1

    for h in range(1, half):
        after(0, h, 1, do(cross_wb, h))
    after(0, half, 0, do(cross_wb, half))
    after(0, half, 0, do(relay_tokens, 0), do(project_near, 0), do(project_far, 0))
    for h in range(1, half):
        after(1, h, 0, do(relay_tokens, h))
        after(1, h, 1, do(project_near, h), do(project_far, h))
    after(1, last, 0, do(relay_tokens, half))
    after(1, half, 0, do(take_diag_tokens, half))
    after(1, half, 0, do(project, half, TWIN, EARLY), do(mix, TWIN, EARLY))
    for p in range(most):
        after(1, half, 0, do(send_mixed, p))
    after(1, half, 0, do(project, half, TWIN, LATE), do(mix, TWIN, LATE), do(send_mixed, most))
    after(1, half, 0, do(project_near, half), do(mix, OWN, ALL))
    after(2, 1, 0, do(mixout, 0))
    after(2, 1, 1, do(make_first, 0), do(mixout, 1), do(make_first, 1))
    for p in range(2, pieces):
        after(2, 2, 0, do(mixout, p), do(make_first, p))
    after(2, 2, 1, do(take_near), do(raise_near, 0), do(raise_near, 1))
    after(2, 3, 0, do(raise_near, 2), do(free_sends))
    for h in range(3, half):
        after(2, h, 1, do(raise_near, h))
    after(2, last, 1, do(relay_first, 0))
    after(2, half, 0, do(raise_near, half), do(lower_near, 0))
    for p in range(1, most):
        after(2, half, 0, do(relay_first, p))
    after(2, half, 0, do(raise_far, EARLY))
    after(3, 1, 0, do(lower_far, 0, EARLY), do(lower_far, 1, EARLY))
    after(3, 1, 0, do(low_pass, 0, EARLY), do(low_pass, 1, EARLY), do(relay_first, most))
    after(3, 1, 1, do(lower_far, 2, EARLY), do(low_pass, 2, EARLY), do(raise_far, LATE))
    for u in range(3):
        after(3, 1, 1, do(lower_far, u, LATE))
    for u in range(3):
        after(3, 1, 1, do(low_pass, u, LATE))
    for u in range(3, n - 1):
        e = (3, (u + 1) // 2, (u + 1) % 2)
        near = u - 2 if u < n - 2 else n - 3
        after(*e, do(lower_far, u, ALL), do(lower_near, near), do(low_pass, u, ALL))
    after(3, last, 0, do(lower_near, n - 4))
    after(3, last, 1, do(lower_near, n - 2))
    after(3, last, 1, do(take_near_sums, 0, n - 2))
    for u in range(n - 3):
        after(3, last, 1, do(add_across, u))
    after(3, half, 0, do(lower_far, n - 1, EARLY), do(lower_far, n - 1, LATE))
    after(3, half, 0, do(last_near, 1))
    after(3, half, 0, do(low_pass, n - 1, EARLY), do(low_pass, n - 1, LATE))
    after(3, half, 0, do(last_near, 0), do(take_near_sums, n - 2, 1))
    for u in range(n - 3, n - 1):
        after(3, half, 0, do(add_across, u))
    after(3, half, 0, do(center), do(take_near_sums, n - 1, 1), do(finish, EARLY))
    after(3, half, 0, do(finish, LATE))

    for ti in range(4):
        for e in events(ti):
            event(*e)
            for work in plan.get(e, ()):
                work()

    mate_whole(tok.at[pl.ds(0, both)], "tok").wait_send()
    for group in ("near", "diag"):
        mate_whole(fst.at[pl.ds(0, rows)], group).wait_send()
    mate_whole(psend, "low").wait_send()
    across_whole(tok.at[pl.ds(0, rows)], "tok").wait_send()
    across_whole(wb.at[pl.ds(0, n - 1), pl.ds(0, wch)], "wb").wait_send()
    across_whole(mixed.at[pl.ds(0, both), pl.ds(0, wch)], "mixed").wait_send()
    across_whole(fst.at[pl.ds(0, rows)], "first").wait_send()
    across_whole(xsend, "low").wait_send()
    for ti, ref in enumerate(
        (
            wb.at[pl.ds(0, n - 1), pl.ds(0, wch)],
            wa.at[pl.ds(0, (n - 1) * ks)],
            wc.at[pl.ds(0, (n - 1) * ks)],
            wd.at[pl.ds(0, n - 1)],
        )
    ):
        pltpu.make_async_remote_copy(
            src_ref=ref,
            dst_ref=ref,
            send_sem=ring_send.at[ti],
            recv_sem=ring_recv.at[0],
            device_id=right,
            device_id_type=MESH,
        ).wait_send()


def fits(mesh, args):
    n = mesh.shape["fs"]
    rows, d = args[0].shape
    ks = args[1].shape[0]
    wch = args[1].shape[1] // 2
    nc = args[5].shape[1]
    ff = args[7].shape[1] // 2
    return (
        mesh.shape["rep"] == 2
        and mesh.shape["tp"] == 2
        and n % 2 == 0
        and n >= 8
        and ks % 128 == 0
        and nc == 256
        and wch % 128 == 0
        and ff % 256 == 0
        and wch <= rows
        and ff <= 4 * rows
        and ff <= 3 * wch
        and ks <= rows
        and rows % SEQ == 0
        and 2 * SEQ <= rows <= 8 * SEQ
    )


def fused(mesh, *args):
    (
        tokens,
        outer_weight,
        inner_weight,
        value_weight,
        conv_taps,
        mix_out,
        norm_first,
        up_weight,
        down_weight,
        norm_second,
    ) = args
    n = mesh.shape["fs"]
    rows, d = tokens.shape
    ks = outer_weight.shape[0]
    wch = outer_weight.shape[1] // 2
    ff = up_weight.shape[1] // 2
    nc = mix_out.shape[1]
    both = 2 * rows
    anywhere = pl.BlockSpec(memory_space=pl.ANY)
    vmem = pl.BlockSpec(memory_space=pltpu.VMEM)
    messages = 2 * (2 * n - 2)
    pairs = 2 * n + 9 + 2 * (rows // SEQ)
    crosses = 2 * n + 5 + 2 * (rows // SEQ)
    return pl.pallas_call(
        functools.partial(layer_kernel, n),
        out_shape=pltpu.VMEM((rows, d), BF),
        in_specs=[anywhere] * 10,
        out_specs=vmem,
        scratch_shapes=[
            pltpu.VMEM((n * ks, 3 * wch), BF),
            pltpu.VMEM((n, 2 * wch, nc), BF),
            pltpu.VMEM((n * ks, ff), BF),
            pltpu.VMEM((n, 2, ff, nc // 2), BF),
            pltpu.VMEM((2 * both, d), BF),
            pltpu.VMEM((2 * both, 3 * wch), F32),
            pltpu.VMEM((2 * both, 2 * wch), BF),
            pltpu.VMEM((n, both, nc), F32),
            pltpu.VMEM((n, both, nc), BF),
            pltpu.VMEM((n, both, nc), BF),
            pltpu.VMEM((n, rows, nc), BF),
            pltpu.VMEM((n, rows, nc), BF),
            pltpu.VMEM((2 * both, d), BF),
            pltpu.VMEM((2 * both, ff), BF),
            pltpu.VMEM((4, rows, 128), F32),
            pltpu.VMEM(conv_taps.shape, F32),
            pltpu.VMEM((1, d), F32),
            pltpu.VMEM((1, d), F32),
            pltpu.SemaphoreType.DMA((11,)),
            pltpu.SemaphoreType.DMA((4,)),
            pltpu.SemaphoreType.DMA((messages,)),
            pltpu.SemaphoreType.DMA((5,)),
            pltpu.SemaphoreType.DMA((pairs,)),
            pltpu.SemaphoreType.DMA((5,)),
            pltpu.SemaphoreType.DMA((crosses,)),
        ],
        compiler_params=pltpu.CompilerParams(
            collective_id=0, has_side_effects=True, vmem_limit_bytes=62 * 2**20
        ),
        name="layer",
    )(
        tokens,
        outer_weight,
        inner_weight,
        value_weight,
        conv_taps,
        mix_out,
        norm_first.reshape(1, d),
        up_weight,
        down_weight,
        norm_second.reshape(1, d),
    )


def solution(mesh):
    def body(*args):
        return fused(mesh, *args) if fits(mesh, args) else local(*args)

    return jax.shard_map(
        body,
        mesh=mesh,
        in_specs=(
            P(("rep", "fs", "tp"), None),
            P("fs", "tp"),
            P("fs", "tp"),
            P("fs", "tp"),
            P(None, "tp"),
            P("tp", "fs"),
            P(),
            P("fs", "tp"),
            P("tp", "fs"),
            P(),
        ),
        out_specs=P(("rep", "fs", "tp"), None),
        check_vma=False,
    )
```
